256 devices in a mesh: sp: 64 (over z, x, core), tp: 4 (over y).
Axes of the slice: x: 4, y: 4, z: 8, core: 2. Of those that a mesh axis runs over, the one named last changes fastest.
Arguments:
- stream: bfloat16 [8192, 2048], P(('sp', 'tp')), may hold values from -2.5 to 2.5
- recurrence_input: bfloat16 [8192, 2, 1024], P('sp', None, 'tp'), may hold values from -6 to 6
- output_gate_input: bfloat16 [8192, 2, 1024], P('sp', None, 'tp'), may hold values from -6 to 6
- convolution_taps: bfloat16 [4, 2, 1024], P(None, None, 'tp'), may hold values from -4 to 4
- first_group_gates: bfloat16 [2, 16, 64, 64], P(None, 'tp'), may hold values from -0.75 to 0.75
- second_group_gates: bfloat16 [2, 8, 128, 128], P(None, 'tp'), may hold values from -0.5 to 0.5
- channel_decay: float32 [2, 1024], P(None, 'tp'), may hold values from 4.7 to 13.6
- position_log_extra: float32 [8192, 2, 1024], P('sp', None, 'tp'), may hold values from -1.4 to 0, as said below
- recurrence_output_weight: bfloat16 [2, 1024, 2048], P(None, 'tp'), may hold values from -0.125 to 0.125
- first_norm_gain: float32 [2048], replicated, may hold values from 0.1 to 1.9
- first_norm_bias: float32 [2048], replicated, may hold values from -1.75 to 1.75
- routed_expert_index: int32 [8192, 4], P('sp'), may hold values from 0 to 63, all different within a row; in each aligned block of 32 rows (0 to 31, 32 to 63, ...) at most 2 rows name the same one
- routed_expert_weight: float32 [8192, 4], P('sp'), may hold values from 0.25 to 1
- routed_gate_weight: bfloat16 [64, 2048, 512], P('sp', None, 'tp'), may hold values from -0.125 to 0.125
- routed_up_weight: bfloat16 [64, 2048, 512], P('sp', None, 'tp'), may hold values from -0.125 to 0.125
- routed_down_weight: bfloat16 [64, 512, 2048], P('sp', 'tp'), may hold values from -0.25 to 0.25
- shared_gate_weight: bfloat16 [2048, 512], replicated, may hold values from -0.125 to 0.125
- shared_up_weight: bfloat16 [2048, 512], replicated, may hold values from -0.125 to 0.125
- shared_down_weight: bfloat16 [512, 2048], replicated, may hold values from -0.25 to 0.25
- second_norm_gain: float32 [2048], replicated, may hold values from 0.1 to 1.9
- second_norm_bias: float32 [2048], replicated, may hold values from -1.75 to 1.75
Outputs:
- result: bfloat16 [8192, 2048], P(('sp', 'tp'))
The draws below stay inside these ranges and needn't reach their ends.
Inputs may be any that keep to these rules, and one draw needn't show every extreme that they name: `routed_expert_index`: each row names 4 different experts. In each aligned block of 32 rows no expert is named more than 2 times, and in some block an expert is named exactly 2 times. `position_log_extra`: every entry is negative.
All inputs are finite; a program needn't handle non-finite values.
Results may differ from the reference program's by a relative error of at most 0.015.
Values may be sent and summed in bfloat16 or wider, within the bound.
A program may use at most 64 MiB of HBM per device.

```python
import math
import jax
import jax.numpy as jnp
import numpy as np
from jax import lax

D = 2048
D_HALF = 1024
HEAD_SMALL = 64
HEAD_LARGE = 128
HEADS_SMALL = 16
HEADS_LARGE = 8
DQ = 256
CONV = 4
FE = 512
FE_DEV = 128
FS = 512
K = 4
EXPERTS = 64
TOK_DEV = 128
TOK_Q = 32
TOKENS = 8192
CAP_Q = 2
N_TP = 4


def draw_channel_decay(key, part):
    key_flag = jax.random.fold_in(key, 11)
    key_rate = jax.random.fold_in(key, 12)
    fast_limit = 5
    flags = jax.random.randint(key_flag, (2, D_HALF // HEAD_SMALL), 0, 10) < fast_limit
    channel = jnp.arange(D_HALF)
    head_index = jnp.stack([channel // HEAD_SMALL, channel // HEAD_LARGE])
    fast = jnp.take_along_axis(flags, head_index, axis=1)
    spread = jax.random.uniform(key_rate, (2, D_HALF), jnp.float32)
    fast_rate = jnp.exp(jnp.log(0.005) + spread * jnp.log(0.009 / 0.005))
    slow_rate = jnp.exp(jnp.log(1.25e-06) + spread * jnp.log(4.0))
    rate = jnp.where(fast, fast_rate, slow_rate)
    return -jnp.log(jnp.expm1(rate))


def draw_position_log_extra(key, part):
    key_base = jax.random.fold_in(key, 21)
    key_spot = jax.random.fold_in(key, 22)
    key_depth = jax.random.fold_in(key, 23)
    block_count = TOKENS // TOK_DEV
    base = jnp.exp(jax.random.uniform(key_base, (block_count, 1, 2, D_HALF), jnp.float32, jnp.log(5e-06), jnp.log(2e-05)))
    base = jnp.broadcast_to(base, (block_count, TOK_DEV, 2, D_HALF)).reshape(TOKENS, 2, D_HALF)
    spots = jax.random.randint(key_spot, (2,), 0, TOKENS)
    position = jnp.arange(TOKENS)
    hits = jnp.sum((position[:, None] == spots[None, :]).astype(jnp.float32), axis=1)
    depth = jax.random.uniform(key_depth, (2, D_HALF), jnp.float32, 0.22, 0.69)
    return -(base + hits[:, None, None] * depth[None])


def levels(own_key, shape, split, low, top_value):
    level, own = 1.0, jax.random.fold_in(own_key, 6)
    for dim, parts in split:
        heights = jnp.exp(jax.random.uniform(jax.random.fold_in(own, dim), (parts,), jnp.float32, low / len(split), top_value / len(split)))
        level = level * jnp.repeat(heights, shape[dim] // parts).reshape([-1 if axis == dim else 1 for axis in range(len(shape))])
    return level


def deal_out(rng, own, number, rows, count, top, limit, slope):
    sequence = jax.random.permutation(rng, count)
    heavy_load, ordinary = portions_of(count, rows * top, limit, slope, True), portions_of(count, rows * top, limit, slope, False)
    places = jnp.arange(count)

    def named(tallies, rotation):
        used = int((tallies > 0).sum())
        fixed = max(1, used // 4)
        moved = fixed + (places - fixed + rotation * (used - fixed)) % max(1, count - fixed)
        return jnp.zeros((count,), jnp.int32).at[sequence[jnp.where(places < fixed, places, moved)]].set(jnp.asarray(tallies, jnp.int32))

    tallies = jnp.where(number % 4 == 0, named(heavy_load, number // 4), named(ordinary, number - number // 4 - 1))
    mixed = jax.random.permutation(jax.random.fold_in(own, 3), count)
    donor, sink = mixed[0:count // 2 * 2:2], mixed[1:count // 2 * 2:2]
    margin = jnp.minimum(tallies[donor] - 1, limit - tallies[sink]) // 2
    margin = jnp.where((donor == sequence[0]) | (sink == sequence[0]) | (tallies[sink] == 0), 0, jnp.maximum(margin, 0))
    moved = jax.random.randint(jax.random.fold_in(own, 4), (count // 2,), 0, 1 << 20) % (margin + 1)
    tallies = tallies.at[donor].add(-moved).at[sink].add(moved)
    items = jnp.searchsorted(jnp.cumsum(tallies), jnp.arange(rows * top), side="right").astype(jnp.int32)
    table = items.reshape(top, rows).T
    table = table[jax.random.permutation(jax.random.fold_in(own, 1), rows)]
    rotation = jax.random.randint(jax.random.fold_in(own, 2), (rows, 1), 0, top)
    return jnp.take_along_axis(table, (jnp.arange(top)[None, :] + rotation) % top, axis=1)


def portions_of(number_of, total, reach, skew, full):
    portions = [(1 << 20) // math.isqrt(grade ** skew) + 1 for grade in range(1, number_of + 1)]
    largest = reach if full else min(reach, max(-(-total // number_of), total * portions[0] // sum(portions)))
    least = 1 if total - largest >= number_of - 1 else 0
    counts, spare = [largest] + [least] * (number_of - 1), total - largest - least * (number_of - 1)
    while spare > 0:
        movable = [i for i in range(1, number_of) if counts[i] < largest] or [i for i in range(1, number_of) if counts[i] < reach]
        mass, budget = sum([portions[i] for i in movable]), spare
        for i in movable:
            more = min(reach - counts[i], max(1, budget * portions[i] // mass), spare)
            counts[i] = counts[i] + more
            spare = spare - more
    return np.array(counts)


def noise(key, dims, scale, most, pieces=(), held_as=jnp.bfloat16):
    array = jax.random.normal(key, dims, jnp.float32) * scale
    if len(pieces) > 0:
        array = levels(key, dims, pieces, -0.22, 0.18) * array
    return jnp.clip(array, min=-most, max=most).astype(held_as)


def setup_inputs(seed: int = 0) -> dict:
    streams_of = jax.random.split(jax.random.key(seed), 22)
    stream = noise(streams_of[0], (TOKENS, D), 0.4, 2.5, ((0, 256),))
    recurrence_input = noise(streams_of[1], (TOKENS, 2, D_HALF), 1.0, 6.0, ((0, 64), (2, 4)))
    output_gate_input = noise(streams_of[2], (TOKENS, 2, D_HALF), 1.0, 6.0, ((0, 64), (2, 4)))
    convolution_taps = noise(streams_of[3], (CONV, 2, D_HALF), 1.0, 4.0, ((2, 4),))
    first_group_gates = noise(streams_of[4], (2, HEADS_SMALL, HEAD_SMALL, HEAD_SMALL), HEAD_SMALL ** -0.5, 0.75, ((1, 4),))
    second_group_gates = noise(streams_of[5], (2, HEADS_LARGE, HEAD_LARGE, HEAD_LARGE), HEAD_LARGE ** -0.5, 0.5, ((1, 4),))
    channel_decay = draw_channel_decay(jax.random.fold_in(streams_of[21], 71), 0)
    position_log_extra = draw_position_log_extra(jax.random.fold_in(streams_of[21], 71), 0)
    recurrence_output_weight = noise(streams_of[8], (2, D_HALF, D), (2 * D_HALF) ** -0.5, 0.125, ((1, 4),))
    first_norm_gain = jnp.clip(1.0 + 0.18 * jax.random.normal(streams_of[9], (D,), jnp.float32), 0.1, 1.9)
    first_norm_bias = noise(streams_of[10], (D,), 0.3, 1.75, (), jnp.float32)
    routed_expert_index_keys = jax.random.split(jax.random.fold_in(streams_of[11], 1), TOKENS // TOK_Q)
    routed_expert_index_turns = jax.random.permutation(jax.random.fold_in(streams_of[11], 3), TOKENS // TOK_Q)
    routed_expert_index = jax.vmap(lambda own, number: deal_out(jax.random.fold_in(streams_of[11], 2), own, number, TOK_Q, EXPERTS, K, CAP_Q, 1))(routed_expert_index_keys, routed_expert_index_turns).reshape((TOKENS, K))
    routed_expert_weight = jnp.clip(0.25 + 0.75 * jax.random.uniform(streams_of[12], (TOKENS, K), jnp.float32) ** levels(streams_of[12], (TOKENS, K), ((0, 64),), -0.2, 0.2), 0.25, 1.0)
    routed_gate_weight = noise(streams_of[13], (EXPERTS, D, FE), D ** -0.5, 0.125, ((0, 64), (2, 4)))
    routed_up_weight = noise(streams_of[14], (EXPERTS, D, FE), D ** -0.5, 0.125, ((0, 64), (2, 4)))
    routed_down_weight = noise(streams_of[15], (EXPERTS, FE, D), FE ** -0.5, 0.25, ((0, 64), (1, 4)))
    shared_gate_weight = noise(streams_of[16], (D, FS), D ** -0.5, 0.125)
    shared_up_weight = noise(streams_of[17], (D, FS), D ** -0.5, 0.125)
    shared_down_weight = noise(streams_of[18], (FS, D), FS ** -0.5, 0.25)
    second_norm_gain = jnp.clip(1.0 + 0.18 * jax.random.normal(streams_of[19], (D,), jnp.float32), 0.1, 1.9)
    second_norm_bias = noise(streams_of[20], (D,), 0.3, 1.75, (), jnp.float32)
    return {"stream": stream, "recurrence_input": recurrence_input, "output_gate_input": output_gate_input, "convolution_taps": convolution_taps, "first_group_gates": first_group_gates, "second_group_gates": second_group_gates, "channel_decay": channel_decay, "position_log_extra": position_log_extra, "recurrence_output_weight": recurrence_output_weight, "first_norm_gain": first_norm_gain, "first_norm_bias": first_norm_bias, "routed_expert_index": routed_expert_index, "routed_expert_weight": routed_expert_weight, "routed_gate_weight": routed_gate_weight, "routed_up_weight": routed_up_weight, "routed_down_weight": routed_down_weight, "shared_gate_weight": shared_gate_weight, "shared_up_weight": shared_up_weight, "shared_down_weight": shared_down_weight, "second_norm_gain": second_norm_gain, "second_norm_bias": second_norm_bias}


RESIDUAL_SCALE = 8.0 ** 0.25
NORM_EPSILON = 1e-05

def layer_norm(values, gain_vec, bias_vec):
    row_mean = lax.optimization_barrier(jnp.mean(values, axis=-1, keepdims=True))
    spread = lax.optimization_barrier(jnp.mean(jnp.square(values - row_mean), axis=-1, keepdims=True))
    return (values - row_mean) * lax.rsqrt(spread + NORM_EPSILON) * gain_vec + bias_vec

def rounded(values):
    return lax.optimization_barrier(values.astype(jnp.bfloat16)).astype(jnp.float32)

def block_gates(conv_rows, weights, head_size):
    length = conv_rows.shape[0]
    head_rows = conv_rows.reshape(length, -1, head_size).astype(jnp.float32)
    pre_act = jnp.einsum('thc,ghcd->gthd', head_rows, weights.astype(jnp.float32))
    gate_pair = jax.nn.sigmoid(pre_act).reshape(2, length, -1)
    return (gate_pair[0], gate_pair[1])

def chain_link(first_part, second_part):
    return (first_part[0] * second_part[0], second_part[0] * first_part[1] + second_part[1])

def recurrence_result(recurrence_input, output_gate_input, convolution_taps, first_group_gates, second_group_gates, channel_decay, position_log_extra):
    length = recurrence_input.shape[0]
    tap_count = convolution_taps.shape[0]
    padded = jnp.pad(recurrence_input.astype(jnp.float32), ((tap_count - 1, 0), (0, 0), (0, 0)))
    tap_weights = convolution_taps.astype(jnp.float32)
    summed = tap_weights[0] * padded[0:length]
    for offset in range(1, tap_count):
        summed = summed + tap_weights[offset] * padded[offset:offset + length]
    conv_rows = summed.astype(jnp.bfloat16)
    recur_a, input_a = block_gates(conv_rows[:, 0], first_group_gates, first_group_gates.shape[-1])
    recur_b, input_b = block_gates(conv_rows[:, 1], second_group_gates, second_group_gates.shape[-1])
    recurrence_gate = jnp.stack([recur_a, recur_b], axis=1)
    input_gate = jnp.stack([input_a, input_b], axis=1)
    decay_logarithm = -8.0 * recurrence_gate * jax.nn.softplus(-channel_decay) + position_log_extra
    driving = jnp.sqrt(-jnp.expm1(2.0 * decay_logarithm)) * input_gate * conv_rows.astype(jnp.float32)
    states = lax.associative_scan(chain_link, (jnp.exp(decay_logarithm), driving), axis=0)[1]
    return (jax.nn.gelu(output_gate_input.astype(jnp.float32)) * states).astype(jnp.bfloat16)

def reference(stream, recurrence_input, output_gate_input, convolution_taps, first_group_gates, second_group_gates, channel_decay, position_log_extra, recurrence_output_weight, first_norm_gain, first_norm_bias, routed_expert_index, routed_expert_weight, routed_gate_weight, routed_up_weight, routed_down_weight, shared_gate_weight, shared_up_weight, shared_down_weight, second_norm_gain, second_norm_bias):
    branch_output = recurrence_result(recurrence_input, output_gate_input, convolution_taps, first_group_gates, second_group_gates, channel_decay, position_log_extra)
    run_rows = branch_output.reshape(TOKENS, 2, N_TP, DQ)
    run_weights = recurrence_output_weight.reshape(2, N_TP, DQ, D)
    mixed = jnp.zeros((TOKENS, D), jnp.float32)
    for run_index in range(N_TP):
        partial_value = jnp.einsum('tgc,gcd->td', run_rows[:, :, run_index].astype(jnp.float32), run_weights[:, run_index].astype(jnp.float32))
        mixed = mixed + rounded(partial_value)
    normed = layer_norm(RESIDUAL_SCALE * stream.astype(jnp.float32) + mixed, first_norm_gain, first_norm_bias).astype(jnp.bfloat16)
    block_count = TOKENS // TOK_Q
    block_ids = routed_expert_index.reshape(block_count, TOK_Q * K)
    onehot = (block_ids[:, :, None] == jnp.arange(EXPERTS, dtype=jnp.int32)[None, None, :]).astype(jnp.int32)
    slot_ranks = lax.optimization_barrier(jnp.sum((jnp.cumsum(onehot, axis=1) - onehot) * onehot, axis=2)).astype(jnp.int32)
    targets = (block_ids * block_count + jnp.arange(block_count, dtype=jnp.int32)[:, None]) * CAP_Q + slot_ranks
    entries = jnp.arange(TOKENS * K, dtype=jnp.int32).reshape(block_count, TOK_Q * K)
    table = jnp.full((EXPERTS * block_count * CAP_Q,), TOKENS * K, jnp.int32)
    table = table.at[targets.reshape(-1)].set(entries.reshape(-1)).reshape(EXPERTS, block_count * CAP_Q)
    padded_rows = jnp.concatenate([normed, jnp.zeros((1, D), jnp.bfloat16)], axis=0)
    padded_weights = jnp.concatenate([routed_expert_weight.reshape(-1), jnp.zeros((1,), jnp.float32)])

    def expert_step(routed, inputs):
        entry_rows, gate_w, up_w, down_w = inputs
        token_rows = entry_rows // K
        picked = padded_rows[token_rows]
        hidden = (jax.nn.silu(jnp.dot(picked, gate_w, preferred_element_type=jnp.float32)) * jnp.dot(picked, up_w, preferred_element_type=jnp.float32)).astype(jnp.bfloat16)
        summed_out = jnp.zeros((picked.shape[0], D), jnp.float32)
        for run_index in range(N_TP):
            partial_out = jnp.dot(hidden[:, run_index * FE_DEV:(run_index + 1) * FE_DEV], down_w[run_index * FE_DEV:(run_index + 1) * FE_DEV], preferred_element_type=jnp.float32)
            summed_out = summed_out + rounded(partial_out)
        weighted = padded_weights[entry_rows][:, None] * rounded(summed_out)
        return (routed.at[token_rows].add(weighted), None)
    routed = lax.scan(expert_step, jnp.zeros((TOKENS + 1, D), jnp.float32), (table, routed_gate_weight, routed_up_weight, routed_down_weight))[0][:TOKENS]
    shared_hidden = (jax.nn.silu(jnp.dot(normed, shared_gate_weight, preferred_element_type=jnp.float32)) * jnp.dot(normed, shared_up_weight, preferred_element_type=jnp.float32)).astype(jnp.bfloat16)
    shared_out = jnp.dot(shared_hidden, shared_down_weight, preferred_element_type=jnp.float32)
    moe = shared_out + routed
    final = layer_norm(RESIDUAL_SCALE * normed.astype(jnp.float32) + moe, second_norm_gain, second_norm_bias)
    return final.astype(jnp.bfloat16)
```

```python
import jax
import jax.numpy as jnp
from jax import lax
from jax.experimental import pallas as pl
from jax.experimental.pallas import tpu as pltpu
from jax.sharding import PartitionSpec as P

RESIDUAL_SCALE = 8.0**0.25
NORM_EPSILON = 1e-05
MESH = pl.DeviceIdType.MESH
F32 = jnp.float32
BF16 = jnp.bfloat16

PLANE = 8
PLANES = 8
TPS = 4
HEAD_ROWS = 16
CHUNKS = 2
FAR_FIRST = (4, 3, 5, 2, 6, 1, 7)


def layer_norm(values, gain_vec, bias_vec):
    row_mean = jnp.mean(values, axis=-1, keepdims=True)
    centred = values - row_mean
    spread = jnp.mean(jnp.square(centred), axis=-1, keepdims=True)
    return centred * lax.rsqrt(spread + NORM_EPSILON) * gain_vec + bias_vec


def softplus_of_minus(d):
    u = jnp.exp(-jnp.abs(d))
    s = u / (2.0 + u)
    q = s * s
    series = jnp.full_like(s, 1.0 / 15.0)
    for odd in (13, 11, 9, 7, 5, 3, 1):
        series = series * q + 1.0 / odd
    return jnp.maximum(-d, 0.0) + 2.0 * s * series


def minus_expm1(z):
    series = jnp.full_like(z, 1.0 / 40320.0)
    for factor in (5040.0, 720.0, 120.0, 24.0, 6.0, 2.0, 1.0):
        series = series * z + 1.0 / factor
    return jnp.where(z > -0.25, -z * series, 1.0 - jnp.exp(z))


def dot(a, b):
    return jnp.dot(a, b, preferred_element_type=F32)


def mega(
    stream_h, rec_h, gatein_h, taps_h, small_gates_h, large_gates_h, decay_h, extra_h,
    wout_h, gain1_h, bias1_h, index_h, weight_h, gate_w_h, up_w_h, down_w_h,
    shared_gate_h, shared_up_h, shared_down_h, gain2_h, bias2_h,
    out_ref,
    stream, rec, gatein, taps, small_gates, large_gates, decay, extra,
    wout, gain1, bias1, index, weight, gate_w, up_w, down_w,
    shared_gate, shared_up, shared_down, gain2, bias2,
    rec_f, border, cum_p, cum_s, carry1, carry2, gelu_buf, branch,
    part, mixed_buf, normed, slot_buf, weight_buf,
    disp, arr1, disp2, arr2, moe_out, ret1, ret1p, ret2, acc,
    load_sem, own_sem, border_sem, weight_sem, carry_sem, mix_sem, disp_sem, ret_sem,
):
    sp = lax.axis_index("sp")
    tp = lax.axis_index("tp")
    zi = sp // PLANE
    pi = sp % PLANE
    sends = []

    def load(k, src, dst):
        copy = pltpu.make_async_copy(src, dst, load_sem.at[k])
        copy.start()
        return copy

    def remote(src, dst, sem, where, sp_to, tp_to):
        copy = pltpu.make_async_remote_copy(
            src_ref=src,
            dst_ref=dst,
            send_sem=sem.at[(0, *where)],
            recv_sem=sem.at[(1, *where)],
            device_id={"sp": sp_to, "tp": tp_to},
            device_id_type=MESH,
        )
        return copy

    def send(*args):
        copy = remote(*args)
        copy.start()
        sends.append(copy)

    def plane_peer(d):
        return zi * PLANE + (pi + d) % PLANE

    def z_peer(d):
        return ((zi + d) % PLANES) * PLANE + pi

    names = (
        (rec_h, rec), (small_gates_h, small_gates), (large_gates_h, large_gates), (taps_h, taps),
        (decay_h, decay), (extra_h, extra), (gatein_h, gatein), (gate_w_h, gate_w.at[tp]),
        (up_w_h, up_w.at[tp]), (down_w_h, down_w.at[tp]), (wout_h, wout), (index_h, index),
        (weight_h, weight), (stream_h, stream), (gain1_h, gain1), (bias1_h, bias1),
        (shared_gate_h, shared_gate), (shared_up_h, shared_up), (shared_down_h, shared_down),
        (gain2_h, gain2), (bias2_h, bias2),
    )
    loads = [load(k, src, dst) for k, (src, dst) in enumerate(names)]

    barrier = pltpu.get_barrier_semaphore()

    def greet(sp_to, tp_to):
        pl.semaphore_signal(
            barrier, inc=1, device_id={"sp": sp_to, "tp": tp_to}, device_id_type=MESH
        )

    for d in range(1, PLANE):
        greet(plane_peer(d), tp)
    for d in range(1, PLANES):
        greet(z_peer(d), tp)
    for d in range(1, TPS):
        greet(sp, (tp + d) % TPS)
    greet((sp + 63) % 64, tp)

    for k in range(6):
        loads[k].wait()
    length = rec.shape[0]
    rec_f[HEAD_ROWS:, :] = rec[...].astype(F32)
    row_i = lax.broadcasted_iota(jnp.int32, (64, 128), 0)
    col_i = lax.broadcasted_iota(jnp.int32, (64, 128), 1)
    put_low = (row_i == col_i).astype(BF16)
    put_high = (row_i + 64 == col_i).astype(BF16)
    blocks = []
    for which in range(2):
        maps = []
        for pair in range(2):
            low = dot(small_gates[which, 2 * pair], put_low)
            high = dot(small_gates[which, 2 * pair + 1], put_high)
            maps.append(jnp.concatenate([low, high], axis=0).astype(BF16))
        for head in range(2):
            maps.append(large_gates[which, head])
        blocks.append(maps)
    rate = -8.0 * softplus_of_minus(decay[...])
    tap_f = taps[...].astype(F32)

    def scanned(first, count):
        for b in range(4):
            lanes = slice(128 * b, 128 * b + 128)
            conv = tap_f[0:1, lanes] * rec_f[first + HEAD_ROWS - 3 : first + HEAD_ROWS - 3 + count, lanes]
            for k in range(1, 4):
                at = first + HEAD_ROWS - 3 + k
                conv = conv + tap_f[k : k + 1, lanes] * rec_f[at : at + count, lanes]
            conv = conv.astype(BF16)
            recur_gate = jax.nn.sigmoid(dot(conv, blocks[0][b]))
            input_gate = jax.nn.sigmoid(dot(conv, blocks[1][b]))
            log_decay = recur_gate * rate[:, lanes] + extra[first : first + count, lanes]
            p = jnp.exp(log_decay)
            s = jnp.sqrt(minus_expm1(2.0 * log_decay)) * input_gate * conv.astype(F32)
            p = p.reshape(count // 8, 8, 128)
            s = s.reshape(count // 8, 8, 128)
            row = lax.broadcasted_iota(jnp.int32, (count // 8, 8, 128), 1)
            for by in (1, 2, 4):
                p_prev = pltpu.roll(p, by, 1)
                s_prev = pltpu.roll(s, by, 1)
                s = jnp.where(row >= by, p * s_prev + s, s)
                p = jnp.where(row >= by, p * p_prev, p)
            p_in = jnp.ones((1, 128), F32)
            s_in = jnp.zeros((1, 128), F32)
            for t in range(count // 8):
                s_t = s[t] + p[t] * s_in
                p_t = p[t] * p_in
                cum_s[first + 8 * t : first + 8 * t + 8, lanes] = s_t
                cum_p[first + 8 * t : first + 8 * t + 8, lanes] = p_t
                s_in = s_t[7:8]
                p_in = p_t[7:8]

    scanned(HEAD_ROWS, length - HEAD_ROWS)

    pl.semaphore_wait(barrier, 7 + 7 + 3 + 1)
    send(rec.at[length - HEAD_ROWS :], border, border_sem, (), (sp + 1) % 64, tp)

    left = (tp + 3) % TPS
    right = (tp + 1) % TPS

    def weights_out(buf, slot, to, k):
        send(buf.at[slot], buf.at[slot], weight_sem, (k,), sp, to)

    def weights_in(buf, slot, k):
        remote(buf.at[slot], buf.at[slot], weight_sem, (k,), sp, left).wait_recv()

    opposite = (tp + 2) % TPS
    loads[7].wait()
    weights_out(gate_w, tp, left, 0)
    weights_out(gate_w, tp, right, 1)

    remote(rec.at[length - HEAD_ROWS :], border, border_sem, (), sp, tp).wait_recv()
    border_f = border[...].astype(F32)
    rec_f[0:HEAD_ROWS, :] = jnp.where(sp > 0, border_f, jnp.zeros_like(border_f))
    scanned(0, HEAD_ROWS)

    head_p = cum_p[HEAD_ROWS - 1 : HEAD_ROWS, :]
    head_s = cum_s[HEAD_ROWS - 1 : HEAD_ROWS, :]
    tail_p = cum_p[length - 1 : length, :]
    tail_s = cum_s[length - 1 : length, :]
    total_p = head_p * tail_p
    total_s = tail_p * head_s + tail_s
    mine1 = carry1.at[pi]
    for b in range(4):
        mine1[0, b : b + 1, :] = total_p[:, 128 * b : 128 * b + 128]
        mine1[1, b : b + 1, :] = total_s[:, 128 * b : 128 * b + 128]
    for d in FAR_FIRST:
        send(mine1, mine1, carry_sem, (0, d), plane_peer(d), tp)

    for k in (6, 11, 12):
        loads[k].wait()
    own_rows = pl.ds(pl.multiple_of(tp * 32, 32), 32)
    ids = index[own_rows, :]
    factors = weight[own_rows, :]
    slot = lax.broadcasted_iota(jnp.int32, (32, 128), 1)
    named = jnp.zeros((32, 128), F32)
    scaled = jnp.zeros((32, 128), F32)
    for k in range(4):
        hit = ids[:, k : k + 1] == slot // 2
        named = named + jnp.where(hit, 1.0, 0.0)
        scaled = scaled + jnp.where(hit, factors[:, k : k + 1], 0.0)
    below = lax.broadcasted_iota(jnp.int32, (32, 32), 0) > lax.broadcasted_iota(
        jnp.int32, (32, 32), 1
    )
    earlier = dot(below.astype(BF16), named.astype(BF16))
    right_slot = jnp.abs(earlier - (slot % 2).astype(F32)) < 0.5
    slot_buf[...] = jnp.where(right_slot, named, 0.0).T.astype(BF16)
    scaled = jnp.where(right_slot, scaled, 0.0)
    high = scaled.astype(BF16)
    weight_buf[0] = high
    weight_buf[1] = (scaled - high.astype(F32)).astype(BF16)
    gelu_buf[...] = jax.nn.gelu(gatein[...].astype(F32))

    for d in FAR_FIRST:
        got = carry1.at[(pi + PLANE - d) % PLANE]
        remote(got, got, carry_sem, (0, d), sp, tp).wait_recv()
    one = jnp.ones((4, 128), F32)
    nought = jnp.zeros((4, 128), F32)
    all_p, all_s, in_p, in_s = one, nought, one, nought
    for j in range(PLANE):
        p_j, s_j = carry1[j, 0], carry1[j, 1]
        all_p, all_s = all_p * p_j, p_j * all_s + s_j
        in_p = jnp.where(j < pi, in_p * p_j, in_p)
        in_s = jnp.where(j < pi, p_j * in_s + s_j, in_s)
    mine2 = carry2.at[zi]
    mine2[0] = all_p
    mine2[1] = all_s
    for d in FAR_FIRST:
        send(mine2, mine2, carry_sem, (1, d), z_peer(d), tp)
    for d in FAR_FIRST:
        got = carry2.at[(zi + PLANES - d) % PLANES]
        remote(got, got, carry_sem, (1, d), sp, tp).wait_recv()
    planes_s = nought
    for k in range(PLANES):
        planes_s = jnp.where(k < zi, carry2[k, 0] * planes_s + carry2[k, 1], planes_s)
    carry_in = in_p * planes_s + in_s
    carry_row = jnp.concatenate([carry_in[b : b + 1] for b in range(4)], axis=1)
    carry_tail = head_s + head_p * carry_row
    states = cum_s[:HEAD_ROWS] + cum_p[:HEAD_ROWS] * carry_row
    branch[:HEAD_ROWS, :] = (gelu_buf[:HEAD_ROWS] * states).astype(BF16)
    states = cum_s[HEAD_ROWS:] + cum_p[HEAD_ROWS:] * carry_tail
    branch[HEAD_ROWS:, :] = (gelu_buf[HEAD_ROWS:] * states).astype(BF16)

    loads[10].wait()
    for c in range(4):
        cols = slice(512 * c, 512 * c + 512)
        value = dot(branch[...], wout[:, cols]).astype(BF16)
        part[:, :, cols] = value.reshape(TPS, 32, 512)
        for d in (2, 1, 3):
            to = (tp + d) % TPS
            send(part.at[to, :, cols], mixed_buf.at[tp, :, cols], mix_sem, (c, d), sp, to)
    for k in (8, 9):
        loads[k].wait()
    weights_out(up_w, tp, left, 2)
    weights_out(up_w, tp, right, 3)
    weights_in(gate_w, right, 0)
    weights_in(gate_w, left, 1)
    weights_out(gate_w, right, left, 4)
    for k in (13, 14, 15):
        loads[k].wait()
    for c in range(4):
        cols = slice(512 * c, 512 * c + 512)
        for d in (2, 1, 3):
            came = (tp + TPS - d) % TPS
            got = mixed_buf.at[came, :, cols]
            remote(got, got, mix_sem, (c, d), sp, tp).wait_recv()
    mixed = part[tp].astype(F32)
    for d in (1, 2, 3):
        mixed = mixed + mixed_buf[(tp + d) % TPS].astype(F32)
    normed[...] = layer_norm(
        RESIDUAL_SCALE * stream[...].astype(F32) + mixed, gain1[...], bias1[...]
    ).astype(BF16)

    width = 2048 // CHUNKS

    def exchange(src, dst, sem, hop, c, me, peer):
        cols = slice(width * c, width * c + width)
        size = src.shape[0]
        for d in FAR_FIRST:
            to = (me + d) % size
            send(src.at[to, :, cols], dst.at[me, :, cols], sem, (hop, c, d), peer(d), tp)
        dst[me, :, cols] = src[me, :, cols]

    def arrived(dst, sem, hop, c, me):
        cols = slice(width * c, width * c + width)
        size = dst.shape[0]
        for d in FAR_FIRST:
            got = dst.at[(me + size - d) % size, :, cols]
            remote(got, got, sem, (hop, c, d), sp, tp).wait_recv()

    def swapped(src, c):
        cols = slice(width * c, width * c + width)
        to_row = lax.broadcasted_iota(jnp.int32, (128, 128), 0)
        from_row = lax.broadcasted_iota(jnp.int32, (128, 128), 1)
        outer, inner, pair = to_row // 16, (to_row // 2) % 8, to_row % 2
        pick = (from_row == inner * 16 + outer * 2 + pair).astype(BF16)
        rows = src[:, :, cols].reshape(128, width)
        return dot(pick, rows).astype(BF16).reshape(8, 16, width)

    for c in range(CHUNKS):
        cols = slice(width * c, width * c + width)
        value = dot(slot_buf[...], normed[:, cols]).astype(BF16)
        disp[:, :, cols] = value.reshape(8, 16, width)
        exchange(disp, arr1, disp_sem, 0, c, zi, z_peer)
    weights_out(down_w, tp, left, 6)
    weights_in(up_w, left, 3)
    weights_out(up_w, left, right, 5)
    weights_out(down_w, tp, right, 7)

    for k in (16, 17, 18, 19, 20):
        loads[k].wait()
    rows = normed[...]
    hidden = jax.nn.silu(dot(rows, shared_gate[...])) * dot(rows, shared_up[...])
    acc[...] = RESIDUAL_SCALE * rows.astype(F32) + dot(hidden.astype(BF16), shared_down[...])

    for c in range(CHUNKS):
        cols = slice(width * c, width * c + width)
        arrived(arr1, disp_sem, 0, c, zi)
        disp2[:, :, cols] = swapped(arr1, c)
        exchange(disp2, arr2, disp_sem, 1, c, pi, plane_peer)

    for c in range(CHUNKS):
        arrived(arr2, disp_sem, 1, c, pi)
    weights_in(up_w, right, 2)
    picked = arr2[...].reshape(128, 2048)
    weights_in(gate_w, opposite, 4)
    gated = [dot(picked, gate_w[k]) for k in range(TPS)]
    weights_in(up_w, opposite, 5)
    lifted = [dot(picked, up_w[k]) for k in range(TPS)]
    hidden = jnp.concatenate(
        [(jax.nn.silu(g) * u).astype(BF16) for g, u in zip(gated, lifted)], axis=1
    )
    half = 64
    weights_in(down_w, right, 6)
    right_half = down_w.at[right, :half]
    send(right_half, right_half, weight_sem, (8,), sp, left)
    weights_in(down_w, left, 7)
    left_half = down_w.at[left, half:]
    send(left_half, left_half, weight_sem, (9,), sp, right)
    low, high = down_w.at[opposite, :half], down_w.at[opposite, half:]
    remote(low, low, weight_sem, (8,), sp, left).wait_recv()
    remote(high, high, weight_sem, (9,), sp, left).wait_recv()
    for c in range(CHUNKS):
        cols = slice(width * c, width * c + width)
        value = dot(hidden, down_w[:, :, cols].reshape(512, width)).astype(BF16)
        moe_out[:, :, cols] = value.reshape(8, 16, width)
        exchange(moe_out, ret1, ret_sem, 0, c, pi, plane_peer)

    for c in range(CHUNKS):
        cols = slice(width * c, width * c + width)
        arrived(ret1, ret_sem, 0, c, pi)
        ret1p[:, :, cols] = swapped(ret1, c)
        exchange(ret1p, ret2, ret_sem, 1, c, zi, z_peer)
    for c in range(CHUNKS):
        cols = slice(width * c, width * c + width)
        arrived(ret2, ret_sem, 1, c, zi)
        back = ret2[:, :, cols].reshape(128, width)
        acc[:, cols] = acc[:, cols] + dot(weight_buf[0], back) + dot(weight_buf[1], back)
    out_ref[...] = layer_norm(acc[...], gain2[...], bias2[...]).astype(BF16)
    for copy in sends:
        copy.wait_send()


def shards(
    stream, recurrence_input, output_gate_input, convolution_taps, first_group_gates,
    second_group_gates, channel_decay, position_log_extra, recurrence_output_weight,
    first_norm_gain, first_norm_bias, routed_expert_index, routed_expert_weight,
    routed_gate_weight, routed_up_weight, routed_down_weight, shared_gate_weight,
    shared_up_weight, shared_down_weight, second_norm_gain, second_norm_bias,
):
    operands = (
        stream,
        recurrence_input.reshape(128, 512),
        output_gate_input.reshape(128, 512),
        convolution_taps.reshape(4, 512),
        first_group_gates,
        second_group_gates,
        channel_decay.reshape(1, 512),
        position_log_extra.reshape(128, 512),
        recurrence_output_weight.reshape(512, 2048),
        first_norm_gain.reshape(1, 2048),
        first_norm_bias.reshape(1, 2048),
        routed_expert_index,
        routed_expert_weight,
        routed_gate_weight.reshape(2048, 128),
        routed_up_weight.reshape(2048, 128),
        routed_down_weight.reshape(128, 2048),
        shared_gate_weight,
        shared_up_weight,
        shared_down_weight,
        second_norm_gain.reshape(1, 2048),
        second_norm_bias.reshape(1, 2048),
    )
    gathered = {13: (4, 2048, 128), 14: (4, 2048, 128), 15: (4, 128, 2048)}
    held = [
        pltpu.VMEM(gathered.get(k, operand.shape), operand.dtype)
        for k, operand in enumerate(operands)
    ]
    wide = pltpu.VMEM((8, 16, 2048), BF16)
    return pl.pallas_call(
        mega,
        out_shape=jax.ShapeDtypeStruct((32, 2048), BF16),
        in_specs=[pl.BlockSpec(memory_space=pl.ANY)] * len(operands),
        out_specs=pl.BlockSpec(memory_space=pltpu.VMEM),
        scratch_shapes=[
            *held,
            pltpu.VMEM((128 + HEAD_ROWS, 512), F32),
            pltpu.VMEM((HEAD_ROWS, 512), BF16),
            pltpu.VMEM((128, 512), F32),
            pltpu.VMEM((128, 512), F32),
            pltpu.VMEM((PLANE, 2, 4, 128), F32),
            pltpu.VMEM((PLANES, 2, 4, 128), F32),
            pltpu.VMEM((128, 512), F32),
            pltpu.VMEM((128, 512), BF16),
            pltpu.VMEM((TPS, 32, 2048), BF16),
            pltpu.VMEM((TPS, 32, 2048), BF16),
            pltpu.VMEM((32, 2048), BF16),
            pltpu.VMEM((128, 32), BF16),
            pltpu.VMEM((2, 32, 128), BF16),
            wide, wide, wide, wide, wide, wide, wide, wide,
            pltpu.VMEM((32, 2048), F32),
            pltpu.SemaphoreType.DMA((len(operands),)),
            pltpu.SemaphoreType.DMA((2,)),
            pltpu.SemaphoreType.DMA((2,)),
            pltpu.SemaphoreType.DMA((2, 10)),
            pltpu.SemaphoreType.DMA((2, 2, 8)),
            pltpu.SemaphoreType.DMA((2, 4, 4)),
            pltpu.SemaphoreType.DMA((2, 2, CHUNKS, 8)),
            pltpu.SemaphoreType.DMA((2, 2, CHUNKS, 8)),
        ],
        compiler_params=pltpu.CompilerParams(
            collective_id=0, has_side_effects=True, vmem_limit_bytes=56 * 2**20
        ),
        name="mega",
    )(*operands)


def solution(mesh):
    in_specs = (
        P(("sp", "tp"), None),
        P("sp", None, "tp"),
        P("sp", None, "tp"),
        P(None, None, "tp"),
        P(None, "tp", None, None),
        P(None, "tp", None, None),
        P(None, "tp"),
        P("sp", None, "tp"),
        P(None, "tp", None),
        P(),
        P(),
        P("sp", None),
        P("sp", None),
        P("sp", None, "tp"),
        P("sp", None, "tp"),
        P("sp", "tp", None),
        P(),
        P(),
        P(),
        P(),
        P(),
    )
    out_specs = P(("sp", "tp"), None)
    return jax.shard_map(shards, mesh=mesh, in_specs=in_specs, out_specs=out_specs, check_vma=False)
```

```python
import jax
import jax.numpy as jnp
from jax import lax
from jax.experimental import pallas as pl
from jax.experimental.pallas import tpu as pltpu
from jax.sharding import PartitionSpec as P

RESIDUAL_SCALE = 8.0**0.25
NORM_EPSILON = 1e-05
MESH = pl.DeviceIdType.MESH
F32 = jnp.float32
BF16 = jnp.bfloat16

PLANE = 8
PLANES = 8
TPS = 4
HEAD_ROWS = 16
CHUNKS = 2
FAR_FIRST = (4, 3, 5, 2, 6, 1, 7)


class Phases:
    def __init__(self):
        self.scope = None

    def __call__(self, name=None):
        if self.scope is not None:
            self.scope.__exit__(None, None, None)
        self.scope = None
        if name is not None:
            self.scope = jax.named_scope(name)
            self.scope.__enter__()


def layer_norm(values, gain_vec, bias_vec):
    row_mean = jnp.mean(values, axis=-1, keepdims=True)
    centred = values - row_mean
    spread = jnp.mean(jnp.square(centred), axis=-1, keepdims=True)
    return centred * lax.rsqrt(spread + NORM_EPSILON) * gain_vec + bias_vec


def softplus_of_minus(d):
    u = jnp.exp(-jnp.abs(d))
    s = u / (2.0 + u)
    q = s * s
    series = jnp.full_like(s, 1.0 / 15.0)
    for odd in (13, 11, 9, 7, 5, 3, 1):
        series = series * q + 1.0 / odd
    return jnp.maximum(-d, 0.0) + 2.0 * s * series


def minus_expm1(z):
    series = jnp.full_like(z, 1.0 / 40320.0)
    for factor in (5040.0, 720.0, 120.0, 24.0, 6.0, 2.0, 1.0):
        series = series * z + 1.0 / factor
    return jnp.where(z > -0.25, -z * series, 1.0 - jnp.exp(z))


def dot(a, b):
    return jnp.dot(a, b, preferred_element_type=F32)


def mega(
    stream_h, rec_h, gatein_h, taps_h, small_gates_h, large_gates_h, decay_h, extra_h,
    wout_h, gain1_h, bias1_h, index_h, weight_h, gate_w_h, up_w_h, down_w_h,
    shared_gate_h, shared_up_h, shared_down_h, gain2_h, bias2_h,
    out_ref,
    stream, rec, gatein, taps, small_gates, large_gates, decay, extra_raw,
    wout, gain1, bias1, index, weight, gate_w, up_w, down_w,
    shared_gate, shared_up, shared_down, gain2, bias2,
    extra, turned, rec_f, border, cum_p, cum_s, carry1, carry2, gelu_buf, branch,
    part, mixed_buf, normed, slot_buf, weight_buf,
    disp, arr1, disp2, arr2, moe_out, ret1, ret1p, ret2, acc,
    load_sem, own_sem, border_sem, weight_sem, carry_sem, mix_sem, disp_sem, ret_sem,
):
    sp = lax.axis_index("sp")
    tp = lax.axis_index("tp")
    zi = sp // PLANE
    pi = sp % PLANE
    sends = []
    phase = Phases()
    phase("loads")

    def load(k, src, dst):
        copy = pltpu.make_async_copy(src, dst, load_sem.at[k])
        copy.start()
        return copy

    def remote(src, dst, sem, where, sp_to, tp_to):
        copy = pltpu.make_async_remote_copy(
            src_ref=src,
            dst_ref=dst,
            send_sem=sem.at[(0, *where)],
            recv_sem=sem.at[(1, *where)],
            device_id={"sp": sp_to, "tp": tp_to},
            device_id_type=MESH,
        )
        return copy

    def send(*args):
        copy = remote(*args)
        copy.start()
        sends.append(copy)

    def plane_peer(d):
        return zi * PLANE + (pi + d) % PLANE

    def z_peer(d):
        return ((zi + d) % PLANES) * PLANE + pi

    names = (
        (rec_h, rec), (small_gates_h, small_gates), (large_gates_h, large_gates), (taps_h, taps),
        (decay_h, decay), (extra_h, extra_raw), (gatein_h, gatein), (gate_w_h, gate_w.at[tp]),
        (up_w_h, up_w.at[tp]), (down_w_h, down_w.at[tp]), (wout_h, wout), (index_h, index),
        (weight_h, weight), (stream_h, stream), (gain1_h, gain1), (bias1_h, bias1),
        (shared_gate_h, shared_gate), (shared_up_h, shared_up), (shared_down_h, shared_down),
        (gain2_h, gain2), (bias2_h, bias2),
    )
    loads = [load(k, src, dst) for k, (src, dst) in enumerate(names)]

    barrier = pltpu.get_barrier_semaphore()

    def greet(sp_to, tp_to):
        pl.semaphore_signal(
            barrier, inc=1, device_id={"sp": sp_to, "tp": tp_to}, device_id_type=MESH
        )

    for d in range(1, PLANE):
        greet(plane_peer(d), tp)
    for d in range(1, PLANES):
        greet(z_peer(d), tp)
    for d in range(1, TPS):
        greet(sp, (tp + d) % TPS)
    greet((sp + 63) % 64, tp)

    phase("wait_loads")
    for k in range(6):
        loads[k].wait()
    length = rec.shape[0]
    phase("prepare")
    for g in range(2):
        rec_f[HEAD_ROWS:, 256 * g : 256 * g + 256] = rec[:, g, :].astype(F32)
        extra[:, 256 * g : 256 * g + 256] = extra_raw[:, g, :]
    row_i = lax.broadcasted_iota(jnp.int32, (64, 128), 0)
    col_i = lax.broadcasted_iota(jnp.int32, (64, 128), 1)
    put_low = (row_i == col_i).astype(BF16)
    put_high = (row_i + 64 == col_i).astype(BF16)
    blocks = []
    for which in range(2):
        maps = []
        for pair in range(2):
            low = dot(small_gates[which, 2 * pair], put_low)
            high = dot(small_gates[which, 2 * pair + 1], put_high)
            maps.append(jnp.concatenate([low, high], axis=0).astype(BF16))
        for head in range(2):
            maps.append(large_gates[which, head])
        blocks.append(maps)
    rate = -8.0 * softplus_of_minus(decay[...])
    tap_f = taps[...].astype(F32)

    def tap(k, b):
        return tap_f[k, b // 2 : b // 2 + 1, 128 * (b % 2) : 128 * (b % 2) + 128]

    def scanned(first, count):
        for b in range(4):
            lanes = slice(128 * b, 128 * b + 128)
            conv = tap(0, b) * rec_f[first + HEAD_ROWS - 3 : first + HEAD_ROWS - 3 + count, lanes]
            for k in range(1, 4):
                at = first + HEAD_ROWS - 3 + k
                conv = conv + tap(k, b) * rec_f[at : at + count, lanes]
            conv = conv.astype(BF16)
            recur_gate = jax.nn.sigmoid(dot(conv, blocks[0][b]))
            input_gate = jax.nn.sigmoid(dot(conv, blocks[1][b]))
            log_decay = recur_gate * rate[b // 2 : b // 2 + 1, 128 * (b % 2) : 128 * (b % 2) + 128] + extra[first : first + count, lanes]
            p = jnp.exp(log_decay)
            s = jnp.sqrt(minus_expm1(2.0 * log_decay)) * input_gate * conv.astype(F32)
            p = p.reshape(count // 8, 8, 128)
            s = s.reshape(count // 8, 8, 128)
            row = lax.broadcasted_iota(jnp.int32, (count // 8, 8, 128), 1)
            for by in (1, 2, 4):
                p_prev = pltpu.roll(p, by, 1)
                s_prev = pltpu.roll(s, by, 1)
                s = jnp.where(row >= by, p * s_prev + s, s)
                p = jnp.where(row >= by, p * p_prev, p)
            p_in = jnp.ones((1, 128), F32)
            s_in = jnp.zeros((1, 128), F32)
            for t in range(count // 8):
                s_t = s[t] + p[t] * s_in
                p_t = p[t] * p_in
                cum_s[first + 8 * t : first + 8 * t + 8, lanes] = s_t
                cum_p[first + 8 * t : first + 8 * t + 8, lanes] = p_t
                s_in = s_t[7:8]
                p_in = p_t[7:8]

    phase("scan_tail")
    scanned(HEAD_ROWS, length - HEAD_ROWS)
    phase("barrier")

    pl.semaphore_wait(barrier, 7 + 7 + 3 + 1)
    send(rec.at[length - HEAD_ROWS :], border, border_sem, (), (sp + 1) % 64, tp)

    left = (tp + 3) % TPS
    right = (tp + 1) % TPS

    def weights_out(buf, slot, to, k):
        send(buf.at[slot], buf.at[slot], weight_sem, (k,), sp, to)

    def weights_in(buf, slot, k):
        remote(buf.at[slot], buf.at[slot], weight_sem, (k,), sp, left).wait_recv()

    opposite = (tp + 2) % TPS
    phase("send_gate")
    loads[7].wait()
    weights_out(gate_w, tp, left, 0)
    weights_out(gate_w, tp, right, 1)

    phase("border")
    remote(rec.at[length - HEAD_ROWS :], border, border_sem, (), sp, tp).wait_recv()
    phase("scan_head")
    for g in range(2):
        border_f = border[:, g, :].astype(F32)
        rec_f[0:HEAD_ROWS, 256 * g : 256 * g + 256] = jnp.where(
            sp > 0, border_f, jnp.zeros_like(border_f)
        )
    scanned(0, HEAD_ROWS)

    head_p = cum_p[HEAD_ROWS - 1 : HEAD_ROWS, :]
    head_s = cum_s[HEAD_ROWS - 1 : HEAD_ROWS, :]
    tail_p = cum_p[length - 1 : length, :]
    tail_s = cum_s[length - 1 : length, :]
    total_p = head_p * tail_p
    total_s = tail_p * head_s + tail_s
    mine1 = carry1.at[pi]
    for b in range(4):
        mine1[0, b : b + 1, :] = total_p[:, 128 * b : 128 * b + 128]
        mine1[1, b : b + 1, :] = total_s[:, 128 * b : 128 * b + 128]
    for d in FAR_FIRST:
        send(mine1, mine1, carry_sem, (0, d), plane_peer(d), tp)

    phase("slots")
    for k in (6, 11, 12):
        loads[k].wait()
    own_rows = pl.ds(pl.multiple_of(tp * 32, 32), 32)
    unused = jnp.zeros((4, 128), F32)
    turned[0] = jnp.concatenate([index[...].astype(F32), unused], axis=0).T
    turned[1] = jnp.concatenate([weight[...], unused], axis=0).T
    ids = turned[0, own_rows, :].astype(jnp.int32)
    factors = turned[1, own_rows, :]
    slot = lax.broadcasted_iota(jnp.int32, (32, 128), 1)
    named = jnp.zeros((32, 128), F32)
    scaled = jnp.zeros((32, 128), F32)
    for k in range(4):
        hit = ids[:, k : k + 1] == slot // 2
        named = named + jnp.where(hit, 1.0, 0.0)
        scaled = scaled + jnp.where(hit, factors[:, k : k + 1], 0.0)
    below = lax.broadcasted_iota(jnp.int32, (32, 32), 0) > lax.broadcasted_iota(
        jnp.int32, (32, 32), 1
    )
    earlier = dot(below.astype(BF16), named.astype(BF16))
    right_slot = jnp.abs(earlier - (slot % 2).astype(F32)) < 0.5
    slot_buf[...] = jnp.where(right_slot, named, 0.0).T.astype(BF16)
    scaled = jnp.where(right_slot, scaled, 0.0)
    high = scaled.astype(BF16)
    weight_buf[0] = high
    weight_buf[1] = (scaled - high.astype(F32)).astype(BF16)
    for g in range(2):
        gelu_buf[:, 256 * g : 256 * g + 256] = jax.nn.gelu(gatein[:, g, :].astype(F32))
    phase("carry1")

    for d in FAR_FIRST:
        got = carry1.at[(pi + PLANE - d) % PLANE]
        remote(got, got, carry_sem, (0, d), sp, tp).wait_recv()
    one = jnp.ones((4, 128), F32)
    nought = jnp.zeros((4, 128), F32)
    all_p, all_s, in_p, in_s = one, nought, one, nought
    for j in range(PLANE):
        p_j, s_j = carry1[j, 0], carry1[j, 1]
        all_p, all_s = all_p * p_j, p_j * all_s + s_j
        in_p = jnp.where(j < pi, in_p * p_j, in_p)
        in_s = jnp.where(j < pi, p_j * in_s + s_j, in_s)
    mine2 = carry2.at[zi]
    mine2[0] = all_p
    mine2[1] = all_s
    for d in FAR_FIRST:
        send(mine2, mine2, carry_sem, (1, d), z_peer(d), tp)
    phase("carry2")
    for d in FAR_FIRST:
        got = carry2.at[(zi + PLANES - d) % PLANES]
        remote(got, got, carry_sem, (1, d), sp, tp).wait_recv()
    phase("fixup")
    planes_s = nought
    for k in range(PLANES):
        planes_s = jnp.where(k < zi, carry2[k, 0] * planes_s + carry2[k, 1], planes_s)
    carry_in = in_p * planes_s + in_s
    carry_row = jnp.concatenate([carry_in[b : b + 1] for b in range(4)], axis=1)
    carry_tail = head_s + head_p * carry_row
    states = cum_s[:HEAD_ROWS] + cum_p[:HEAD_ROWS] * carry_row
    branch[:HEAD_ROWS, :] = (gelu_buf[:HEAD_ROWS] * states).astype(BF16)
    states = cum_s[HEAD_ROWS:] + cum_p[HEAD_ROWS:] * carry_tail
    branch[HEAD_ROWS:, :] = (gelu_buf[HEAD_ROWS:] * states).astype(BF16)

    phase("out_proj")
    loads[10].wait()
    for c in range(4):
        cols = slice(512 * c, 512 * c + 512)
        value = dot(branch[...], wout[:, cols]).astype(BF16)
        part[:, :, cols] = value.reshape(TPS, 32, 512)
        for d in (2, 1, 3):
            to = (tp + d) % TPS
            send(part.at[to, :, cols], mixed_buf.at[tp, :, cols], mix_sem, (c, d), sp, to)
    phase("gate_arrive")
    for k in (8, 9):
        loads[k].wait()
    weights_out(up_w, tp, left, 2)
    weights_out(up_w, tp, right, 3)
    weights_in(gate_w, right, 0)
    weights_in(gate_w, left, 1)
    weights_out(gate_w, right, left, 4)
    phase("mix_arrive")
    for k in (13, 14, 15):
        loads[k].wait()
    for c in range(4):
        cols = slice(512 * c, 512 * c + 512)
        for d in (2, 1, 3):
            came = (tp + TPS - d) % TPS
            got = mixed_buf.at[came, :, cols]
            remote(got, got, mix_sem, (c, d), sp, tp).wait_recv()
    phase("norm1")
    mixed = part[tp].astype(F32)
    for d in (1, 2, 3):
        mixed = mixed + mixed_buf[(tp + d) % TPS].astype(F32)
    normed[...] = layer_norm(
        RESIDUAL_SCALE * stream[...].astype(F32) + mixed, gain1[...], bias1[...]
    ).astype(BF16)

    width = 2048 // CHUNKS

    def exchange(src, dst, sem, hop, c, me, peer):
        cols = slice(width * c, width * c + width)
        size = src.shape[0]
        for d in FAR_FIRST:
            to = (me + d) % size
            send(src.at[to, :, cols], dst.at[me, :, cols], sem, (hop, c, d), peer(d), tp)
        dst[me, :, cols] = src[me, :, cols]

    def arrived(dst, sem, hop, c, me):
        cols = slice(width * c, width * c + width)
        size = dst.shape[0]
        for d in FAR_FIRST:
            got = dst.at[(me + size - d) % size, :, cols]
            remote(got, got, sem, (hop, c, d), sp, tp).wait_recv()

    def swapped(src, c):
        cols = slice(width * c, width * c + width)
        to_row = lax.broadcasted_iota(jnp.int32, (128, 128), 0)
        from_row = lax.broadcasted_iota(jnp.int32, (128, 128), 1)
        outer, inner, pair = to_row // 16, (to_row // 2) % 8, to_row % 2
        pick = (from_row == inner * 16 + outer * 2 + pair).astype(BF16)
        rows = src[:, :, cols].reshape(128, width)
        return dot(pick, rows).astype(BF16).reshape(8, 16, width)

    phase("dispatch")
    for c in range(CHUNKS):
        cols = slice(width * c, width * c + width)
        value = dot(slot_buf[...], normed[:, cols]).astype(BF16)
        disp[:, :, cols] = value.reshape(8, 16, width)
        exchange(disp, arr1, disp_sem, 0, c, zi, z_peer)
    phase("up_from_left")
    weights_out(down_w, tp, left, 6)
    weights_in(up_w, left, 3)
    weights_out(up_w, left, right, 5)
    weights_out(down_w, tp, right, 7)

    phase("shared")
    for k in (16, 17, 18, 19, 20):
        loads[k].wait()
    rows = normed[...]
    hidden = jax.nn.silu(dot(rows, shared_gate[...])) * dot(rows, shared_up[...])
    acc[...] = RESIDUAL_SCALE * rows.astype(F32) + dot(hidden.astype(BF16), shared_down[...])

    for c in range(CHUNKS):
        cols = slice(width * c, width * c + width)
        phase(f"disp_z_{c}")
        arrived(arr1, disp_sem, 0, c, zi)
        phase(f"disp_swap_{c}")
        disp2[:, :, cols] = swapped(arr1, c)
        exchange(disp2, arr2, disp_sem, 1, c, pi, plane_peer)

    for c in range(CHUNKS):
        phase(f"disp_p_{c}")
        arrived(arr2, disp_sem, 1, c, pi)
    phase("gate_opposite")
    weights_in(up_w, right, 2)
    picked = arr2[...].reshape(128, 2048)
    weights_in(gate_w, opposite, 4)
    phase("gated")
    gated = [dot(picked, gate_w[k]) for k in range(TPS)]
    phase("up_opposite")
    weights_in(up_w, opposite, 5)
    phase("lifted")
    lifted = [dot(picked, up_w[k]) for k in range(TPS)]
    hidden = jnp.concatenate(
        [(jax.nn.silu(g) * u).astype(BF16) for g, u in zip(gated, lifted)], axis=1
    )
    phase("down_arrive")
    half = 64
    weights_in(down_w, right, 6)
    right_half = down_w.at[right, :half]
    send(right_half, right_half, weight_sem, (8,), sp, left)
    weights_in(down_w, left, 7)
    left_half = down_w.at[left, half:]
    send(left_half, left_half, weight_sem, (9,), sp, right)
    phase("down_opposite")
    low, high = down_w.at[opposite, :half], down_w.at[opposite, half:]
    remote(low, low, weight_sem, (8,), sp, left).wait_recv()
    remote(high, high, weight_sem, (9,), sp, left).wait_recv()
    for c in range(CHUNKS):
        cols = slice(width * c, width * c + width)
        phase(f"down_{c}")
        value = dot(hidden, down_w[:, :, cols].reshape(512, width)).astype(BF16)
        moe_out[:, :, cols] = value.reshape(8, 16, width)
        exchange(moe_out, ret1, ret_sem, 0, c, pi, plane_peer)

    for c in range(CHUNKS):
        cols = slice(width * c, width * c + width)
        phase(f"ret_p_{c}")
        arrived(ret1, ret_sem, 0, c, pi)
        phase(f"ret_swap_{c}")
        ret1p[:, :, cols] = swapped(ret1, c)
        exchange(ret1p, ret2, ret_sem, 1, c, zi, z_peer)
    for c in range(CHUNKS):
        cols = slice(width * c, width * c + width)
        phase(f"ret_z_{c}")
        arrived(ret2, ret_sem, 1, c, zi)
        phase(f"combine_{c}")
        back = ret2[:, :, cols].reshape(128, width)
        acc[:, cols] = acc[:, cols] + dot(weight_buf[0], back) + dot(weight_buf[1], back)
    phase("norm2")
    out_ref[...] = layer_norm(acc[...], gain2[...], bias2[...]).astype(BF16)
    phase("drain")
    for copy in sends:
        copy.wait_send()
    phase()


def shards(
    stream, recurrence_input, output_gate_input, convolution_taps, first_group_gates,
    second_group_gates, channel_decay, position_log_extra, recurrence_output_weight,
    first_norm_gain, first_norm_bias, routed_expert_index, routed_expert_weight,
    routed_gate_weight, routed_up_weight, routed_down_weight, shared_gate_weight,
    shared_up_weight, shared_down_weight, second_norm_gain, second_norm_bias,
):
    operands = (
        stream,
        recurrence_input,
        output_gate_input,
        convolution_taps,
        first_group_gates,
        second_group_gates,
        channel_decay,
        position_log_extra,
        recurrence_output_weight.reshape(512, 2048),
        first_norm_gain.reshape(1, 2048),
        first_norm_bias.reshape(1, 2048),
        routed_expert_index.T,
        routed_expert_weight.T,
        routed_gate_weight.reshape(2048, 128),
        routed_up_weight.reshape(2048, 128),
        routed_down_weight.reshape(128, 2048),
        shared_gate_weight,
        shared_up_weight,
        shared_down_weight,
        second_norm_gain.reshape(1, 2048),
        second_norm_bias.reshape(1, 2048),
    )
    gathered = {13: (4, 2048, 128), 14: (4, 2048, 128), 15: (4, 128, 2048)}
    held = [
        pltpu.VMEM(gathered.get(k, operand.shape), operand.dtype)
        for k, operand in enumerate(operands)
    ]
    wide = pltpu.VMEM((8, 16, 2048), BF16)
    return pl.pallas_call(
        mega,
        out_shape=jax.ShapeDtypeStruct((32, 2048), BF16),
        in_specs=[pl.BlockSpec(memory_space=pl.ANY)] * len(operands),
        out_specs=pl.BlockSpec(memory_space=pltpu.VMEM),
        scratch_shapes=[
            *held,
            pltpu.VMEM((128, 512), F32),
            pltpu.VMEM((2, 128, 8), F32),
            pltpu.VMEM((128 + HEAD_ROWS, 512), F32),
            pltpu.VMEM((HEAD_ROWS, 2, 256), BF16),
            pltpu.VMEM((128, 512), F32),
            pltpu.VMEM((128, 512), F32),
            pltpu.VMEM((PLANE, 2, 4, 128), F32),
            pltpu.VMEM((PLANES, 2, 4, 128), F32),
            pltpu.VMEM((128, 512), F32),
            pltpu.VMEM((128, 512), BF16),
            pltpu.VMEM((TPS, 32, 2048), BF16),
            pltpu.VMEM((TPS, 32, 2048), BF16),
            pltpu.VMEM((32, 2048), BF16),
            pltpu.VMEM((128, 32), BF16),
            pltpu.VMEM((2, 32, 128), BF16),
            wide, wide, wide, wide, wide, wide, wide, wide,
            pltpu.VMEM((32, 2048), F32),
            pltpu.SemaphoreType.DMA((len(operands),)),
            pltpu.SemaphoreType.DMA((2,)),
            pltpu.SemaphoreType.DMA((2,)),
            pltpu.SemaphoreType.DMA((2, 10)),
            pltpu.SemaphoreType.DMA((2, 2, 8)),
            pltpu.SemaphoreType.DMA((2, 4, 4)),
            pltpu.SemaphoreType.DMA((2, 2, CHUNKS, 8)),
            pltpu.SemaphoreType.DMA((2, 2, CHUNKS, 8)),
        ],
        compiler_params=pltpu.CompilerParams(
            collective_id=0, has_side_effects=True, vmem_limit_bytes=56 * 2**20
        ),
        name="mega",
    )(*operands)


def solution(mesh):
    in_specs = (
        P(("sp", "tp"), None),
        P("sp", None, "tp"),
        P("sp", None, "tp"),
        P(None, None, "tp"),
        P(None, "tp", None, None),
        P(None, "tp", None, None),
        P(None, "tp"),
        P("sp", None, "tp"),
        P(None, "tp", None),
        P(),
        P(),
        P("sp", None),
        P("sp", None),
        P("sp", None, "tp"),
        P("sp", None, "tp"),
        P("sp", "tp", None),
        P(),
        P(),
        P(),
        P(),
        P(),
    )
    out_specs = P(("sp", "tp"), None)
    return jax.shard_map(shards, mesh=mesh, in_specs=in_specs, out_specs=out_specs, check_vma=False)
```

```python
import jax
import jax.numpy as jnp
from jax import lax
from jax.experimental import pallas as pl
from jax.experimental.pallas import tpu as pltpu
from jax.sharding import PartitionSpec as P

RESIDUAL_SCALE = 8.0**0.25
NORM_EPSILON = 1e-05
MESH = pl.DeviceIdType.MESH
F32 = jnp.float32
BF16 = jnp.bfloat16

PLANE = 8
PLANES = 8
TPS = 4
HEAD_ROWS = 16
CHUNKS = 2
FAR_FIRST = (4, 3, 5, 2, 6, 1, 7)


class Phases:
    def __init__(self):
        self.scope = None

    def __call__(self, name=None):
        if self.scope is not None:
            self.scope.__exit__(None, None, None)
        self.scope = None
        if name is not None:
            self.scope = jax.named_scope(name)
            self.scope.__enter__()


def layer_norm(values, gain_vec, bias_vec):
    row_mean = jnp.mean(values, axis=-1, keepdims=True)
    centred = values - row_mean
    spread = jnp.mean(jnp.square(centred), axis=-1, keepdims=True)
    return centred * lax.rsqrt(spread + NORM_EPSILON) * gain_vec + bias_vec


def softplus_of_minus(d):
    u = jnp.exp(-jnp.abs(d))
    s = u / (2.0 + u)
    q = s * s
    series = jnp.full_like(s, 1.0 / 15.0)
    for odd in (13, 11, 9, 7, 5, 3, 1):
        series = series * q + 1.0 / odd
    return jnp.maximum(-d, 0.0) + 2.0 * s * series


def minus_expm1(z):
    series = jnp.full_like(z, 1.0 / 40320.0)
    for factor in (5040.0, 720.0, 120.0, 24.0, 6.0, 2.0, 1.0):
        series = series * z + 1.0 / factor
    return jnp.where(z > -0.25, -z * series, 1.0 - jnp.exp(z))


def dot(a, b):
    return jnp.dot(a, b, preferred_element_type=F32)


def mega(
    stream_h, rec_h, gatein_h, taps_h, small_gates_h, large_gates_h, decay_h, extra_h,
    wout_h, gain1_h, bias1_h, index_h, weight_h, gate_w_h, up_w_h, down_w_h,
    shared_gate_h, shared_up_h, shared_down_h, gain2_h, bias2_h,
    out_ref,
    stream, rec, gatein, taps, small_gates, large_gates, decay, extra_raw,
    wout, gain1, bias1, index, weight, gate_w, up_w, down_w,
    shared_gate, shared_up, shared_down, gain2, bias2,
    extra, turned, rec_f, border, cum_p, cum_s, carry1, carry2, gelu_buf, branch,
    part, mixed_buf, normed, slot_buf, weight_buf,
    disp, arr1, disp2, arr2, moe_out, ret1, ret1p, ret2, acc,
    own_gate, own_up, own_down,
    load_sem, slot_sem, border_sem, weight_sem, carry_sem, mix_sem, disp_sem, ret_sem,
):
    sp = lax.axis_index("sp")
    tp = lax.axis_index("tp")
    zi = sp // PLANE
    pi = sp % PLANE
    xi = pi // 2
    core = sp % 2
    hosted = tp // 2
    mirror = 3 - tp
    mate = tp + 1 - 2 * (tp % 2)
    sibling = sp + 1 - 2 * core
    owner = core == hosted
    guest = core != hosted
    sends = []
    phase = Phases()
    phase("loads")

    def load(k, src, dst):
        copy = pltpu.make_async_copy(src, dst, load_sem.at[k])
        copy.start()
        return copy

    def remote(src, dst, sem, where, sp_to, tp_to, lands=None):
        copy = pltpu.make_async_remote_copy(
            src_ref=src,
            dst_ref=dst,
            send_sem=sem.at[(0, *where)],
            recv_sem=sem.at[(1, *(lands or where))],
            device_id={"sp": sp_to, "tp": tp_to},
            device_id_type=MESH,
        )
        return copy

    def send(*args, lands=None, when=None):
        copy = remote(*args, lands=lands)
        if when is None:
            copy.start()
        else:
            pl.when(when)(copy.start)
        sends.append((copy, when))

    def plane_peer(d):
        return zi * PLANE + (pi + d) % PLANE

    def z_peer(d):
        return ((zi + d) % PLANES) * PLANE + pi

    names = (
        (rec_h, rec), (small_gates_h, small_gates), (large_gates_h, large_gates), (taps_h, taps),
        (decay_h, decay), (extra_h, extra_raw), (gatein_h, gatein), (gate_w_h, own_gate),
        (up_w_h, own_up), (down_w_h, own_down), (wout_h, wout), (index_h, index),
        (weight_h, weight), (stream_h, stream), (gain1_h, gain1), (bias1_h, bias1),
        (shared_gate_h, shared_gate), (shared_up_h, shared_up), (shared_down_h, shared_down),
        (gain2_h, gain2), (bias2_h, bias2),
    )
    loads = [load(k, src, dst) for k, (src, dst) in enumerate(names)]
    owns = (own_gate, own_up, own_down)
    wholes = (gate_w, up_w, down_w)
    slot_loads = [
        pltpu.make_async_copy(src, dst.at[tp], slot_sem.at[m])
        for m, (src, dst) in enumerate(zip((gate_w_h, up_w_h, down_w_h), wholes))
    ]

    @pl.when(owner)
    def _():
        for copy in slot_loads:
            copy.start()

    barrier = pltpu.get_barrier_semaphore()

    def greet(sp_to, tp_to):
        pl.semaphore_signal(
            barrier, inc=1, device_id={"sp": sp_to, "tp": tp_to}, device_id_type=MESH
        )

    for d in range(1, PLANE):
        greet(plane_peer(d), tp)
    for d in range(1, PLANES):
        greet(z_peer(d), tp)
    for d in range(1, TPS):
        greet(sp, (tp + d) % TPS)
    greet((sp + 63) % 64, tp)
    for j in range(PLANE):
        greet(zi * PLANE + j, mirror)

    phase("wait_loads")
    for k in range(6):
        loads[k].wait()
    length = rec.shape[0]
    phase("prepare")
    for g in range(2):
        rec_f[HEAD_ROWS:, 256 * g : 256 * g + 256] = rec[:, g, :].astype(F32)
        extra[:, 256 * g : 256 * g + 256] = extra_raw[:, g, :]
    row_i = lax.broadcasted_iota(jnp.int32, (64, 128), 0)
    col_i = lax.broadcasted_iota(jnp.int32, (64, 128), 1)
    put_low = (row_i == col_i).astype(BF16)
    put_high = (row_i + 64 == col_i).astype(BF16)
    blocks = []
    for which in range(2):
        maps = []
        for pair in range(2):
            low = dot(small_gates[which, 2 * pair], put_low)
            high = dot(small_gates[which, 2 * pair + 1], put_high)
            maps.append(jnp.concatenate([low, high], axis=0).astype(BF16))
        for head in range(2):
            maps.append(large_gates[which, head])
        blocks.append(maps)
    rate = -8.0 * softplus_of_minus(decay[...])
    tap_f = taps[...].astype(F32)

    def tap(k, b):
        return tap_f[k, b // 2 : b // 2 + 1, 128 * (b % 2) : 128 * (b % 2) + 128]

    def scanned(first, count):
        for b in range(4):
            lanes = slice(128 * b, 128 * b + 128)
            conv = tap(0, b) * rec_f[first + HEAD_ROWS - 3 : first + HEAD_ROWS - 3 + count, lanes]
            for k in range(1, 4):
                at = first + HEAD_ROWS - 3 + k
                conv = conv + tap(k, b) * rec_f[at : at + count, lanes]
            conv = conv.astype(BF16)
            recur_gate = jax.nn.sigmoid(dot(conv, blocks[0][b]))
            input_gate = jax.nn.sigmoid(dot(conv, blocks[1][b]))
            log_decay = recur_gate * rate[b // 2 : b // 2 + 1, 128 * (b % 2) : 128 * (b % 2) + 128] + extra[first : first + count, lanes]
            p = jnp.exp(log_decay)
            s = jnp.sqrt(minus_expm1(2.0 * log_decay)) * input_gate * conv.astype(F32)
            p = p.reshape(count // 8, 8, 128)
            s = s.reshape(count // 8, 8, 128)
            row = lax.broadcasted_iota(jnp.int32, (count // 8, 8, 128), 1)
            for by in (1, 2, 4):
                p_prev = pltpu.roll(p, by, 1)
                s_prev = pltpu.roll(s, by, 1)
                s = jnp.where(row >= by, p * s_prev + s, s)
                p = jnp.where(row >= by, p * p_prev, p)
            p_in = jnp.ones((1, 128), F32)
            s_in = jnp.zeros((1, 128), F32)
            for t in range(count // 8):
                s_t = s[t] + p[t] * s_in
                p_t = p[t] * p_in
                cum_s[first + 8 * t : first + 8 * t + 8, lanes] = s_t
                cum_p[first + 8 * t : first + 8 * t + 8, lanes] = p_t
                s_in = s_t[7:8]
                p_in = p_t[7:8]

    phase("scan_tail")
    scanned(HEAD_ROWS, length - HEAD_ROWS)
    phase("barrier")

    pl.semaphore_wait(barrier, 7 + 7 + 3 + 1 + 8)
    send(rec.at[length - HEAD_ROWS :], border, border_sem, (), (sp + 1) % 64, tp)

    far = 3 - mate
    FROM_MATE, FROM_MIRROR, FROM_FAR, OWN, MATE, MIRROR, FAR = range(7)
    slots = {
        FROM_MATE: mate, FROM_MIRROR: mirror, FROM_FAR: far,
        OWN: tp, MATE: mate, MIRROR: mirror, FAR: far,
    }

    def part_out(src, m, at, kind, sp_to, tp_to, when):
        send(src, wholes[m].at[at], weight_sem, (kind, m), sp_to, tp_to, when=when)

    def part_in(m, kind):
        got = wholes[m].at[slots[kind]]
        remote(got, got, weight_sem, (kind, m), sp, tp).wait_recv()

    def pass_on(m, kind, to_sibling):
        got = wholes[m].at[slots[kind]]
        part_out(got, m, slots[kind], to_sibling, sibling, tp, owner)

    phase("send_gate")
    for k in (7, 8, 9):
        loads[k].wait()
    for m in (0, 1):
        part_out(owns[m], m, tp, FROM_MATE, sp, mate, owner)
        part_out(owns[m], m, tp, FROM_MIRROR, sp, mirror, guest)
    for m in (0, 1, 2):
        part_out(owns[m], m, tp, OWN, sibling, tp, owner)

    phase("border")
    remote(rec.at[length - HEAD_ROWS :], border, border_sem, (), sp, tp).wait_recv()
    phase("scan_head")
    for g in range(2):
        border_f = border[:, g, :].astype(F32)
        rec_f[0:HEAD_ROWS, 256 * g : 256 * g + 256] = jnp.where(
            sp > 0, border_f, jnp.zeros_like(border_f)
        )
    scanned(0, HEAD_ROWS)

    head_p = cum_p[HEAD_ROWS - 1 : HEAD_ROWS, :]
    head_s = cum_s[HEAD_ROWS - 1 : HEAD_ROWS, :]
    tail_p = cum_p[length - 1 : length, :]
    tail_s = cum_s[length - 1 : length, :]
    total_p = head_p * tail_p
    total_s = tail_p * head_s + tail_s
    mine1 = carry1.at[pi]
    for b in range(4):
        mine1[0, b : b + 1, :] = total_p[:, 128 * b : 128 * b + 128]
        mine1[1, b : b + 1, :] = total_s[:, 128 * b : 128 * b + 128]
    for d in FAR_FIRST:
        send(mine1, mine1, carry_sem, (0, d), plane_peer(d), tp)

    phase("slots")
    for k in (6, 11, 12):
        loads[k].wait()
    own_rows = pl.ds(pl.multiple_of(tp * 32, 32), 32)
    unused = jnp.zeros((4, 128), F32)
    turned[0] = jnp.concatenate([index[...].astype(F32), unused], axis=0).T
    turned[1] = jnp.concatenate([weight[...], unused], axis=0).T
    ids = turned[0, own_rows, :].astype(jnp.int32)
    factors = turned[1, own_rows, :]
    slot = lax.broadcasted_iota(jnp.int32, (32, 128), 1)
    named = jnp.zeros((32, 128), F32)
    scaled = jnp.zeros((32, 128), F32)
    for k in range(4):
        hit = ids[:, k : k + 1] == slot // 2
        named = named + jnp.where(hit, 1.0, 0.0)
        scaled = scaled + jnp.where(hit, factors[:, k : k + 1], 0.0)
    below = lax.broadcasted_iota(jnp.int32, (32, 32), 0) > lax.broadcasted_iota(
        jnp.int32, (32, 32), 1
    )
    earlier = dot(below.astype(BF16), named.astype(BF16))
    right_slot = jnp.abs(earlier - (slot % 2).astype(F32)) < 0.5
    slot_buf[...] = jnp.where(right_slot, named, 0.0).T.astype(BF16)
    scaled = jnp.where(right_slot, scaled, 0.0)
    high = scaled.astype(BF16)
    weight_buf[0] = high
    weight_buf[1] = (scaled - high.astype(F32)).astype(BF16)
    for g in range(2):
        gelu_buf[:, 256 * g : 256 * g + 256] = jax.nn.gelu(gatein[:, g, :].astype(F32))
    phase("carry1")

    for d in FAR_FIRST:
        got = carry1.at[(pi + PLANE - d) % PLANE]
        remote(got, got, carry_sem, (0, d), sp, tp).wait_recv()
    one = jnp.ones((4, 128), F32)
    nought = jnp.zeros((4, 128), F32)
    all_p, all_s, in_p, in_s = one, nought, one, nought
    for j in range(PLANE):
        p_j, s_j = carry1[j, 0], carry1[j, 1]
        all_p, all_s = all_p * p_j, p_j * all_s + s_j
        in_p = jnp.where(j < pi, in_p * p_j, in_p)
        in_s = jnp.where(j < pi, p_j * in_s + s_j, in_s)
    mine2 = carry2.at[zi]
    mine2[0] = all_p
    mine2[1] = all_s
    for d in FAR_FIRST:
        send(mine2, mine2, carry_sem, (1, d), z_peer(d), tp)
    phase("carry2")
    for d in FAR_FIRST:
        got = carry2.at[(zi + PLANES - d) % PLANES]
        remote(got, got, carry_sem, (1, d), sp, tp).wait_recv()
    phase("fixup")
    planes_s = nought
    for k in range(PLANES):
        planes_s = jnp.where(k < zi, carry2[k, 0] * planes_s + carry2[k, 1], planes_s)
    carry_in = in_p * planes_s + in_s
    carry_row = jnp.concatenate([carry_in[b : b + 1] for b in range(4)], axis=1)
    carry_tail = head_s + head_p * carry_row
    states = cum_s[:HEAD_ROWS] + cum_p[:HEAD_ROWS] * carry_row
    branch[:HEAD_ROWS, :] = (gelu_buf[:HEAD_ROWS] * states).astype(BF16)
    states = cum_s[HEAD_ROWS:] + cum_p[HEAD_ROWS:] * carry_tail
    branch[HEAD_ROWS:, :] = (gelu_buf[HEAD_ROWS:] * states).astype(BF16)

    phase("out_proj")
    loads[10].wait()
    for c in range(4):
        cols = slice(512 * c, 512 * c + 512)
        value = dot(branch[...], wout[:, cols]).astype(BF16)
        part[:, :, cols] = value.reshape(TPS, 32, 512)
        for d in (2, 1, 3):
            to = (tp + d) % TPS
            send(part.at[to, :, cols], mixed_buf.at[tp, :, cols], mix_sem, (c, d), sp, to)
    phase("gate_arrive")
    for m in (0, 1):

        @pl.when(owner)
        def _():
            part_in(m, FROM_MIRROR)

        mirrored = wholes[m].at[mirror]
        part_out(mirrored, m, mirror, FROM_FAR, sp, mate, owner)
        pass_on(m, FROM_MIRROR, MIRROR)
    part_out(own_down, 2, tp, FROM_MATE, sp, mate, owner)
    part_out(own_down, 2, tp, FROM_MIRROR, sp, mirror, guest)
    for m in (0, 1):

        @pl.when(owner)
        def _():
            part_in(m, FROM_MATE)

        pass_on(m, FROM_MATE, MATE)
    phase("mix_arrive")
    for k in (13, 14, 15):
        loads[k].wait()
    for c in range(4):
        cols = slice(512 * c, 512 * c + 512)
        for d in (2, 1, 3):
            came = (tp + TPS - d) % TPS
            got = mixed_buf.at[came, :, cols]
            remote(got, got, mix_sem, (c, d), sp, tp).wait_recv()
    phase("norm1")
    mixed = part[tp].astype(F32)
    for d in (1, 2, 3):
        mixed = mixed + mixed_buf[(tp + d) % TPS].astype(F32)
    normed[...] = layer_norm(
        RESIDUAL_SCALE * stream[...].astype(F32) + mixed, gain1[...], bias1[...]
    ).astype(BF16)

    width = 2048 // CHUNKS

    def exchange(src, dst, sem, hop, c, me, peer):
        cols = slice(width * c, width * c + width)
        size = src.shape[0]
        for d in FAR_FIRST:
            to = (me + d) % size
            send(src.at[to, :, cols], dst.at[me, :, cols], sem, (hop, c, d), peer(d), tp)
        dst[me, :, cols] = src[me, :, cols]

    def arrived(dst, sem, hop, c, me):
        cols = slice(width * c, width * c + width)
        size = dst.shape[0]
        for d in FAR_FIRST:
            got = dst.at[(me + size - d) % size, :, cols]
            remote(got, got, sem, (hop, c, d), sp, tp).wait_recv()

    def swapped(src, c):
        cols = slice(width * c, width * c + width)
        to_row = lax.broadcasted_iota(jnp.int32, (128, 128), 0)
        from_row = lax.broadcasted_iota(jnp.int32, (128, 128), 1)
        outer, inner, pair = to_row // 16, (to_row // 2) % 8, to_row % 2
        pick = (from_row == inner * 16 + outer * 2 + pair).astype(BF16)
        rows = src[:, :, cols].reshape(128, width)
        return dot(pick, rows).astype(BF16).reshape(8, 16, width)

    phase("dispatch")
    for c in range(CHUNKS):
        cols = slice(width * c, width * c + width)
        value = dot(slot_buf[...], normed[:, cols]).astype(BF16)
        disp[:, :, cols] = value.reshape(8, 16, width)
        exchange(disp, arr1, disp_sem, 0, c, zi, z_peer)
    phase("shared")
    for k in (16, 17, 18, 19, 20):
        loads[k].wait()
    rows = normed[...]
    hidden = jax.nn.silu(dot(rows, shared_gate[...])) * dot(rows, shared_up[...])
    acc[...] = RESIDUAL_SCALE * rows.astype(F32) + dot(hidden.astype(BF16), shared_down[...])

    phase("down_from_mirror")

    @pl.when(owner)
    def _():
        part_in(2, FROM_MIRROR)

    part_out(down_w.at[mirror], 2, mirror, FROM_FAR, sp, mate, owner)
    pass_on(2, FROM_MIRROR, MIRROR)

    for c in range(CHUNKS):
        cols = slice(width * c, width * c + width)
        phase(f"disp_z_{c}")
        arrived(arr1, disp_sem, 0, c, zi)
        phase(f"disp_swap_{c}")
        disp2[:, :, cols] = swapped(arr1, c)
        for dx in (2, 1, 3, 0):
            x_to = (xi + dx) % 4
            for other in (1, 0):
                expert = hosted + other * (1 - 2 * hosted)
                send(
                    disp2.at[x_to * 2 + expert, :, cols],
                    arr2.at[pi, :, cols],
                    disp_sem,
                    (1, c, dx * 2 + other),
                    zi * PLANE + x_to * 2 + hosted,
                    mirror if other else tp,
                    lands=(1, c, dx * 2 + core),
                    when=guest if dx == 0 and other == 0 else None,
                )

        @pl.when(owner)
        def _():
            arr2[pi, :, cols] = disp2[pi, :, cols]

    phase("far_gate_up")
    for m in (0, 1):

        @pl.when(owner)
        def _():
            part_in(m, FROM_FAR)

        pass_on(m, FROM_FAR, FAR)
    for c in range(CHUNKS):
        cols = slice(width * c, width * c + width)
        phase(f"disp_p_{c}")
        for dx in (2, 1, 3, 0):
            for source_core in (0, 1):
                got = arr2.at[((xi + 4 - dx) % 4) * 2 + source_core, :, cols]
                copy = remote(got, got, disp_sem, (1, c, dx * 2 + source_core), sp, tp)
                if dx == 0:
                    pl.when(jnp.logical_or(guest, core != source_core))(copy.wait_recv)
                else:
                    copy.wait_recv()
    picked = arr2[...].reshape(128, 2048)
    phase("down_from_mate")

    @pl.when(owner)
    def _():
        part_in(2, FROM_MATE)

    pass_on(2, FROM_MATE, MATE)
    phase("gate_up_guest")

    @pl.when(owner)
    def _():
        for copy in slot_loads:
            copy.wait()

    @pl.when(guest)
    def _():
        for m in (0, 1):
            for kind in (OWN, MATE, MIRROR, FAR):
                part_in(m, kind)

    phase("gated")
    gated = [dot(picked, gate_w[k]) for k in range(TPS)]
    phase("lifted")
    lifted = [dot(picked, up_w[k]) for k in range(TPS)]
    hidden = jnp.concatenate(
        [(jax.nn.silu(g) * u).astype(BF16) for g, u in zip(gated, lifted)], axis=1
    )
    phase("down_arrive")

    @pl.when(owner)
    def _():
        part_in(2, FROM_FAR)

    pass_on(2, FROM_FAR, FAR)
    phase("down_guest")

    @pl.when(guest)
    def _():
        for kind in (OWN, MATE, MIRROR, FAR):
            part_in(2, kind)

    for c in range(CHUNKS):
        cols = slice(width * c, width * c + width)
        phase(f"down_{c}")
        value = dot(hidden, down_w[:, :, cols].reshape(512, width)).astype(BF16)
        moe_out[:, :, cols] = value.reshape(8, 16, width)
        home = jnp.where(owner, tp, mirror)
        foreign = jnp.where(owner, 0, 1)
        for dx in (2, 1, 3, 0):
            for target_core in (0, 1):
                j = ((xi + dx) % 4) * 2 + target_core
                send(
                    moe_out.at[j, :, cols],
                    ret1.at[xi * 2 + hosted, :, cols],
                    ret_sem,
                    (0, c, dx * 2 + target_core),
                    zi * PLANE + j,
                    home,
                    lands=(0, c, dx * 2 + foreign),
                    when=jnp.logical_or(guest, core != target_core) if dx == 0 else None,
                )

        @pl.when(owner)
        def _():
            ret1[pi, :, cols] = moe_out[pi, :, cols]

    for c in range(CHUNKS):
        cols = slice(width * c, width * c + width)
        phase(f"ret_p_{c}")
        for dx in (2, 1, 3, 0):
            for other in (1, 0):
                expert = hosted + other * (1 - 2 * hosted)
                got = ret1.at[((xi + 4 - dx) % 4) * 2 + expert, :, cols]
                copy = remote(got, got, ret_sem, (0, c, dx * 2 + other), sp, tp)
                if dx == 0 and other == 0:
                    pl.when(guest)(copy.wait_recv)
                else:
                    copy.wait_recv()
        phase(f"ret_swap_{c}")
        ret1p[:, :, cols] = swapped(ret1, c)
        exchange(ret1p, ret2, ret_sem, 1, c, zi, z_peer)
    for c in range(CHUNKS):
        cols = slice(width * c, width * c + width)
        phase(f"ret_z_{c}")
        arrived(ret2, ret_sem, 1, c, zi)
        phase(f"combine_{c}")
        back = ret2[:, :, cols].reshape(128, width)
        acc[:, cols] = acc[:, cols] + dot(weight_buf[0], back) + dot(weight_buf[1], back)
    phase("norm2")
    out_ref[...] = layer_norm(acc[...], gain2[...], bias2[...]).astype(BF16)
    phase("drain")
    for copy, when in sends:
        if when is None:
            copy.wait_send()
        else:
            pl.when(when)(copy.wait_send)
    phase()


def shards(
    stream, recurrence_input, output_gate_input, convolution_taps, first_group_gates,
    second_group_gates, channel_decay, position_log_extra, recurrence_output_weight,
    first_norm_gain, first_norm_bias, routed_expert_index, routed_expert_weight,
    routed_gate_weight, routed_up_weight, routed_down_weight, shared_gate_weight,
    shared_up_weight, shared_down_weight, second_norm_gain, second_norm_bias,
):
    operands = (
        stream,
        recurrence_input,
        output_gate_input,
        convolution_taps,
        first_group_gates,
        second_group_gates,
        channel_decay,
        position_log_extra,
        recurrence_output_weight.reshape(512, 2048),
        first_norm_gain.reshape(1, 2048),
        first_norm_bias.reshape(1, 2048),
        routed_expert_index.T,
        routed_expert_weight.T,
        routed_gate_weight.reshape(2048, 128),
        routed_up_weight.reshape(2048, 128),
        routed_down_weight.reshape(128, 2048),
        shared_gate_weight,
        shared_up_weight,
        shared_down_weight,
        second_norm_gain.reshape(1, 2048),
        second_norm_bias.reshape(1, 2048),
    )
    gathered = {13: (4, 2048, 128), 14: (4, 2048, 128), 15: (4, 128, 2048)}
    held = [
        pltpu.VMEM(gathered.get(k, operand.shape), operand.dtype)
        for k, operand in enumerate(operands)
    ]
    wide = pltpu.VMEM((8, 16, 2048), BF16)
    return pl.pallas_call(
        mega,
        out_shape=jax.ShapeDtypeStruct((32, 2048), BF16),
        in_specs=[pl.BlockSpec(memory_space=pl.ANY)] * len(operands),
        out_specs=pl.BlockSpec(memory_space=pltpu.VMEM),
        scratch_shapes=[
            *held,
            pltpu.VMEM((128, 512), F32),
            pltpu.VMEM((2, 128, 8), F32),
            pltpu.VMEM((128 + HEAD_ROWS, 512), F32),
            pltpu.VMEM((HEAD_ROWS, 2, 256), BF16),
            pltpu.VMEM((128, 512), F32),
            pltpu.VMEM((128, 512), F32),
            pltpu.VMEM((PLANE, 2, 4, 128), F32),
            pltpu.VMEM((PLANES, 2, 4, 128), F32),
            pltpu.VMEM((128, 512), F32),
            pltpu.VMEM((128, 512), BF16),
            pltpu.VMEM((TPS, 32, 2048), BF16),
            pltpu.VMEM((TPS, 32, 2048), BF16),
            pltpu.VMEM((32, 2048), BF16),
            pltpu.VMEM((128, 32), BF16),
            pltpu.VMEM((2, 32, 128), BF16),
            wide, wide, wide, wide, wide, wide, wide, wide,
            pltpu.VMEM((32, 2048), F32),
            pltpu.VMEM((2048, 128), BF16),
            pltpu.VMEM((2048, 128), BF16),
            pltpu.VMEM((128, 2048), BF16),
            pltpu.SemaphoreType.DMA((len(operands),)),
            pltpu.SemaphoreType.DMA((3,)),
            pltpu.SemaphoreType.DMA((2,)),
            pltpu.SemaphoreType.DMA((2, 7, 3)),
            pltpu.SemaphoreType.DMA((2, 2, 8)),
            pltpu.SemaphoreType.DMA((2, 4, 4)),
            pltpu.SemaphoreType.DMA((2, 2, CHUNKS, 8)),
            pltpu.SemaphoreType.DMA((2, 2, CHUNKS, 8)),
        ],
        compiler_params=pltpu.CompilerParams(
            collective_id=0, has_side_effects=True, vmem_limit_bytes=56 * 2**20
        ),
        name="mega",
    )(*operands)


def solution(mesh):
    in_specs = (
        P(("sp", "tp"), None),
        P("sp", None, "tp"),
        P("sp", None, "tp"),
        P(None, None, "tp"),
        P(None, "tp", None, None),
        P(None, "tp", None, None),
        P(None, "tp"),
        P("sp", None, "tp"),
        P(None, "tp", None),
        P(),
        P(),
        P("sp", None),
        P("sp", None),
        P("sp", None, "tp"),
        P("sp", None, "tp"),
        P("sp", "tp", None),
        P(),
        P(),
        P(),
        P(),
        P(),
    )
    out_specs = P(("sp", "tp"), None)
    return jax.shard_map(shards, mesh=mesh, in_specs=in_specs, out_specs=out_specs, check_vma=False)
```

```python
import jax
import jax.numpy as jnp
from jax import lax
from jax.experimental import pallas as pl
from jax.experimental.pallas import tpu as pltpu
from jax.sharding import PartitionSpec as P

RESIDUAL_SCALE = 8.0**0.25
NORM_EPSILON = 1e-05
MESH = pl.DeviceIdType.MESH
F32 = jnp.float32
BF16 = jnp.bfloat16

PLANE = 8
PLANES = 8
TPS = 4
HEAD_ROWS = 16
CHUNKS = 4
FAR_FIRST = (4, 3, 5, 2, 6, 1, 7)


class Phases:
    def __init__(self):
        self.scope = None

    def __call__(self, name=None):
        if self.scope is not None:
            self.scope.__exit__(None, None, None)
        self.scope = None
        if name is not None:
            self.scope = jax.named_scope(name)
            self.scope.__enter__()


def layer_norm(values, gain_vec, bias_vec):
    row_mean = jnp.mean(values, axis=-1, keepdims=True)
    centred = values - row_mean
    spread = jnp.mean(jnp.square(centred), axis=-1, keepdims=True)
    return centred * lax.rsqrt(spread + NORM_EPSILON) * gain_vec + bias_vec


def softplus_of_minus(d):
    u = jnp.exp(-jnp.abs(d))
    s = u / (2.0 + u)
    q = s * s
    series = jnp.full_like(s, 1.0 / 15.0)
    for odd in (13, 11, 9, 7, 5, 3, 1):
        series = series * q + 1.0 / odd
    return jnp.maximum(-d, 0.0) + 2.0 * s * series


def minus_expm1(z):
    series = jnp.full_like(z, 1.0 / 40320.0)
    for factor in (5040.0, 720.0, 120.0, 24.0, 6.0, 2.0, 1.0):
        series = series * z + 1.0 / factor
    return jnp.where(z > -0.25, -z * series, 1.0 - jnp.exp(z))


def dot(a, b):
    return jnp.dot(a, b, preferred_element_type=F32)


def mega(
    stream_h, rec_h, gatein_h, taps_h, small_gates_h, large_gates_h, decay_h, extra_h,
    wout_h, gain1_h, bias1_h, index_h, weight_h, gate_w_h, up_w_h, down_w_h,
    shared_gate_h, shared_up_h, shared_down_h, gain2_h, bias2_h,
    out_ref,
    stream, rec, gatein, taps, small_gates, large_gates, decay, extra_raw,
    wout, gain1, bias1, index, weight, own_gate, own_up, own_down,
    shared_gate, shared_up, shared_down, gain2, bias2,
    gate_up, down_w,
    extra, turned, rec_f, border, cum_p, cum_s, carry1, carry2, gelu_buf, branch,
    part, mixed_buf, normed, slot_buf, weight_buf,
    disp, arr1, disp2, arr2, moe_out, ret1, ret1p, ret2, acc,
    load_sem, slot_sem, border_sem, part_sem, guest_sem, part_out_sem, carry_sem, mix_sem,
    z_sem, p_sem, hop_out_sem,
):
    sp = lax.axis_index("sp")
    tp = lax.axis_index("tp")
    zi = sp // PLANE
    pi = sp % PLANE
    xi = pi // 2
    core = sp % 2
    hosted = tp // 2
    mirror = 3 - tp
    mate = tp + 1 - 2 * (tp % 2)
    far = 3 - mate
    sibling = sp + 1 - 2 * core
    owner = core == hosted
    guest = core != hosted
    phase = Phases()
    phase("loads")

    def remote(src, dst, send_sem, recv_sem, sp_to, tp_to):
        return pltpu.make_async_remote_copy(
            src_ref=src,
            dst_ref=dst,
            send_sem=send_sem,
            recv_sem=recv_sem,
            device_id={"sp": sp_to, "tp": tp_to},
            device_id_type=MESH,
        )

    def send(*args, when=None):
        copy = remote(*args)
        if when is None:
            copy.start()
        else:
            pl.when(when)(copy.start)

    def came(ref, sem):
        remote(ref, ref, sem, sem, sp, tp).wait_recv()

    def left(ref, sem):
        remote(ref, ref, sem, sem, sp, tp).wait_send()

    def plane_peer(d):
        return zi * PLANE + (pi + d) % PLANE

    def z_peer(d):
        return ((zi + d) % PLANES) * PLANE + pi

    barrier = pltpu.get_barrier_semaphore()

    def greet(sp_to, tp_to):
        pl.semaphore_signal(
            barrier, inc=1, device_id={"sp": sp_to, "tp": tp_to}, device_id_type=MESH
        )

    for d in FAR_FIRST:
        greet(z_peer(d), tp)
    for d in FAR_FIRST:
        greet(plane_peer(d), tp)
    for d in range(1, TPS):
        greet(sp, (tp + d) % TPS)
    greet((sp + 63) % 64, tp)
    for j in range(PLANE):
        greet(zi * PLANE + j, mirror)

    names = (
        (rec_h, rec), (small_gates_h, small_gates), (large_gates_h, large_gates), (taps_h, taps),
        (decay_h, decay), (extra_h, extra_raw), (gatein_h, gatein), (gate_w_h, own_gate),
        (up_w_h, own_up), (down_w_h, own_down), (wout_h, wout), (index_h, index),
        (weight_h, weight), (stream_h, stream), (gain1_h, gain1), (bias1_h, bias1),
        (shared_gate_h, shared_gate), (shared_up_h, shared_up), (shared_down_h, shared_down),
        (gain2_h, gain2), (bias2_h, bias2),
    )
    loads = []
    for k, (src, dst) in enumerate(names):
        loads.append(pltpu.make_async_copy(src, dst, load_sem.at[k]))
        loads[-1].start()
    wholes = (gate_up.at[0], gate_up.at[1], down_w)
    owns = (own_gate, own_up, own_down)
    slot_loads = [
        pltpu.make_async_copy(src, dst.at[tp], slot_sem.at[m])
        for m, (src, dst) in enumerate(zip((gate_w_h, up_w_h, down_w_h), wholes))
    ]

    @pl.when(owner)
    def _():
        for copy in slot_loads:
            copy.start()

    phase("wait_loads")
    length = rec.shape[0]
    loads[0].wait()
    phase("barrier")
    pl.semaphore_wait(barrier, 7 + 7 + 3 + 1 + 8)
    phase("send_gate")
    border_out = rec.at[length - HEAD_ROWS :]
    send(border_out, border, border_sem.at[0], border_sem.at[1], (sp + 1) % 64, tp)

    FROM_MATE, FROM_MIRROR, FROM_FAR = range(3)
    origin = {FROM_MATE: mate, FROM_MIRROR: mirror, FROM_FAR: far}
    TO_SIBLING, ACROSS = range(2)

    def piece_of(ref, k, lead=()):
        if k < 4:
            return ref.at[(*lead, slice(1024 * (k % 2), 1024 * (k % 2) + 1024))]
        return ref.at[(*lead, slice(None), slice(512 * (k - 4), 512 * (k - 4) + 512))]

    def buffer_of(k):
        return k // 2 if k < 4 else 2

    def held_piece(k, at):
        return piece_of(wholes[buffer_of(k)], k, (at,))

    def across(src, k, at, kind, tp_to, when):
        out = part_out_sem.at[ACROSS, int(k >= 4)]
        send(src, held_piece(k, at), out, part_sem.at[kind, k], sp, tp_to, when=when)

    def to_sibling(src, k, at):
        out = part_out_sem.at[TO_SIBLING, int(k >= 4)]
        lands = guest_sem.at[max(k - 3, 0)]
        send(src, held_piece(k, at), out, lands, sibling, tp, when=owner)

    def own_out(k):
        src = piece_of(owns[buffer_of(k)], k)
        across(src, k, tp, FROM_MATE, mate, owner)

    def own_mirror(k):
        src = piece_of(owns[buffer_of(k)], k)
        across(src, k, tp, FROM_MIRROR, mirror, guest)

    def relay(k, kind):
        got = held_piece(k, origin[kind])

        @pl.when(owner)
        def _():
            came(got, part_sem.at[kind, k])

        if kind == FROM_MIRROR:
            across(got, k, origin[kind], FROM_FAR, mate, owner)
        to_sibling(got, k, origin[kind])

    for k in (7, 8):
        loads[k].wait()
    for k in (0, 1, 2):
        own_out(k)
        own_mirror(k)

    phase("prepare")
    for k in range(1, 6):
        loads[k].wait()
    for g in range(2):
        rec_f[HEAD_ROWS:, 256 * g : 256 * g + 256] = rec[:, g, :].astype(F32)
        extra[:, 256 * g : 256 * g + 256] = extra_raw[:, g, :]
    row_i = lax.broadcasted_iota(jnp.int32, (64, 128), 0)
    col_i = lax.broadcasted_iota(jnp.int32, (64, 128), 1)
    put_low = (row_i == col_i).astype(BF16)
    put_high = (row_i + 64 == col_i).astype(BF16)
    blocks = []
    for which in range(2):
        maps = []
        for pair in range(2):
            low = dot(small_gates[which, 2 * pair], put_low)
            high = dot(small_gates[which, 2 * pair + 1], put_high)
            maps.append(jnp.concatenate([low, high], axis=0).astype(BF16))
        for head in range(2):
            maps.append(large_gates[which, head])
        blocks.append(maps)
    rate = -8.0 * softplus_of_minus(decay[...])
    tap_f = taps[...].astype(F32)

    def tap(k, b):
        return tap_f[k, b // 2 : b // 2 + 1, 128 * (b % 2) : 128 * (b % 2) + 128]

    def scanned(first, count):
        for b in range(4):
            lanes = slice(128 * b, 128 * b + 128)
            conv = tap(0, b) * rec_f[first + HEAD_ROWS - 3 : first + HEAD_ROWS - 3 + count, lanes]
            for k in range(1, 4):
                at = first + HEAD_ROWS - 3 + k
                conv = conv + tap(k, b) * rec_f[at : at + count, lanes]
            conv = conv.astype(BF16)
            recur_gate = jax.nn.sigmoid(dot(conv, blocks[0][b]))
            input_gate = jax.nn.sigmoid(dot(conv, blocks[1][b]))
            log_decay = recur_gate * rate[b // 2 : b // 2 + 1, 128 * (b % 2) : 128 * (b % 2) + 128] + extra[first : first + count, lanes]
            p = jnp.exp(log_decay)
            s = jnp.sqrt(minus_expm1(2.0 * log_decay)) * input_gate * conv.astype(F32)
            p = p.reshape(count // 8, 8, 128)
            s = s.reshape(count // 8, 8, 128)
            row = lax.broadcasted_iota(jnp.int32, (count // 8, 8, 128), 1)
            for by in (1, 2, 4):
                p_prev = pltpu.roll(p, by, 1)
                s_prev = pltpu.roll(s, by, 1)
                s = jnp.where(row >= by, p * s_prev + s, s)
                p = jnp.where(row >= by, p * p_prev, p)
            p_in = jnp.ones((1, 128), F32)
            s_in = jnp.zeros((1, 128), F32)
            for t in range(count // 8):
                s_t = s[t] + p[t] * s_in
                p_t = p[t] * p_in
                cum_s[first + 8 * t : first + 8 * t + 8, lanes] = s_t
                cum_p[first + 8 * t : first + 8 * t + 8, lanes] = p_t
                s_in = s_t[7:8]
                p_in = p_t[7:8]

    phase("scan_tail")
    scanned(HEAD_ROWS, length - HEAD_ROWS)
    loads[9].wait()
    for k in range(8):
        to_sibling(piece_of(owns[buffer_of(k)], k), k, tp)
    phase("border")
    came(border, border_sem.at[1])
    phase("scan_head")
    for g in range(2):
        border_f = border[:, g, :].astype(F32)
        rec_f[0:HEAD_ROWS, 256 * g : 256 * g + 256] = jnp.where(
            sp > 0, border_f, jnp.zeros_like(border_f)
        )
    scanned(0, HEAD_ROWS)

    head_p = cum_p[HEAD_ROWS - 1 : HEAD_ROWS, :]
    head_s = cum_s[HEAD_ROWS - 1 : HEAD_ROWS, :]
    tail_p = cum_p[length - 1 : length, :]
    tail_s = cum_s[length - 1 : length, :]
    total_p = head_p * tail_p
    total_s = tail_p * head_s + tail_s
    mine1 = carry1.at[pi]
    for b in range(4):
        mine1[0, b : b + 1, :] = total_p[:, 128 * b : 128 * b + 128]
        mine1[1, b : b + 1, :] = total_s[:, 128 * b : 128 * b + 128]
    for d in FAR_FIRST:
        send(mine1, mine1, carry_sem.at[0, 0], carry_sem.at[1, 0], plane_peer(d), tp)

    phase("slots")
    for k in (6, 11, 12):
        loads[k].wait()
    own_rows = pl.ds(pl.multiple_of(tp * 32, 32), 32)
    unused = jnp.zeros((4, 128), F32)
    turned[0] = jnp.concatenate([index[...].astype(F32), unused], axis=0).T
    turned[1] = jnp.concatenate([weight[...], unused], axis=0).T
    ids = turned[0, own_rows, :].astype(jnp.int32)
    factors = turned[1, own_rows, :]
    slot = lax.broadcasted_iota(jnp.int32, (32, 128), 1)
    named = jnp.zeros((32, 128), F32)
    scaled = jnp.zeros((32, 128), F32)
    for k in range(4):
        hit = ids[:, k : k + 1] == slot // 2
        named = named + jnp.where(hit, 1.0, 0.0)
        scaled = scaled + jnp.where(hit, factors[:, k : k + 1], 0.0)
    below = lax.broadcasted_iota(jnp.int32, (32, 32), 0) > lax.broadcasted_iota(
        jnp.int32, (32, 32), 1
    )
    earlier = dot(below.astype(BF16), named.astype(BF16))
    right_slot = jnp.abs(earlier - (slot % 2).astype(F32)) < 0.5
    slot_buf[...] = jnp.where(right_slot, named, 0.0).T.astype(BF16)
    scaled = jnp.where(right_slot, scaled, 0.0)
    high = scaled.astype(BF16)
    weight_buf[0] = high
    weight_buf[1] = (scaled - high.astype(F32)).astype(BF16)
    for g in range(2):
        gelu_buf[:, 256 * g : 256 * g + 256] = jax.nn.gelu(gatein[:, g, :].astype(F32))
    phase("carry1")

    came(carry1.at[0:7], carry_sem.at[1, 0])
    one = jnp.ones((4, 128), F32)
    nought = jnp.zeros((4, 128), F32)
    all_p, all_s, in_p, in_s = one, nought, one, nought
    for j in range(PLANE):
        p_j, s_j = carry1[j, 0], carry1[j, 1]
        all_p, all_s = all_p * p_j, p_j * all_s + s_j
        in_p = jnp.where(j < pi, in_p * p_j, in_p)
        in_s = jnp.where(j < pi, p_j * in_s + s_j, in_s)
    mine2 = carry2.at[zi]
    mine2[0] = all_p
    mine2[1] = all_s
    for d in FAR_FIRST:
        send(mine2, mine2, carry_sem.at[0, 1], carry_sem.at[1, 1], z_peer(d), tp)
    phase("carry2")
    came(carry2.at[0:7], carry_sem.at[1, 1])
    phase("fixup")
    planes_s = nought
    for k in range(PLANES):
        planes_s = jnp.where(k < zi, carry2[k, 0] * planes_s + carry2[k, 1], planes_s)
    carry_in = in_p * planes_s + in_s
    carry_row = jnp.concatenate([carry_in[b : b + 1] for b in range(4)], axis=1)
    carry_tail = head_s + head_p * carry_row
    states = cum_s[:HEAD_ROWS] + cum_p[:HEAD_ROWS] * carry_row
    branch[:HEAD_ROWS, :] = (gelu_buf[:HEAD_ROWS] * states).astype(BF16)
    states = cum_s[HEAD_ROWS:] + cum_p[HEAD_ROWS:] * carry_tail
    branch[HEAD_ROWS:, :] = (gelu_buf[HEAD_ROWS:] * states).astype(BF16)

    phase("out_proj")
    loads[10].wait()
    for c in range(4):
        cols = slice(512 * c, 512 * c + 512)
        value = dot(branch[...], wout[:, cols]).astype(BF16)
        part[:, :, cols] = value.reshape(TPS, 32, 512)
        for d in (2, 1, 3):
            to = (tp + d) % TPS
            lands = mixed_buf.at[tp, :, cols]
            send(part.at[to, :, cols], lands, mix_sem.at[0], mix_sem.at[1], sp, to)
    phase("gate_arrive")
    own_out(3)
    own_mirror(3)
    for k in (0, 1, 2):
        relay(k, FROM_MIRROR)
    for k in (4, 5, 6, 7):
        own_mirror(k)
    for k in (0, 1, 2):
        relay(k, FROM_MATE)
    phase("mix_arrive")
    for k in (13, 14, 15):
        loads[k].wait()
    came(mixed_buf.at[0:3], mix_sem.at[1])
    phase("norm1")
    mixed = part[tp].astype(F32)
    for d in (1, 2, 3):
        mixed = mixed + mixed_buf[(tp + d) % TPS].astype(F32)
    normed[...] = layer_norm(
        RESIDUAL_SCALE * stream[...].astype(F32) + mixed, gain1[...], bias1[...]
    ).astype(BF16)

    width = 2048 // CHUNKS

    def cols_of(c):
        return slice(width * c, width * c + width)

    def z_out(src, dst, trip, c):
        cols = cols_of(c)
        for d in FAR_FIRST:
            to = (zi + d) % PLANES
            lands = dst.at[zi, :, cols]
            send(
                src.at[to, :, cols], lands, hop_out_sem.at[trip, 0], z_sem.at[trip, c], z_peer(d), tp
            )
        dst[zi, :, cols] = src[zi, :, cols]

    def z_in(dst, trip, c):
        came(dst.at[0:7, :, cols_of(c)], z_sem.at[trip, c])

    def plane_in(dst, trip, c):
        @pl.when(owner)
        def _():
            came(dst.at[0:7, :, cols_of(c)], p_sem.at[trip, c])

        @pl.when(guest)
        def _():
            came(dst.at[:, :, cols_of(c)], p_sem.at[trip, c])

    def plane_out(src, dst, c):
        cols = cols_of(c)
        for dx in (2, 1, 3, 0):
            x_to = (xi + dx) % 4
            for other in (1, 0):
                expert = hosted + other * (1 - 2 * hosted)
                send(
                    src.at[x_to * 2 + expert, :, cols],
                    dst.at[pi, :, cols],
                    hop_out_sem.at[0, 1],
                    p_sem.at[0, c],
                    zi * PLANE + x_to * 2 + hosted,
                    mirror if other else tp,
                    when=guest if dx == 0 and other == 0 else None,
                )

        @pl.when(owner)
        def _():
            dst[pi, :, cols] = src[pi, :, cols]

    home = jnp.where(owner, tp, mirror)

    def plane_back(src, dst, c):
        cols = cols_of(c)
        for dx in (2, 1, 3, 0):
            for target_core in (0, 1):
                j = ((xi + dx) % 4) * 2 + target_core
                send(
                    src.at[j, :, cols],
                    dst.at[xi * 2 + hosted, :, cols],
                    hop_out_sem.at[1, 1],
                    p_sem.at[1, c],
                    zi * PLANE + j,
                    home,
                    when=jnp.logical_or(guest, core != target_core) if dx == 0 else None,
                )

        @pl.when(owner)
        def _():
            dst[pi, :, cols] = src[pi, :, cols]

    def swapped(src, c):
        cols = slice(width * c, width * c + width)
        to_row = lax.broadcasted_iota(jnp.int32, (128, 128), 0)
        from_row = lax.broadcasted_iota(jnp.int32, (128, 128), 1)
        outer, inner, pair = to_row // 16, (to_row // 2) % 8, to_row % 2
        pick = (from_row == inner * 16 + outer * 2 + pair).astype(BF16)
        rows = src[:, :, cols].reshape(128, width)
        return dot(pick, rows).astype(BF16).reshape(8, 16, width)

    phase("dispatch")
    for c in range(CHUNKS):
        cols = slice(width * c, width * c + width)
        value = dot(slot_buf[...], normed[:, cols]).astype(BF16)
        disp[:, :, cols] = value.reshape(8, 16, width)
        z_out(disp, arr1, 0, c)
    phase("shared")
    for k in (16, 17, 18, 19, 20):
        loads[k].wait()
    rows = normed[...]
    hidden = jax.nn.silu(dot(rows, shared_gate[...])) * dot(rows, shared_up[...])
    acc[...] = RESIDUAL_SCALE * rows.astype(F32) + dot(hidden.astype(BF16), shared_down[...])

    phase("relay_mid")
    relay(3, FROM_MIRROR)
    own_out(4)
    relay(3, FROM_MATE)

    for c in range(CHUNKS):
        phase(f"disp_z_{c}")
        z_in(arr1, 0, c)
        phase(f"disp_swap_{c}")
        disp2[:, :, cols_of(c)] = swapped(arr1, c)
        plane_out(disp2, arr2, c)
        if c == CHUNKS // 2 - 1:
            phase("relay_down")
            for k in (4, 5):
                relay(k, FROM_MIRROR)
                own_out(k + 1)
            relay(0, FROM_FAR)

    phase("far_gate_up")
    for k in (6, 7):
        relay(k, FROM_MIRROR)
        if k == 6:
            own_out(7)
    for k in (1, 2, 3):
        relay(k, FROM_FAR)
    phase("gate_up_guest")

    @pl.when(owner)
    def _():
        for copy in slot_loads:
            copy.wait()

    @pl.when(guest)
    def _():
        came(gate_up, guest_sem.at[0])

    both = None
    for c in range(CHUNKS):
        cols = cols_of(c)
        phase(f"disp_p_{c}")
        plane_in(arr2, 0, c)
        phase(f"gate_up_{c}")
        picked = arr2[:, :, cols].reshape(128, width)
        terms = [
            dot(picked, jnp.concatenate([gate_up[0, k, cols], gate_up[1, k, cols]], axis=1))
            for k in range(TPS)
        ]
        both = terms if both is None else [x + y for x, y in zip(both, terms)]
    phase("hidden")
    hidden = jnp.concatenate(
        [(jax.nn.silu(x[:, :128]) * x[:, 128:]).astype(BF16) for x in both], axis=1
    )

    def back_through_plane(c):
        phase(f"ret_p_{c}")
        plane_in(ret1, 1, c)
        phase(f"ret_swap_{c}")
        ret1p[:, :, cols_of(c)] = swapped(ret1, c)
        z_out(ret1p, ret2, 1, c)

    for c in range(CHUNKS):
        cols = cols_of(c)
        phase(f"down_arrive_{c}")
        relay(4 + c, FROM_MATE)
        relay(4 + c, FROM_FAR)
        phase(f"down_guest_{c}")

        @pl.when(guest)
        def _():
            came(down_w.at[:, :, cols], guest_sem.at[1 + c])

        phase(f"down_{c}")
        value = dot(hidden, down_w[:, :, cols].reshape(512, width)).astype(BF16)
        moe_out[:, :, cols] = value.reshape(8, 16, width)
        plane_back(moe_out, ret1, c)
        if c >= 1:
            back_through_plane(c - 1)

    back_through_plane(CHUNKS - 1)
    for c in range(CHUNKS):
        cols = cols_of(c)
        phase(f"ret_z_{c}")
        z_in(ret2, 1, c)
        phase(f"combine_{c}")
        back = ret2[:, :, cols].reshape(128, width)
        acc[:, cols] = acc[:, cols] + dot(weight_buf[0], back) + dot(weight_buf[1], back)
    phase("norm2")
    out_ref[...] = layer_norm(acc[...], gain2[...], bias2[...]).astype(BF16)
    phase("drain")
    left(border_out, border_sem.at[0])
    left(carry1.at[0:7], carry_sem.at[0, 0])
    left(carry2.at[0:7], carry_sem.at[0, 1])
    left(part.at[0:3], mix_sem.at[0])
    for trip, (z_src, p_src) in enumerate(((disp, disp2), (ret1p, moe_out))):
        left(z_src.at[0:7], hop_out_sem.at[trip, 0])

        @pl.when(owner)
        def _():
            left(p_src.at[0:7], hop_out_sem.at[trip, 1])

        @pl.when(guest)
        def _():
            left(p_src, hop_out_sem.at[trip, 1])

    @pl.when(owner)
    def _():
        left(gate_up, part_out_sem.at[TO_SIBLING, 0])
        left(down_w, part_out_sem.at[TO_SIBLING, 1])
        left(gate_up.at[:, 0:2], part_out_sem.at[ACROSS, 0])
        left(down_w.at[0:2], part_out_sem.at[ACROSS, 1])

    @pl.when(guest)
    def _():
        left(gate_up.at[0, 0:2], part_out_sem.at[ACROSS, 0])
        left(down_w.at[0], part_out_sem.at[ACROSS, 1])

    phase()


def shards(
    stream, recurrence_input, output_gate_input, convolution_taps, first_group_gates,
    second_group_gates, channel_decay, position_log_extra, recurrence_output_weight,
    first_norm_gain, first_norm_bias, routed_expert_index, routed_expert_weight,
    routed_gate_weight, routed_up_weight, routed_down_weight, shared_gate_weight,
    shared_up_weight, shared_down_weight, second_norm_gain, second_norm_bias,
):
    operands = (
        stream,
        recurrence_input,
        output_gate_input,
        convolution_taps,
        first_group_gates,
        second_group_gates,
        channel_decay,
        position_log_extra,
        recurrence_output_weight.reshape(512, 2048),
        first_norm_gain.reshape(1, 2048),
        first_norm_bias.reshape(1, 2048),
        routed_expert_index.T,
        routed_expert_weight.T,
        routed_gate_weight.reshape(2048, 128),
        routed_up_weight.reshape(2048, 128),
        routed_down_weight.reshape(128, 2048),
        shared_gate_weight,
        shared_up_weight,
        shared_down_weight,
        second_norm_gain.reshape(1, 2048),
        second_norm_bias.reshape(1, 2048),
    )
    held = [pltpu.VMEM(operand.shape, operand.dtype) for operand in operands]
    wide = pltpu.VMEM((8, 16, 2048), BF16)
    return pl.pallas_call(
        mega,
        out_shape=jax.ShapeDtypeStruct((32, 2048), BF16),
        in_specs=[pl.BlockSpec(memory_space=pl.ANY)] * len(operands),
        out_specs=pl.BlockSpec(memory_space=pltpu.VMEM),
        scratch_shapes=[
            *held,
            pltpu.VMEM((2, TPS, 2048, 128), BF16),
            pltpu.VMEM((TPS, 128, 2048), BF16),
            pltpu.VMEM((128, 512), F32),
            pltpu.VMEM((2, 128, 8), F32),
            pltpu.VMEM((128 + HEAD_ROWS, 512), F32),
            pltpu.VMEM((HEAD_ROWS, 2, 256), BF16),
            pltpu.VMEM((128, 512), F32),
            pltpu.VMEM((128, 512), F32),
            pltpu.VMEM((PLANE, 2, 4, 128), F32),
            pltpu.VMEM((PLANES, 2, 4, 128), F32),
            pltpu.VMEM((128, 512), F32),
            pltpu.VMEM((128, 512), BF16),
            pltpu.VMEM((TPS, 32, 2048), BF16),
            pltpu.VMEM((TPS, 32, 2048), BF16),
            pltpu.VMEM((32, 2048), BF16),
            pltpu.VMEM((128, 32), BF16),
            pltpu.VMEM((2, 32, 128), BF16),
            wide, wide, wide, wide, wide, wide, wide, wide,
            pltpu.VMEM((32, 2048), F32),
            pltpu.SemaphoreType.DMA((len(operands),)),
            pltpu.SemaphoreType.DMA((3,)),
            pltpu.SemaphoreType.DMA((2,)),
            pltpu.SemaphoreType.DMA((3, 8)),
            pltpu.SemaphoreType.DMA((5,)),
            pltpu.SemaphoreType.DMA((2, 2)),
            pltpu.SemaphoreType.DMA((2, 2)),
            pltpu.SemaphoreType.DMA((2,)),
            pltpu.SemaphoreType.DMA((2, CHUNKS)),
            pltpu.SemaphoreType.DMA((2, CHUNKS)),
            pltpu.SemaphoreType.DMA((2, 2)),
        ],
        compiler_params=pltpu.CompilerParams(
            collective_id=0, has_side_effects=True, vmem_limit_bytes=56 * 2**20
        ),
        name="mega",
    )(*operands)


def solution(mesh):
    in_specs = (
        P(("sp", "tp"), None),
        P("sp", None, "tp"),
        P("sp", None, "tp"),
        P(None, None, "tp"),
        P(None, "tp", None, None),
        P(None, "tp", None, None),
        P(None, "tp"),
        P("sp", None, "tp"),
        P(None, "tp", None),
        P(),
        P(),
        P("sp", None),
        P("sp", None),
        P("sp", None, "tp"),
        P("sp", None, "tp"),
        P("sp", "tp", None),
        P(),
        P(),
        P(),
        P(),
        P(),
    )
    out_specs = P(("sp", "tp"), None)
    return jax.shard_map(shards, mesh=mesh, in_specs=in_specs, out_specs=out_specs, check_vma=False)
```

```python
import jax
import jax.numpy as jnp
from jax import lax
from jax.experimental import pallas as pl
from jax.experimental.pallas import tpu as pltpu
from jax.sharding import PartitionSpec as P

RESIDUAL_SCALE = 8.0**0.25
NORM_EPSILON = 1e-05
MESH = pl.DeviceIdType.MESH
F32 = jnp.float32
BF16 = jnp.bfloat16

PLANE = 8
PLANES = 8
TPS = 4
HEAD_ROWS = 16
CHUNKS = 4
FAR_FIRST = (4, 3, 5, 2, 6, 1, 7)


class Phases:
    def __init__(self):
        self.scope = None

    def __call__(self, name=None):
        if self.scope is not None:
            self.scope.__exit__(None, None, None)
        self.scope = None
        if name is not None:
            self.scope = jax.named_scope(name)
            self.scope.__enter__()


def layer_norm(values, gain_vec, bias_vec):
    row_mean = jnp.mean(values, axis=-1, keepdims=True)
    centred = values - row_mean
    spread = jnp.mean(jnp.square(centred), axis=-1, keepdims=True)
    return centred * lax.rsqrt(spread + NORM_EPSILON) * gain_vec + bias_vec


def softplus_of_minus(d):
    u = jnp.exp(-jnp.abs(d))
    s = u / (2.0 + u)
    q = s * s
    series = jnp.full_like(s, 1.0 / 15.0)
    for odd in (13, 11, 9, 7, 5, 3, 1):
        series = series * q + 1.0 / odd
    return jnp.maximum(-d, 0.0) + 2.0 * s * series


def minus_expm1(z):
    series = jnp.full_like(z, 1.0 / 40320.0)
    for factor in (5040.0, 720.0, 120.0, 24.0, 6.0, 2.0, 1.0):
        series = series * z + 1.0 / factor
    return jnp.where(z > -0.25, -z * series, 1.0 - jnp.exp(z))


def dot(a, b):
    return jnp.dot(a, b, preferred_element_type=F32)


def mega(
    stream_h, rec_h, gatein_h, taps_h, small_gates_h, large_gates_h, decay_h, extra_h,
    wout_h, gain1_h, bias1_h, index_h, weight_h, gate_w_h, up_w_h, down_w_h,
    shared_gate_h, shared_up_h, shared_down_h, gain2_h, bias2_h,
    out_ref,
    stream, rec, gatein, taps, small_gates, large_gates, decay, extra_raw,
    wout, gain1, bias1, index, weight, own_gate, own_up, own_down,
    shared_gate, shared_up, shared_down, gain2, bias2,
    gate_up, down_w,
    extra, turned, rec_f, border, cum_p, cum_s, carry1, carry2, gelu_buf, branch,
    part, mixed_buf, normed, slot_buf, weight_buf,
    disp, arr1, disp2, arr2, moe_out, ret1, ret1p, ret2, acc,
    load_sem, slot_sem, border_sem, part_sem, guest_sem, part_out_sem, carry_sem, plane_sem, mix_sem,
    z_sem, p_sem, hop_out_sem,
):
    sp = lax.axis_index("sp")
    tp = lax.axis_index("tp")
    zi = sp // PLANE
    pi = sp % PLANE
    xi = pi // 2
    core = sp % 2
    hosted = tp // 2
    mirror = 3 - tp
    mate = tp + 1 - 2 * (tp % 2)
    far = 3 - mate
    sibling = sp + 1 - 2 * core
    owner = core == hosted
    guest = core != hosted
    phase = Phases()
    phase("loads")

    def remote(src, dst, send_sem, recv_sem, sp_to, tp_to):
        return pltpu.make_async_remote_copy(
            src_ref=src,
            dst_ref=dst,
            send_sem=send_sem,
            recv_sem=recv_sem,
            device_id={"sp": sp_to, "tp": tp_to},
            device_id_type=MESH,
        )

    def send(*args, when=None):
        copy = remote(*args)
        if when is None:
            copy.start()
        else:
            pl.when(when)(copy.start)

    def came(ref, sem):
        remote(ref, ref, sem, sem, sp, tp).wait_recv()

    def left(ref, sem):
        remote(ref, ref, sem, sem, sp, tp).wait_send()

    def plane_peer(d):
        return zi * PLANE + (pi + d) % PLANE

    def z_peer(d):
        return ((zi + d) % PLANES) * PLANE + pi

    barrier = pltpu.get_barrier_semaphore()

    def greet(sp_to, tp_to):
        pl.semaphore_signal(
            barrier, inc=1, device_id={"sp": sp_to, "tp": tp_to}, device_id_type=MESH
        )

    for d in FAR_FIRST:
        greet(z_peer(d), tp)
    for d in FAR_FIRST:
        greet(plane_peer(d), tp)
    for d in range(1, TPS):
        greet(sp, (tp + d) % TPS)
    greet((sp + 63) % 64, tp)
    for j in range(PLANE):
        greet(zi * PLANE + j, mirror)

    names = (
        (rec_h, rec), (small_gates_h, small_gates), (large_gates_h, large_gates), (taps_h, taps),
        (decay_h, decay), (extra_h, extra_raw), (gatein_h, gatein), (gate_w_h, own_gate),
        (up_w_h, own_up), (down_w_h, own_down), (wout_h, wout), (index_h, index),
        (weight_h, weight), (stream_h, stream), (gain1_h, gain1), (bias1_h, bias1),
        (shared_gate_h, shared_gate), (shared_up_h, shared_up), (shared_down_h, shared_down),
        (gain2_h, gain2), (bias2_h, bias2),
    )
    loads = []
    for k, (src, dst) in enumerate(names):
        loads.append(pltpu.make_async_copy(src, dst, load_sem.at[k]))
        loads[-1].start()
    wholes = (gate_up.at[0], gate_up.at[1], down_w)
    owns = (own_gate, own_up, own_down)
    slot_loads = [
        pltpu.make_async_copy(src, dst.at[tp], slot_sem.at[m])
        for m, (src, dst) in enumerate(zip((gate_w_h, up_w_h, down_w_h), wholes))
    ]

    @pl.when(owner)
    def _():
        for copy in slot_loads:
            copy.start()

    phase("wait_loads")
    length = rec.shape[0]
    loads[0].wait()
    phase("barrier")
    pl.semaphore_wait(barrier, 7 + 7 + 3 + 1 + 8)
    phase("send_gate")
    border_out = rec.at[length - HEAD_ROWS :]
    send(border_out, border, border_sem.at[0], border_sem.at[1], (sp + 1) % 64, tp)

    FROM_MATE, FROM_MIRROR, FROM_FAR = range(3)
    origin = {FROM_MATE: mate, FROM_MIRROR: mirror, FROM_FAR: far}
    TO_SIBLING, ACROSS = range(2)

    def piece_of(ref, k, lead=()):
        if k < 4:
            return ref.at[(*lead, slice(1024 * (k % 2), 1024 * (k % 2) + 1024))]
        return ref.at[(*lead, slice(None), slice(512 * (k - 4), 512 * (k - 4) + 512))]

    def buffer_of(k):
        return k // 2 if k < 4 else 2

    def held_piece(k, at):
        return piece_of(wholes[buffer_of(k)], k, (at,))

    def across(src, k, at, kind, tp_to, when):
        out = part_out_sem.at[ACROSS, int(k >= 4)]
        send(src, held_piece(k, at), out, part_sem.at[kind, k], sp, tp_to, when=when)

    def to_sibling(src, k, at):
        out = part_out_sem.at[TO_SIBLING, int(k >= 4)]
        lands = guest_sem.at[max(k - 3, 0)]
        send(src, held_piece(k, at), out, lands, sibling, tp, when=owner)

    def own_out(k):
        src = piece_of(owns[buffer_of(k)], k)
        across(src, k, tp, FROM_MATE, mate, owner)

    def own_mirror(k):
        src = piece_of(owns[buffer_of(k)], k)
        across(src, k, tp, FROM_MIRROR, mirror, guest)

    def relay(k, kind):
        got = held_piece(k, origin[kind])

        @pl.when(owner)
        def _():
            came(got, part_sem.at[kind, k])

        if kind == FROM_MIRROR:
            across(got, k, origin[kind], FROM_FAR, mate, owner)
        to_sibling(got, k, origin[kind])

    for k in (7, 8):
        loads[k].wait()
    for k in (0, 1, 2, 3):
        own_out(k)
        own_mirror(k)

    phase("prepare")
    for k in range(1, 6):
        loads[k].wait()
    for g in range(2):
        rec_f[HEAD_ROWS:, 256 * g : 256 * g + 256] = rec[:, g, :].astype(F32)
        extra[:, 256 * g : 256 * g + 256] = extra_raw[:, g, :]
    row_i = lax.broadcasted_iota(jnp.int32, (64, 128), 0)
    col_i = lax.broadcasted_iota(jnp.int32, (64, 128), 1)
    put_low = (row_i == col_i).astype(BF16)
    put_high = (row_i + 64 == col_i).astype(BF16)
    blocks = []
    for which in range(2):
        maps = []
        for pair in range(2):
            low = dot(small_gates[which, 2 * pair], put_low)
            high = dot(small_gates[which, 2 * pair + 1], put_high)
            maps.append(jnp.concatenate([low, high], axis=0).astype(BF16))
        for head in range(2):
            maps.append(large_gates[which, head])
        blocks.append(maps)
    rate = -8.0 * softplus_of_minus(decay[...])
    tap_f = taps[...].astype(F32)

    def tap(k, b):
        return tap_f[k, b // 2 : b // 2 + 1, 128 * (b % 2) : 128 * (b % 2) + 128]

    def scanned(first, count):
        for b in range(4):
            lanes = slice(128 * b, 128 * b + 128)
            conv = tap(0, b) * rec_f[first + HEAD_ROWS - 3 : first + HEAD_ROWS - 3 + count, lanes]
            for k in range(1, 4):
                at = first + HEAD_ROWS - 3 + k
                conv = conv + tap(k, b) * rec_f[at : at + count, lanes]
            conv = conv.astype(BF16)
            recur_gate = jax.nn.sigmoid(dot(conv, blocks[0][b]))
            input_gate = jax.nn.sigmoid(dot(conv, blocks[1][b]))
            log_decay = recur_gate * rate[b // 2 : b // 2 + 1, 128 * (b % 2) : 128 * (b % 2) + 128] + extra[first : first + count, lanes]
            p = jnp.exp(log_decay)
            s = jnp.sqrt(minus_expm1(2.0 * log_decay)) * input_gate * conv.astype(F32)
            p = p.reshape(count // 8, 8, 128)
            s = s.reshape(count // 8, 8, 128)
            row = lax.broadcasted_iota(jnp.int32, (count // 8, 8, 128), 1)
            for by in (1, 2, 4):
                p_prev = pltpu.roll(p, by, 1)
                s_prev = pltpu.roll(s, by, 1)
                s = jnp.where(row >= by, p * s_prev + s, s)
                p = jnp.where(row >= by, p * p_prev, p)
            p_in = jnp.ones((1, 128), F32)
            s_in = jnp.zeros((1, 128), F32)
            for t in range(count // 8):
                s_t = s[t] + p[t] * s_in
                p_t = p[t] * p_in
                cum_s[first + 8 * t : first + 8 * t + 8, lanes] = s_t
                cum_p[first + 8 * t : first + 8 * t + 8, lanes] = p_t
                s_in = s_t[7:8]
                p_in = p_t[7:8]

    phase("scan_tail")
    scanned(HEAD_ROWS, length - HEAD_ROWS)
    loads[9].wait()
    for k in range(8):
        to_sibling(piece_of(owns[buffer_of(k)], k), k, tp)
    phase("border")
    came(border, border_sem.at[1])
    phase("scan_head")
    for g in range(2):
        border_f = border[:, g, :].astype(F32)
        rec_f[0:HEAD_ROWS, 256 * g : 256 * g + 256] = jnp.where(
            sp > 0, border_f, jnp.zeros_like(border_f)
        )
    scanned(0, HEAD_ROWS)

    head_p = cum_p[HEAD_ROWS - 1 : HEAD_ROWS, :]
    head_s = cum_s[HEAD_ROWS - 1 : HEAD_ROWS, :]
    tail_p = cum_p[length - 1 : length, :]
    tail_s = cum_s[length - 1 : length, :]
    total_p = head_p * tail_p
    total_s = tail_p * head_s + tail_s
    mine1 = carry1.at[pi]
    for b in range(4):
        mine1[0, b : b + 1, :] = total_p[:, 128 * b : 128 * b + 128]
        mine1[1, b : b + 1, :] = total_s[:, 128 * b : 128 * b + 128]
    for d in FAR_FIRST:
        send(mine1, mine1, carry_sem.at[0], carry_sem.at[1], plane_peer(d), tp)

    phase("slots")
    for k in (6, 11, 12):
        loads[k].wait()
    own_rows = pl.ds(pl.multiple_of(tp * 32, 32), 32)
    unused = jnp.zeros((4, 128), F32)
    turned[0] = jnp.concatenate([index[...].astype(F32), unused], axis=0).T
    turned[1] = jnp.concatenate([weight[...], unused], axis=0).T
    ids = turned[0, own_rows, :].astype(jnp.int32)
    factors = turned[1, own_rows, :]
    slot = lax.broadcasted_iota(jnp.int32, (32, 128), 1)
    named = jnp.zeros((32, 128), F32)
    scaled = jnp.zeros((32, 128), F32)
    for k in range(4):
        hit = ids[:, k : k + 1] == slot // 2
        named = named + jnp.where(hit, 1.0, 0.0)
        scaled = scaled + jnp.where(hit, factors[:, k : k + 1], 0.0)
    below = lax.broadcasted_iota(jnp.int32, (32, 32), 0) > lax.broadcasted_iota(
        jnp.int32, (32, 32), 1
    )
    earlier = dot(below.astype(BF16), named.astype(BF16))
    right_slot = jnp.abs(earlier - (slot % 2).astype(F32)) < 0.5
    to_row = lax.broadcasted_iota(jnp.int32, (128, 128), 0)
    from_row = lax.broadcasted_iota(jnp.int32, (128, 128), 1)
    outer, inner, pair = to_row // 16, (to_row // 2) % 8, to_row % 2
    pick = (from_row == inner * 16 + outer * 2 + pair).astype(BF16)
    slot_rows = jnp.where(right_slot, named, 0.0).T.astype(BF16)
    slot_buf[0] = slot_rows
    slot_buf[1] = dot(pick, slot_rows).astype(BF16)
    scaled = jnp.where(right_slot, scaled, 0.0)
    high = scaled.astype(BF16)
    low = (scaled - high.astype(F32)).astype(BF16)
    for part_no, values in enumerate((high, low)):
        weight_buf[part_no] = dot(values, pick).astype(BF16)
        weight_buf[2 + part_no] = values
    for g in range(2):
        gelu_buf[:, 256 * g : 256 * g + 256] = jax.nn.gelu(gatein[:, g, :].astype(F32))
    phase("carry1")

    came(carry1.at[0:7], carry_sem.at[1])
    one = jnp.ones((4, 128), F32)
    nought = jnp.zeros((4, 128), F32)
    all_p, all_s, in_p, in_s = one, nought, one, nought
    for j in range(PLANE):
        p_j, s_j = carry1[j, 0], carry1[j, 1]
        all_p, all_s = all_p * p_j, p_j * all_s + s_j
        in_p = jnp.where(j < pi, in_p * p_j, in_p)
        in_s = jnp.where(j < pi, p_j * in_s + s_j, in_s)
    mine2 = carry2.at[zi]
    mine2[0] = all_p
    mine2[1] = all_s
    for d in (4, 3, 5, 2, 6, 1, 7):
        send(
            mine2,
            mine2,
            plane_sem.at[0, d - 1],
            plane_sem.at[1, d - 1],
            z_peer(d),
            tp,
            when=zi + d < PLANES,
        )
    phase("carry2")
    for d in range(1, PLANES):
        got = carry2.at[(zi + PLANES - d) % PLANES]

        @pl.when(zi >= d)
        def _():
            came(got, plane_sem.at[1, d - 1])

    phase("fixup")
    planes_s = nought
    for k in range(PLANES):
        planes_s = jnp.where(k < zi, carry2[k, 0] * planes_s + carry2[k, 1], planes_s)
    carry_in = in_p * planes_s + in_s
    carry_row = jnp.concatenate([carry_in[b : b + 1] for b in range(4)], axis=1)
    carry_tail = head_s + head_p * carry_row
    states = cum_s[:HEAD_ROWS] + cum_p[:HEAD_ROWS] * carry_row
    branch[:HEAD_ROWS, :] = (gelu_buf[:HEAD_ROWS] * states).astype(BF16)
    states = cum_s[HEAD_ROWS:] + cum_p[HEAD_ROWS:] * carry_tail
    branch[HEAD_ROWS:, :] = (gelu_buf[HEAD_ROWS:] * states).astype(BF16)

    phase("out_proj")
    loads[10].wait()
    for c in range(4):
        cols = slice(512 * c, 512 * c + 512)
        value = dot(branch[...], wout[:, cols]).astype(BF16)
        part[:, :, cols] = value.reshape(TPS, 32, 512)
        for d in (2, 1, 3):
            to = (tp + d) % TPS
            lands = mixed_buf.at[tp, :, cols]
            send(part.at[to, :, cols], lands, mix_sem.at[0], mix_sem.at[1], sp, to)
    phase("gate_arrive")
    for k in (4, 5, 6, 7):
        own_mirror(k)
    for k in (0, 1, 2, 3):
        relay(k, FROM_MIRROR)
    own_out(4)
    for k in (0, 1, 2, 3):
        relay(k, FROM_MATE)
    phase("mix_arrive")
    for k in (13, 14, 15):
        loads[k].wait()
    came(mixed_buf.at[0:3], mix_sem.at[1])
    phase("norm1")
    mixed = part[tp].astype(F32)
    for d in (1, 2, 3):
        mixed = mixed + mixed_buf[(tp + d) % TPS].astype(F32)
    normed[...] = layer_norm(
        RESIDUAL_SCALE * stream[...].astype(F32) + mixed, gain1[...], bias1[...]
    ).astype(BF16)

    width = 2048 // CHUNKS

    def cols_of(c):
        return slice(width * c, width * c + width)

    def z_out(src, dst, trip, c):
        cols = cols_of(c)
        for d in FAR_FIRST:
            to = (zi + d) % PLANES
            lands = dst.at[zi, :, cols]
            send(
                src.at[to, :, cols], lands, hop_out_sem.at[trip, 0], z_sem.at[trip, c], z_peer(d), tp
            )
        dst[zi, :, cols] = src[zi, :, cols]

    def z_in(dst, trip, c):
        came(dst.at[0:7, :, cols_of(c)], z_sem.at[trip, c])

    def plane_in(dst, trip, c):
        @pl.when(owner)
        def _():
            came(dst.at[0:7, :, cols_of(c)], p_sem.at[trip, c])

        @pl.when(guest)
        def _():
            came(dst.at[:, :, cols_of(c)], p_sem.at[trip, c])

    def plane_out(src, dst, c):
        cols = cols_of(c)
        for dx in (2, 1, 3, 0):
            x_to = (xi + dx) % 4
            for other in (1, 0):
                expert = hosted + other * (1 - 2 * hosted)
                send(
                    src.at[x_to * 2 + expert, :, cols],
                    dst.at[pi, :, cols],
                    hop_out_sem.at[0, 1],
                    p_sem.at[0, c],
                    zi * PLANE + x_to * 2 + hosted,
                    mirror if other else tp,
                    when=guest if dx == 0 and other == 0 else None,
                )

        @pl.when(owner)
        def _():
            dst[pi, :, cols] = src[pi, :, cols]

    home = jnp.where(owner, tp, mirror)

    def plane_back(src, dst, c):
        cols = cols_of(c)
        for dx in (2, 1, 3, 0):
            for target_core in (0, 1):
                j = ((xi + dx) % 4) * 2 + target_core
                send(
                    src.at[j, :, cols],
                    dst.at[xi * 2 + hosted, :, cols],
                    hop_out_sem.at[1, 1],
                    p_sem.at[1, c],
                    zi * PLANE + j,
                    home,
                    when=jnp.logical_or(guest, core != target_core) if dx == 0 else None,
                )

        @pl.when(owner)
        def _():
            dst[pi, :, cols] = src[pi, :, cols]

    def swapped(src, c):
        rows = src[:, :, cols_of(c)].reshape(128, width)
        return dot(pick, rows).astype(BF16).reshape(8, 16, width)

    Z_FIRST = tuple(range(CHUNKS // 2))
    P_FIRST = tuple(range(CHUNKS // 2, CHUNKS))
    for c in (*Z_FIRST, *P_FIRST):
        cols = cols_of(c)
        order = int(c in P_FIRST)
        value = dot(slot_buf[order], normed[:, cols]).astype(BF16)
        disp[:, :, cols] = value.reshape(8, 16, width)
        if c in Z_FIRST:
            z_out(disp, arr1, 0, c)
        else:
            plane_out(disp, arr1, c)
    phase("shared")
    for k in (16, 17, 18, 19, 20):
        loads[k].wait()
    rows = normed[...]
    hidden = jax.nn.silu(dot(rows, shared_gate[...])) * dot(rows, shared_up[...])
    acc[...] = RESIDUAL_SCALE * rows.astype(F32) + dot(hidden.astype(BF16), shared_down[...])

    phase("relay_mid")
    relay(4, FROM_MIRROR)
    own_out(5)

    for c in P_FIRST:
        phase(f"disp_p1_{c}")
        plane_in(arr1, 0, c)
        phase(f"disp_swap_{c}")
        disp2[:, :, cols_of(c)] = swapped(arr1, c)
        z_out(disp2, arr2, 0, c)
    phase("relay_down")
    for k in (5, 6, 7):
        relay(k, FROM_MIRROR)
        if k < 7:
            own_out(k + 1)
    relay(0, FROM_FAR)
    for c in Z_FIRST:
        phase(f"disp_z1_{c}")
        z_in(arr1, 0, c)
        phase(f"disp_swap_{c}")
        disp2[:, :, cols_of(c)] = swapped(arr1, c)
        plane_out(disp2, arr2, c)

    phase("far_gate_up")
    for k in (1, 2, 3):
        relay(k, FROM_FAR)
    phase("gate_up_guest")

    @pl.when(owner)
    def _():
        for copy in slot_loads:
            copy.wait()

    @pl.when(guest)
    def _():
        came(gate_up, guest_sem.at[0])

    both = None
    for n, c in enumerate([c for both_kinds in zip(Z_FIRST, P_FIRST) for c in both_kinds]):
        cols = cols_of(c)
        if n == CHUNKS - 1:
            phase("relay_down_0")
            relay(4, FROM_MATE)
            relay(4, FROM_FAR)
        phase(f"disp_2_{c}")
        if c in Z_FIRST:
            plane_in(arr2, 0, c)
            phase(f"gate_up_{c}")
            picked = arr2[:, :, cols].reshape(128, width)
        else:
            z_in(arr2, 0, c)
            phase(f"gate_up_{c}")
            picked = swapped(arr2, c).reshape(128, width)
        terms = [
            dot(picked, jnp.concatenate([gate_up[0, k, cols], gate_up[1, k, cols]], axis=1))
            for k in range(TPS)
        ]
        both = terms if both is None else [x + y for x, y in zip(both, terms)]
    phase("hidden")
    hidden = jnp.concatenate(
        [(jax.nn.silu(x[:, :128]) * x[:, 128:]).astype(BF16) for x in both], axis=1
    )

    hidden_by_z = dot(pick, hidden).astype(BF16)

    def second_hop(c):
        phase(f"ret_1_{c}")
        if c in Z_FIRST:
            z_in(ret1, 1, c)
        else:
            plane_in(ret1, 1, c)
        phase(f"ret_swap_{c}")
        ret1p[:, :, cols_of(c)] = swapped(ret1, c)
        if c in Z_FIRST:
            plane_back(ret1p, ret2, c)
        else:
            z_out(ret1p, ret2, 1, c)

    for c in range(CHUNKS):
        cols = cols_of(c)
        phase(f"down_arrive_{c}")
        if c > 0:
            relay(4 + c, FROM_MATE)
            relay(4 + c, FROM_FAR)
        phase(f"down_guest_{c}")

        @pl.when(guest)
        def _():
            came(down_w.at[:, :, cols], guest_sem.at[1 + c])

        phase(f"down_{c}")
        rows = hidden_by_z if c in Z_FIRST else hidden
        value = dot(rows, down_w[:, :, cols].reshape(512, width)).astype(BF16)
        moe_out[:, :, cols] = value.reshape(8, 16, width)
        if c in Z_FIRST:
            z_out(moe_out, ret1, 1, c)
        else:
            plane_back(moe_out, ret1, c)
        if c == CHUNKS - 2:
            second_hop(0)

    for c in range(1, CHUNKS):
        second_hop(c)
    for c in range(CHUNKS):
        cols = cols_of(c)
        phase(f"ret_2_{c}")
        if c in Z_FIRST:
            plane_in(ret2, 1, c)
        else:
            z_in(ret2, 1, c)
        phase(f"combine_{c}")
        back = ret2[:, :, cols].reshape(128, width)
        order = 0 if c in Z_FIRST else 2
        acc[:, cols] = (
            acc[:, cols] + dot(weight_buf[order], back) + dot(weight_buf[order + 1], back)
        )
    phase("norm2")
    out_ref[...] = layer_norm(acc[...], gain2[...], bias2[...]).astype(BF16)
    phase("drain")
    left(border_out, border_sem.at[0])
    left(carry1.at[0:7], carry_sem.at[0])
    for d in range(1, PLANES):

        @pl.when(zi + d < PLANES)
        def _():
            left(mine2, plane_sem.at[0, d - 1])

    left(part.at[0:3], mix_sem.at[0])
    for trip, (z_src, p_src) in enumerate(((disp, disp2), (ret1p, moe_out))):
        left(z_src.at[0:7], hop_out_sem.at[trip, 0])

        @pl.when(owner)
        def _():
            left(p_src.at[0:7], hop_out_sem.at[trip, 1])

        @pl.when(guest)
        def _():
            left(p_src, hop_out_sem.at[trip, 1])

    @pl.when(owner)
    def _():
        left(gate_up, part_out_sem.at[TO_SIBLING, 0])
        left(down_w, part_out_sem.at[TO_SIBLING, 1])
        left(gate_up.at[:, 0:2], part_out_sem.at[ACROSS, 0])
        left(down_w.at[0:2], part_out_sem.at[ACROSS, 1])

    @pl.when(guest)
    def _():
        left(gate_up.at[0, 0:2], part_out_sem.at[ACROSS, 0])
        left(down_w.at[0], part_out_sem.at[ACROSS, 1])

    phase()


def shards(
    stream, recurrence_input, output_gate_input, convolution_taps, first_group_gates,
    second_group_gates, channel_decay, position_log_extra, recurrence_output_weight,
    first_norm_gain, first_norm_bias, routed_expert_index, routed_expert_weight,
    routed_gate_weight, routed_up_weight, routed_down_weight, shared_gate_weight,
    shared_up_weight, shared_down_weight, second_norm_gain, second_norm_bias,
):
    operands = (
        stream,
        recurrence_input,
        output_gate_input,
        convolution_taps,
        first_group_gates,
        second_group_gates,
        channel_decay,
        position_log_extra,
        recurrence_output_weight.reshape(512, 2048),
        first_norm_gain.reshape(1, 2048),
        first_norm_bias.reshape(1, 2048),
        routed_expert_index.T,
        routed_expert_weight.T,
        routed_gate_weight.reshape(2048, 128),
        routed_up_weight.reshape(2048, 128),
        routed_down_weight.reshape(128, 2048),
        shared_gate_weight,
        shared_up_weight,
        shared_down_weight,
        second_norm_gain.reshape(1, 2048),
        second_norm_bias.reshape(1, 2048),
    )
    held = [pltpu.VMEM(operand.shape, operand.dtype) for operand in operands]
    wide = pltpu.VMEM((8, 16, 2048), BF16)
    return pl.pallas_call(
        mega,
        out_shape=jax.ShapeDtypeStruct((32, 2048), BF16),
        in_specs=[pl.BlockSpec(memory_space=pl.ANY)] * len(operands),
        out_specs=pl.BlockSpec(memory_space=pltpu.VMEM),
        scratch_shapes=[
            *held,
            pltpu.VMEM((2, TPS, 2048, 128), BF16),
            pltpu.VMEM((TPS, 128, 2048), BF16),
            pltpu.VMEM((128, 512), F32),
            pltpu.VMEM((2, 128, 8), F32),
            pltpu.VMEM((128 + HEAD_ROWS, 512), F32),
            pltpu.VMEM((HEAD_ROWS, 2, 256), BF16),
            pltpu.VMEM((128, 512), F32),
            pltpu.VMEM((128, 512), F32),
            pltpu.VMEM((PLANE, 2, 4, 128), F32),
            pltpu.VMEM((PLANES, 2, 4, 128), F32),
            pltpu.VMEM((128, 512), F32),
            pltpu.VMEM((128, 512), BF16),
            pltpu.VMEM((TPS, 32, 2048), BF16),
            pltpu.VMEM((TPS, 32, 2048), BF16),
            pltpu.VMEM((32, 2048), BF16),
            pltpu.VMEM((2, 128, 32), BF16),
            pltpu.VMEM((4, 32, 128), BF16),
            wide, wide, wide, wide, wide, wide, wide, wide,
            pltpu.VMEM((32, 2048), F32),
            pltpu.SemaphoreType.DMA((len(operands),)),
            pltpu.SemaphoreType.DMA((3,)),
            pltpu.SemaphoreType.DMA((2,)),
            pltpu.SemaphoreType.DMA((3, 8)),
            pltpu.SemaphoreType.DMA((5,)),
            pltpu.SemaphoreType.DMA((2, 2)),
            pltpu.SemaphoreType.DMA((2,)),
            pltpu.SemaphoreType.DMA((2, 7)),
            pltpu.SemaphoreType.DMA((2,)),
            pltpu.SemaphoreType.DMA((2, CHUNKS)),
            pltpu.SemaphoreType.DMA((2, CHUNKS)),
            pltpu.SemaphoreType.DMA((2, 2)),
        ],
        compiler_params=pltpu.CompilerParams(
            collective_id=0, has_side_effects=True, vmem_limit_bytes=56 * 2**20
        ),
        name="mega",
    )(*operands)


def solution(mesh):
    in_specs = (
        P(("sp", "tp"), None),
        P("sp", None, "tp"),
        P("sp", None, "tp"),
        P(None, None, "tp"),
        P(None, "tp", None, None),
        P(None, "tp", None, None),
        P(None, "tp"),
        P("sp", None, "tp"),
        P(None, "tp", None),
        P(),
        P(),
        P("sp", None),
        P("sp", None),
        P("sp", None, "tp"),
        P("sp", None, "tp"),
        P("sp", "tp", None),
        P(),
        P(),
        P(),
        P(),
        P(),
    )
    out_specs = P(("sp", "tp"), None)
    return jax.shard_map(shards, mesh=mesh, in_specs=in_specs, out_specs=out_specs, check_vma=False)
```

```python
import jax
import jax.numpy as jnp
from jax import lax
from jax.experimental import pallas as pl
from jax.experimental.pallas import tpu as pltpu
from jax.sharding import PartitionSpec as P

RESIDUAL_SCALE = 8.0**0.25
NORM_EPSILON = 1e-05
MESH = pl.DeviceIdType.MESH
F32 = jnp.float32
BF16 = jnp.bfloat16

PLANE = 8
PLANES = 8
TPS = 4
HEAD_ROWS = 16
CHUNKS = 4
FAR_FIRST = (4, 3, 5, 2, 6, 1, 7)


class Phases:
    def __init__(self):
        self.scope = None

    def __call__(self, name=None):
        if self.scope is not None:
            self.scope.__exit__(None, None, None)
        self.scope = None
        if name is not None:
            self.scope = jax.named_scope(name)
            self.scope.__enter__()


def layer_norm(values, gain_vec, bias_vec):
    row_mean = jnp.mean(values, axis=-1, keepdims=True)
    centred = values - row_mean
    spread = jnp.mean(jnp.square(centred), axis=-1, keepdims=True)
    return centred * lax.rsqrt(spread + NORM_EPSILON) * gain_vec + bias_vec


def softplus_of_minus(d):
    u = jnp.exp(-jnp.abs(d))
    s = u / (2.0 + u)
    q = s * s
    series = jnp.full_like(s, 1.0 / 15.0)
    for odd in (13, 11, 9, 7, 5, 3, 1):
        series = series * q + 1.0 / odd
    return jnp.maximum(-d, 0.0) + 2.0 * s * series


def minus_expm1(z):
    series = jnp.full_like(z, 1.0 / 40320.0)
    for factor in (5040.0, 720.0, 120.0, 24.0, 6.0, 2.0, 1.0):
        series = series * z + 1.0 / factor
    return jnp.where(z > -0.25, -z * series, 1.0 - jnp.exp(z))


def dot(a, b):
    return jnp.dot(a, b, preferred_element_type=F32)


def mega(
    stream_h, rec_h, gatein_h, taps_h, small_gates_h, large_gates_h, decay_h, extra_h,
    wout_h, gain1_h, bias1_h, index_h, weight_h, gate_w_h, up_w_h, down_w_h,
    shared_gate_h, shared_up_h, shared_down_h, gain2_h, bias2_h,
    out_ref,
    stream, rec, gatein, taps, small_gates, large_gates, decay, extra_raw,
    wout, gain1, bias1, index, weight, own_gate, own_up, own_down,
    shared_gate, shared_up, shared_down, gain2, bias2,
    gate_up, down_w,
    extra, turned, rec_f, border, cum_p, cum_s, carry1, carry2, gelu_buf, branch,
    part, mixed_buf, normed, slot_buf, weight_buf,
    disp, arr1, disp2, arr2, moe_out, ret1, ret1p, ret2, acc,
    load_sem, slot_sem, border_sem, part_sem, part_out_sem, carry_sem, plane_sem, mix_sem,
    z_sem, p_sem, last_sem, out_sem,
):
    sp = lax.axis_index("sp")
    tp = lax.axis_index("tp")
    zi = sp // PLANE
    pi = sp % PLANE
    xi = pi // 2
    core = sp % 2
    hosted = tp // 2
    mirror = 3 - tp
    mate = tp + 1 - 2 * (tp % 2)
    far = 3 - mate
    place = xi * 2 + hosted
    owner = core == hosted
    guest = core != hosted
    phase = Phases()
    phase("loads")

    def remote(src, dst, send_sem, recv_sem, sp_to, tp_to):
        return pltpu.make_async_remote_copy(
            src_ref=src,
            dst_ref=dst,
            send_sem=send_sem,
            recv_sem=recv_sem,
            device_id={"sp": sp_to, "tp": tp_to},
            device_id_type=MESH,
        )

    def send(*args, when=None):
        copy = remote(*args)
        if when is None:
            copy.start()
        else:
            pl.when(when)(copy.start)

    def came(ref, sem):
        remote(ref, ref, sem, sem, sp, tp).wait_recv()

    def left(ref, sem):
        remote(ref, ref, sem, sem, sp, tp).wait_send()

    def plane_peer(d):
        return zi * PLANE + (pi + d) % PLANE

    def z_peer(d):
        return ((zi + d) % PLANES) * PLANE + pi

    barrier = pltpu.get_barrier_semaphore()

    def greet(sp_to, tp_to):
        pl.semaphore_signal(
            barrier, inc=1, device_id={"sp": sp_to, "tp": tp_to}, device_id_type=MESH
        )

    for d in FAR_FIRST:
        greet(z_peer(d), tp)
    for d in FAR_FIRST:
        greet(plane_peer(d), tp)
    for d in range(1, TPS):
        greet(sp, (tp + d) % TPS)
    greet((sp + 63) % 64, tp)
    for j in range(PLANE):
        greet(zi * PLANE + j, mirror)
    for d in FAR_FIRST:
        greet(z_peer(d) + 1 - 2 * core, tp)

    names = (
        (rec_h, rec), (small_gates_h, small_gates), (large_gates_h, large_gates), (taps_h, taps),
        (decay_h, decay), (extra_h, extra_raw), (gatein_h, gatein), (gate_w_h, own_gate),
        (up_w_h, own_up), (down_w_h, own_down), (wout_h, wout), (index_h, index),
        (weight_h, weight), (stream_h, stream), (gain1_h, gain1), (bias1_h, bias1),
        (shared_gate_h, shared_gate), (shared_up_h, shared_up), (shared_down_h, shared_down),
        (gain2_h, gain2), (bias2_h, bias2),
    )
    loads = []
    for k, (src, dst) in enumerate(names):
        loads.append(pltpu.make_async_copy(src, dst, load_sem.at[k]))
        loads[-1].start()
    wholes = (gate_up.at[0], gate_up.at[1], down_w)
    owns = (own_gate, own_up, own_down)
    slot_loads = [
        pltpu.make_async_copy(src, dst.at[tp], slot_sem.at[m])
        for m, (src, dst) in enumerate(zip((gate_w_h, up_w_h, down_w_h), wholes))
    ]

    @pl.when(owner)
    def _():
        for copy in slot_loads:
            copy.start()

    phase("wait_loads")
    length = rec.shape[0]
    loads[0].wait()
    phase("barrier")
    pl.semaphore_wait(barrier, 7 + 7 + 3 + 1 + 8 + 7)
    phase("send_gate")
    border_out = rec.at[length - HEAD_ROWS :]
    send(border_out, border, border_sem.at[0], border_sem.at[1], (sp + 1) % 64, tp)

    FROM_MATE, FROM_MIRROR, FROM_FAR = range(3)
    origin = {FROM_MATE: mate, FROM_MIRROR: mirror, FROM_FAR: far}

    def piece_of(ref, k, lead=()):
        if k < 4:
            return ref.at[(*lead, slice(1024 * (k % 2), 1024 * (k % 2) + 1024))]
        return ref.at[(*lead, slice(None), slice(512 * (k - 4), 512 * (k - 4) + 512))]

    def buffer_of(k):
        return k // 2 if k < 4 else 2

    def held_piece(k, at):
        return piece_of(wholes[buffer_of(k)], k, (at,))

    def across(src, k, at, kind, tp_to, when):
        out = part_out_sem.at[int(k >= 4)]
        send(src, held_piece(k, at), out, part_sem.at[kind, k], sp, tp_to, when=when)

    def own_out(k):
        src = piece_of(owns[buffer_of(k)], k)
        across(src, k, tp, FROM_MATE, mate, owner)

    def own_mirror(k):
        src = piece_of(owns[buffer_of(k)], k)
        across(src, k, tp, FROM_MIRROR, mirror, guest)

    def held(k, kind):
        came(held_piece(k, origin[kind]), part_sem.at[kind, k])

    def relay(k):
        @pl.when(owner)
        def _():
            held(k, FROM_MIRROR)

        across(held_piece(k, mirror), k, mirror, FROM_FAR, mate, owner)

    for k in (7, 8):
        loads[k].wait()
    for k in (0, 1, 2, 3):
        own_out(k)
        own_mirror(k)

    phase("prepare")
    for k in range(1, 6):
        loads[k].wait()
    for g in range(2):
        rec_f[HEAD_ROWS:, 256 * g : 256 * g + 256] = rec[:, g, :].astype(F32)
        extra[:, 256 * g : 256 * g + 256] = extra_raw[:, g, :]
    row_i = lax.broadcasted_iota(jnp.int32, (64, 128), 0)
    col_i = lax.broadcasted_iota(jnp.int32, (64, 128), 1)
    put_low = (row_i == col_i).astype(BF16)
    put_high = (row_i + 64 == col_i).astype(BF16)
    blocks = []
    for which in range(2):
        maps = []
        for pair in range(2):
            low = dot(small_gates[which, 2 * pair], put_low)
            high = dot(small_gates[which, 2 * pair + 1], put_high)
            maps.append(jnp.concatenate([low, high], axis=0).astype(BF16))
        for head in range(2):
            maps.append(large_gates[which, head])
        blocks.append(maps)
    rate = -8.0 * softplus_of_minus(decay[...])
    tap_f = taps[...].astype(F32)

    def tap(k, b):
        return tap_f[k, b // 2 : b // 2 + 1, 128 * (b % 2) : 128 * (b % 2) + 128]

    def scanned(first, count):
        for b in range(4):
            lanes = slice(128 * b, 128 * b + 128)
            conv = tap(0, b) * rec_f[first + HEAD_ROWS - 3 : first + HEAD_ROWS - 3 + count, lanes]
            for k in range(1, 4):
                at = first + HEAD_ROWS - 3 + k
                conv = conv + tap(k, b) * rec_f[at : at + count, lanes]
            conv = conv.astype(BF16)
            recur_gate = jax.nn.sigmoid(dot(conv, blocks[0][b]))
            input_gate = jax.nn.sigmoid(dot(conv, blocks[1][b]))
            log_decay = recur_gate * rate[b // 2 : b // 2 + 1, 128 * (b % 2) : 128 * (b % 2) + 128] + extra[first : first + count, lanes]
            p = jnp.exp(log_decay)
            s = jnp.sqrt(minus_expm1(2.0 * log_decay)) * input_gate * conv.astype(F32)
            p = p.reshape(count // 8, 8, 128)
            s = s.reshape(count // 8, 8, 128)
            row = lax.broadcasted_iota(jnp.int32, (count // 8, 8, 128), 1)
            for by in (1, 2, 4):
                p_prev = pltpu.roll(p, by, 1)
                s_prev = pltpu.roll(s, by, 1)
                s = jnp.where(row >= by, p * s_prev + s, s)
                p = jnp.where(row >= by, p * p_prev, p)
            p_in = jnp.ones((1, 128), F32)
            s_in = jnp.zeros((1, 128), F32)
            for t in range(count // 8):
                s_t = s[t] + p[t] * s_in
                p_t = p[t] * p_in
                cum_s[first + 8 * t : first + 8 * t + 8, lanes] = s_t
                cum_p[first + 8 * t : first + 8 * t + 8, lanes] = p_t
                s_in = s_t[7:8]
                p_in = p_t[7:8]

    phase("scan_tail")
    scanned(HEAD_ROWS, length - HEAD_ROWS)
    loads[9].wait()
    phase("border")
    came(border, border_sem.at[1])
    phase("scan_head")
    for g in range(2):
        border_f = border[:, g, :].astype(F32)
        rec_f[0:HEAD_ROWS, 256 * g : 256 * g + 256] = jnp.where(
            sp > 0, border_f, jnp.zeros_like(border_f)
        )
    scanned(0, HEAD_ROWS)

    head_p = cum_p[HEAD_ROWS - 1 : HEAD_ROWS, :]
    head_s = cum_s[HEAD_ROWS - 1 : HEAD_ROWS, :]
    tail_p = cum_p[length - 1 : length, :]
    tail_s = cum_s[length - 1 : length, :]
    total_p = head_p * tail_p
    total_s = tail_p * head_s + tail_s
    mine1 = carry1.at[pi]
    for b in range(4):
        mine1[0, b : b + 1, :] = total_p[:, 128 * b : 128 * b + 128]
        mine1[1, b : b + 1, :] = total_s[:, 128 * b : 128 * b + 128]
    for d in FAR_FIRST:
        send(mine1, mine1, carry_sem.at[0], carry_sem.at[1], plane_peer(d), tp)

    phase("slots")
    for k in (6, 11, 12):
        loads[k].wait()
    own_rows = pl.ds(pl.multiple_of(tp * 32, 32), 32)
    unused = jnp.zeros((4, 128), F32)
    turned[0] = jnp.concatenate([index[...].astype(F32), unused], axis=0).T
    turned[1] = jnp.concatenate([weight[...], unused], axis=0).T
    ids = turned[0, own_rows, :].astype(jnp.int32)
    factors = turned[1, own_rows, :]
    slot = lax.broadcasted_iota(jnp.int32, (32, 128), 1)
    named = jnp.zeros((32, 128), F32)
    scaled = jnp.zeros((32, 128), F32)
    for k in range(4):
        hit = ids[:, k : k + 1] == slot // 2
        named = named + jnp.where(hit, 1.0, 0.0)
        scaled = scaled + jnp.where(hit, factors[:, k : k + 1], 0.0)
    below = lax.broadcasted_iota(jnp.int32, (32, 32), 0) > lax.broadcasted_iota(
        jnp.int32, (32, 32), 1
    )
    earlier = dot(below.astype(BF16), named.astype(BF16))
    right_slot = jnp.abs(earlier - (slot % 2).astype(F32)) < 0.5
    to_row = lax.broadcasted_iota(jnp.int32, (128, 128), 0)
    from_row = lax.broadcasted_iota(jnp.int32, (128, 128), 1)
    outer, inner, pair = to_row // 16, (to_row // 2) % 8, to_row % 2
    pick = (from_row == inner * 16 + outer * 2 + pair).astype(BF16)
    slot_rows = jnp.where(right_slot, named, 0.0).T.astype(BF16)
    slot_buf[0] = slot_rows
    slot_buf[1] = dot(pick, slot_rows).astype(BF16)
    scaled = jnp.where(right_slot, scaled, 0.0)
    high = scaled.astype(BF16)
    low = (scaled - high.astype(F32)).astype(BF16)
    for part_no, values in enumerate((high, low)):
        weight_buf[part_no] = dot(values, pick).astype(BF16)
        weight_buf[2 + part_no] = values
    for g in range(2):
        gelu_buf[:, 256 * g : 256 * g + 256] = jax.nn.gelu(gatein[:, g, :].astype(F32))
    phase("carry1")

    came(carry1.at[0:7], carry_sem.at[1])
    one = jnp.ones((4, 128), F32)
    nought = jnp.zeros((4, 128), F32)
    all_p, all_s, in_p, in_s = one, nought, one, nought
    for j in range(PLANE):
        p_j, s_j = carry1[j, 0], carry1[j, 1]
        all_p, all_s = all_p * p_j, p_j * all_s + s_j
        in_p = jnp.where(j < pi, in_p * p_j, in_p)
        in_s = jnp.where(j < pi, p_j * in_s + s_j, in_s)
    mine2 = carry2.at[zi]
    mine2[0] = all_p
    mine2[1] = all_s
    for d in (4, 3, 5, 2, 6, 1, 7):
        send(
            mine2,
            mine2,
            plane_sem.at[0, d - 1],
            plane_sem.at[1, d - 1],
            z_peer(d),
            tp,
            when=zi + d < PLANES,
        )
    phase("carry2")
    for d in range(1, PLANES):
        got = carry2.at[(zi + PLANES - d) % PLANES]

        @pl.when(zi >= d)
        def _():
            came(got, plane_sem.at[1, d - 1])

    phase("fixup")
    planes_s = nought
    for k in range(PLANES):
        planes_s = jnp.where(k < zi, carry2[k, 0] * planes_s + carry2[k, 1], planes_s)
    carry_in = in_p * planes_s + in_s
    carry_row = jnp.concatenate([carry_in[b : b + 1] for b in range(4)], axis=1)
    carry_tail = head_s + head_p * carry_row
    states = cum_s[:HEAD_ROWS] + cum_p[:HEAD_ROWS] * carry_row
    branch[:HEAD_ROWS, :] = (gelu_buf[:HEAD_ROWS] * states).astype(BF16)
    states = cum_s[HEAD_ROWS:] + cum_p[HEAD_ROWS:] * carry_tail
    branch[HEAD_ROWS:, :] = (gelu_buf[HEAD_ROWS:] * states).astype(BF16)

    phase("out_proj")
    loads[10].wait()
    for c in range(4):
        cols = slice(512 * c, 512 * c + 512)
        value = dot(branch[...], wout[:, cols]).astype(BF16)
        part[:, :, cols] = value.reshape(TPS, 32, 512)
        for d in (2, 1, 3):
            to = (tp + d) % TPS
            lands = mixed_buf.at[tp, :, cols]
            send(part.at[to, :, cols], lands, mix_sem.at[0], mix_sem.at[1], sp, to)
    phase("gate_arrive")
    for k in (0, 1, 2, 3):
        relay(k)
    own_out(4)
    phase("mix_arrive")
    for k in (13, 14, 15):
        loads[k].wait()
    came(mixed_buf.at[0:3], mix_sem.at[1])
    phase("norm1")
    mixed = part[tp].astype(F32)
    for d in (1, 2, 3):
        mixed = mixed + mixed_buf[(tp + d) % TPS].astype(F32)
    normed[...] = layer_norm(
        RESIDUAL_SCALE * stream[...].astype(F32) + mixed, gain1[...], bias1[...]
    ).astype(BF16)

    width = 2048 // CHUNKS

    def cols_of(c):
        return slice(width * c, width * c + width)

    def z_out(src, dst, trip, c, out):
        cols = cols_of(c)
        for d in FAR_FIRST:
            to = (zi + d) % PLANES
            lands = dst.at[zi, :, cols]
            send(src.at[to, :, cols], lands, out_sem.at[out], z_sem.at[trip, c], z_peer(d), tp)
        dst[zi, :, cols] = src[zi, :, cols]

    def by_role(ref_of, sem):
        @pl.when(owner)
        def _():
            came(ref_of(slice(0, 7)), sem)

        @pl.when(guest)
        def _():
            came(ref_of(slice(0, 8)), sem)

    def plane_out(src, c, first):
        cols = cols_of(c)
        for dx in (2, 1, 3, 0):
            x_to = (xi + dx) % 4
            for other in (1, 0):
                expert = hosted + other * (1 - 2 * hosted)
                if first:
                    core_to, lands = hosted, arr1.at[pi, :, cols]
                    recv = p_sem.at[0, c]
                else:
                    core_to, lands = expert, arr2.at[other, pi, :, cols]
                    recv = last_sem.at[other, c]
                send(
                    src.at[x_to * 2 + expert, :, cols],
                    lands,
                    out_sem.at[1 if first else 2],
                    recv,
                    zi * PLANE + x_to * 2 + core_to,
                    mirror if other else tp,
                    when=guest if dx == 0 and other == 0 else None,
                )

        @pl.when(owner)
        def _():
            if first:
                arr1[pi, :, cols] = src[pi, :, cols]
            else:
                arr2[0, pi, :, cols] = src[pi, :, cols]

    def z_to_expert(src, c):
        cols = cols_of(c)
        group = jnp.where(owner, 0, 1)
        for d in (*FAR_FIRST, 0):
            to = (zi + d) % PLANES
            send(
                src.at[to, :, cols],
                arr2.at[group, zi, :, cols],
                out_sem.at[3],
                last_sem.at[group, c],
                to * PLANE + place,
                tp,
                when=guest if d == 0 else None,
            )

        @pl.when(owner)
        def _():
            arr2[0, zi, :, cols] = src[zi, :, cols]

    def expert_to_z(c):
        cols = cols_of(c)
        for d in (*FAR_FIRST, 0):
            to = (zi + d) % PLANES
            for group in (0, 1):
                if d == 0 and group == 0:
                    ret1[zi, :, cols] = moe_out[0, zi, :, cols]
                    continue
                remote(
                    moe_out.at[group, to, :, cols],
                    ret1.at[zi, :, cols],
                    out_sem.at[4 + group],
                    z_sem.at[1, c],
                    to * PLANE + place + group * (1 - 2 * hosted),
                    tp,
                ).start()

    def expert_to_plane(c):
        cols = cols_of(c)
        for d in (*FAR_FIRST, 0):
            j = (pi + d) % PLANE
            for group in (1, 0):
                if d == 0 and group == 0:
                    ret1[pi, :, cols] = moe_out[0, pi, :, cols]
                    continue
                remote(
                    moe_out.at[group, j, :, cols],
                    ret1.at[place, :, cols],
                    out_sem.at[6 + group],
                    p_sem.at[1, c],
                    zi * PLANE + j,
                    mirror if group else tp,
                ).start()

    home = jnp.where(owner, tp, mirror)

    def plane_back(src, dst, c):
        cols = cols_of(c)
        for dx in (2, 1, 3, 0):
            for target_core in (0, 1):
                j = ((xi + dx) % 4) * 2 + target_core
                send(
                    src.at[j, :, cols],
                    dst.at[place, :, cols],
                    out_sem.at[8],
                    p_sem.at[1, c],
                    zi * PLANE + j,
                    home,
                    when=jnp.logical_or(guest, core != target_core) if dx == 0 else None,
                )

        @pl.when(owner)
        def _():
            dst[pi, :, cols] = src[pi, :, cols]

    def permuted(rows):
        return dot(pick, rows).astype(BF16)

    def swapped(src, c):
        rows = src[:, :, cols_of(c)].reshape(128, width)
        return dot(pick, rows).astype(BF16).reshape(8, 16, width)

    Z_FIRST = tuple(range(CHUNKS // 2))
    P_FIRST = tuple(range(CHUNKS // 2, CHUNKS))
    for c in (*Z_FIRST, *P_FIRST):
        cols = cols_of(c)
        order = int(c in P_FIRST)
        value = dot(slot_buf[order], normed[:, cols]).astype(BF16)
        disp[:, :, cols] = value.reshape(8, 16, width)
        if c in Z_FIRST:
            z_out(disp, arr1, 0, c, 0)
        else:
            plane_out(disp, c, True)
    for k in (4, 5, 6, 7):
        own_mirror(k)
    phase("shared")
    for k in (16, 17, 18, 19, 20):
        loads[k].wait()
    rows = normed[...]
    hidden = jax.nn.silu(dot(rows, shared_gate[...])) * dot(rows, shared_up[...])
    acc[...] = RESIDUAL_SCALE * rows.astype(F32) + dot(hidden.astype(BF16), shared_down[...])

    for c in P_FIRST:
        phase(f"disp_p1_{c}")
        by_role(lambda blocks: arr1.at[blocks, :, cols_of(c)], p_sem.at[0, c])
        phase(f"disp_swap_{c}")
        disp2[:, :, cols_of(c)] = swapped(arr1, c)
        z_to_expert(disp2, c)
    for c in Z_FIRST:
        phase(f"disp_z1_{c}")
        came(arr1.at[0:7, :, cols_of(c)], z_sem.at[0, c])
        phase(f"disp_swap_{c}")
        disp2[:, :, cols_of(c)] = swapped(arr1, c)
        plane_out(disp2, c, False)
        phase(f"relay_{c}")
        for k in range(4 + 2 * c, 6 + 2 * c):
            relay(k)
            if k < 7:
                own_out(k + 1)
    phase()

    @pl.when(owner)
    def _():
        phase("weights")
        for copy in slot_loads:
            copy.wait()
        for kind in (FROM_MATE, FROM_FAR):
            for k in (0, 1, 2, 3):
                held(k, kind)
        both = None
        for c in [c for both_kinds in zip(Z_FIRST, P_FIRST) for c in both_kinds]:
            cols = cols_of(c)
            phase(f"disp_2_{c}")
            came(arr2.at[0, 0:7, :, cols], last_sem.at[0, c])
            came(arr2.at[1, :, :, cols], last_sem.at[1, c])
            phase(f"gate_up_{c}")
            groups = [arr2[g, :, :, cols].reshape(128, width) for g in (0, 1)]
            if c in P_FIRST:
                groups = [permuted(rows) for rows in groups]
            picked = jnp.concatenate(groups, axis=0)
            terms = [
                dot(picked, jnp.concatenate([gate_up[0, k, cols], gate_up[1, k, cols]], axis=1))
                for k in range(TPS)
            ]
            both = terms if both is None else [x + y for x, y in zip(both, terms)]
        phase("hidden")
        hidden = jnp.concatenate(
            [(jax.nn.silu(x[:, :128]) * x[:, 128:]).astype(BF16) for x in both], axis=1
        )
        by_plane = hidden
        by_z = jnp.concatenate([permuted(hidden[:128]), permuted(hidden[128:])], axis=0)
        for c in range(CHUNKS):
            cols = cols_of(c)
            phase(f"down_arrive_{c}")
            held(4 + c, FROM_MATE)
            held(4 + c, FROM_FAR)
            phase(f"down_{c}")
            rows = by_z if c in Z_FIRST else by_plane
            value = dot(rows, down_w[:, :, cols].reshape(512, width)).astype(BF16)
            moe_out[:, :, :, cols] = value.reshape(2, 8, 16, width)
            if c in Z_FIRST:
                expert_to_z(c)
            else:
                expert_to_plane(c)
        phase()

    for c in range(CHUNKS):
        phase(f"ret_1_{c}")
        sem = z_sem.at[1, c] if c in Z_FIRST else p_sem.at[1, c]
        by_role(lambda blocks: ret1.at[blocks, :, cols_of(c)], sem)
        phase(f"ret_swap_{c}")
        ret1p[:, :, cols_of(c)] = swapped(ret1, c)
        if c in Z_FIRST:
            plane_back(ret1p, ret2, c)
        else:
            z_out(ret1p, ret2, 1, c, 9)
    for c in range(CHUNKS):
        cols = cols_of(c)
        phase(f"ret_2_{c}")
        if c in Z_FIRST:
            by_role(lambda blocks: ret2.at[blocks, :, cols], p_sem.at[1, c])
        else:
            came(ret2.at[0:7, :, cols], z_sem.at[1, c])
        phase(f"combine_{c}")
        back = ret2[:, :, cols].reshape(128, width)
        order = 0 if c in Z_FIRST else 2
        acc[:, cols] = (
            acc[:, cols] + dot(weight_buf[order], back) + dot(weight_buf[order + 1], back)
        )
    phase("norm2")
    out_ref[...] = layer_norm(acc[...], gain2[...], bias2[...]).astype(BF16)
    phase("drain")
    left(border_out, border_sem.at[0])
    left(carry1.at[0:7], carry_sem.at[0])
    for d in range(1, PLANES):

        @pl.when(zi + d < PLANES)
        def _():
            left(mine2, plane_sem.at[0, d - 1])

    left(part.at[0:3], mix_sem.at[0])
    half = slice(0, 1024)
    seven, eight = disp.at[0:7, :, half], disp.at[:, :, half]
    for k in (0, 9):
        left(seven, out_sem.at[k])

    @pl.when(owner)
    def _():
        for k in (1, 2, 3, 4, 6, 8):
            left(seven, out_sem.at[k])
        for k in (5, 7):
            left(eight, out_sem.at[k])
        left(gate_up.at[:, 0:2], part_out_sem.at[0])
        left(down_w.at[0:2], part_out_sem.at[1])

    @pl.when(guest)
    def _():
        for k in (1, 2, 3, 8):
            left(eight, out_sem.at[k])
        left(gate_up.at[0, 0:2], part_out_sem.at[0])
        left(down_w.at[0], part_out_sem.at[1])

    phase()


def shards(
    stream, recurrence_input, output_gate_input, convolution_taps, first_group_gates,
    second_group_gates, channel_decay, position_log_extra, recurrence_output_weight,
    first_norm_gain, first_norm_bias, routed_expert_index, routed_expert_weight,
    routed_gate_weight, routed_up_weight, routed_down_weight, shared_gate_weight,
    shared_up_weight, shared_down_weight, second_norm_gain, second_norm_bias,
):
    operands = (
        stream,
        recurrence_input,
        output_gate_input,
        convolution_taps,
        first_group_gates,
        second_group_gates,
        channel_decay,
        position_log_extra,
        recurrence_output_weight.reshape(512, 2048),
        first_norm_gain.reshape(1, 2048),
        first_norm_bias.reshape(1, 2048),
        routed_expert_index.T,
        routed_expert_weight.T,
        routed_gate_weight.reshape(2048, 128),
        routed_up_weight.reshape(2048, 128),
        routed_down_weight.reshape(128, 2048),
        shared_gate_weight,
        shared_up_weight,
        shared_down_weight,
        second_norm_gain.reshape(1, 2048),
        second_norm_bias.reshape(1, 2048),
    )
    held = [pltpu.VMEM(operand.shape, operand.dtype) for operand in operands]
    wide = pltpu.VMEM((8, 16, 2048), BF16)
    return pl.pallas_call(
        mega,
        out_shape=jax.ShapeDtypeStruct((32, 2048), BF16),
        in_specs=[pl.BlockSpec(memory_space=pl.ANY)] * len(operands),
        out_specs=pl.BlockSpec(memory_space=pltpu.VMEM),
        scratch_shapes=[
            *held,
            pltpu.VMEM((2, TPS, 2048, 128), BF16),
            pltpu.VMEM((TPS, 128, 2048), BF16),
            pltpu.VMEM((128, 512), F32),
            pltpu.VMEM((2, 128, 8), F32),
            pltpu.VMEM((128 + HEAD_ROWS, 512), F32),
            pltpu.VMEM((HEAD_ROWS, 2, 256), BF16),
            pltpu.VMEM((128, 512), F32),
            pltpu.VMEM((128, 512), F32),
            pltpu.VMEM((PLANE, 2, 4, 128), F32),
            pltpu.VMEM((PLANES, 2, 4, 128), F32),
            pltpu.VMEM((128, 512), F32),
            pltpu.VMEM((128, 512), BF16),
            pltpu.VMEM((TPS, 32, 2048), BF16),
            pltpu.VMEM((TPS, 32, 2048), BF16),
            pltpu.VMEM((32, 2048), BF16),
            pltpu.VMEM((2, 128, 32), BF16),
            pltpu.VMEM((4, 32, 128), BF16),
            wide, wide, wide,
            pltpu.VMEM((2, 8, 16, 2048), BF16),
            pltpu.VMEM((2, 8, 16, 2048), BF16),
            wide, wide, wide,
            pltpu.VMEM((32, 2048), F32),
            pltpu.SemaphoreType.DMA((len(operands),)),
            pltpu.SemaphoreType.DMA((3,)),
            pltpu.SemaphoreType.DMA((2,)),
            pltpu.SemaphoreType.DMA((3, 8)),
            pltpu.SemaphoreType.DMA((2,)),
            pltpu.SemaphoreType.DMA((2,)),
            pltpu.SemaphoreType.DMA((2, 7)),
            pltpu.SemaphoreType.DMA((2,)),
            pltpu.SemaphoreType.DMA((2, CHUNKS)),
            pltpu.SemaphoreType.DMA((2, CHUNKS)),
            pltpu.SemaphoreType.DMA((2, CHUNKS)),
            pltpu.SemaphoreType.DMA((10,)),
        ],
        compiler_params=pltpu.CompilerParams(
            collective_id=0, has_side_effects=True, vmem_limit_bytes=56 * 2**20
        ),
        name="mega",
    )(*operands)


def solution(mesh):
    in_specs = (
        P(("sp", "tp"), None),
        P("sp", None, "tp"),
        P("sp", None, "tp"),
        P(None, None, "tp"),
        P(None, "tp", None, None),
        P(None, "tp", None, None),
        P(None, "tp"),
        P("sp", None, "tp"),
        P(None, "tp", None),
        P(),
        P(),
        P("sp", None),
        P("sp", None),
        P("sp", None, "tp"),
        P("sp", None, "tp"),
        P("sp", "tp", None),
        P(),
        P(),
        P(),
        P(),
        P(),
    )
    out_specs = P(("sp", "tp"), None)
    return jax.shard_map(shards, mesh=mesh, in_specs=in_specs, out_specs=out_specs, check_vma=False)
```

```python
import jax
import jax.numpy as jnp
from jax import lax
from jax.experimental import pallas as pl
from jax.experimental.pallas import tpu as pltpu
from jax.sharding import PartitionSpec as P

RESIDUAL_SCALE = 8.0**0.25
NORM_EPSILON = 1e-05
MESH = pl.DeviceIdType.MESH
F32 = jnp.float32
BF16 = jnp.bfloat16

PLANE = 8
PLANES = 8
TPS = 4
HEAD_ROWS = 16
CHUNKS = 4
BACK = (
    (slice(0, 512), "z"),
    (slice(512, 1024), "z"),
    (slice(1024, 1280), "z"),
    (slice(1280, 1536), "plane"),
    (slice(1536, 1792), "plane"),
    (slice(1792, 2048), "plane"),
)
PIECES = 4 + len(BACK)
FAR_FIRST = (4, 3, 5, 2, 6, 1, 7)


class Phases:
    def __init__(self):
        self.scope = None

    def __call__(self, name=None):
        if self.scope is not None:
            self.scope.__exit__(None, None, None)
        self.scope = None
        if name is not None:
            self.scope = jax.named_scope(name)
            self.scope.__enter__()


def layer_norm(values, gain_vec, bias_vec):
    row_mean = jnp.mean(values, axis=-1, keepdims=True)
    centred = values - row_mean
    spread = jnp.mean(jnp.square(centred), axis=-1, keepdims=True)
    return centred * lax.rsqrt(spread + NORM_EPSILON) * gain_vec + bias_vec


def softplus_of_minus(d):
    u = jnp.exp(-jnp.abs(d))
    s = u / (2.0 + u)
    q = s * s
    series = jnp.full_like(s, 1.0 / 15.0)
    for odd in (13, 11, 9, 7, 5, 3, 1):
        series = series * q + 1.0 / odd
    return jnp.maximum(-d, 0.0) + 2.0 * s * series


def minus_expm1(z):
    series = jnp.full_like(z, 1.0 / 40320.0)
    for factor in (5040.0, 720.0, 120.0, 24.0, 6.0, 2.0, 1.0):
        series = series * z + 1.0 / factor
    return jnp.where(z > -0.25, -z * series, 1.0 - jnp.exp(z))


def dot(a, b):
    return jnp.dot(a, b, preferred_element_type=F32)


def mega(
    stream_h, rec_h, gatein_h, taps_h, small_gates_h, large_gates_h, decay_h, extra_h,
    wout_h, gain1_h, bias1_h, index_h, weight_h, gate_w_h, up_w_h, down_w_h,
    shared_gate_h, shared_up_h, shared_down_h, gain2_h, bias2_h,
    out_ref,
    stream, rec, gatein, taps, small_gates, large_gates, decay, extra_raw,
    wout, gain1, bias1, index, weight, own_gate, own_up, own_down,
    shared_gate, shared_up, shared_down, gain2, bias2,
    gate_up, down_w,
    extra, turned, rec_f, border, cum_p, cum_s, carry1, carry2, gelu_buf, branch,
    part, mixed_buf, normed, slot_buf, weight_buf,
    disp, arr1, disp2, arr2, moe_out, ret1, ret1p, ret2, acc,
    load_sem, slot_sem, border_sem, part_sem, part_out_sem, carry_sem, plane_sem, mix_sem,
    first_sem, last_sem, back_sem, out_sem,
):
    sp = lax.axis_index("sp")
    tp = lax.axis_index("tp")
    zi = sp // PLANE
    pi = sp % PLANE
    xi = pi // 2
    core = sp % 2
    hosted = tp // 2
    mirror = 3 - tp
    mate = tp + 1 - 2 * (tp % 2)
    far = 3 - mate
    place = xi * 2 + hosted
    owner = core == hosted
    guest = core != hosted
    phase = Phases()
    phase("loads")

    def remote(src, dst, send_sem, recv_sem, sp_to, tp_to):
        return pltpu.make_async_remote_copy(
            src_ref=src,
            dst_ref=dst,
            send_sem=send_sem,
            recv_sem=recv_sem,
            device_id={"sp": sp_to, "tp": tp_to},
            device_id_type=MESH,
        )

    def send(*args, when=None):
        copy = remote(*args)
        if when is None:
            copy.start()
        else:
            pl.when(when)(copy.start)

    def came(ref, sem):
        remote(ref, ref, sem, sem, sp, tp).wait_recv()

    def left(ref, sem):
        remote(ref, ref, sem, sem, sp, tp).wait_send()

    def plane_peer(d):
        return zi * PLANE + (pi + d) % PLANE

    def z_peer(d):
        return ((zi + d) % PLANES) * PLANE + pi

    barrier = pltpu.get_barrier_semaphore()

    def greet(sp_to, tp_to):
        pl.semaphore_signal(
            barrier, inc=1, device_id={"sp": sp_to, "tp": tp_to}, device_id_type=MESH
        )

    for d in FAR_FIRST:
        greet(z_peer(d), tp)
    for d in FAR_FIRST:
        greet(plane_peer(d), tp)
    for d in range(1, TPS):
        greet(sp, (tp + d) % TPS)
    greet((sp + 63) % 64, tp)
    for j in range(PLANE):
        greet(zi * PLANE + j, mirror)
    for d in FAR_FIRST:
        greet(z_peer(d) + 1 - 2 * core, tp)

    names = (
        (rec_h, rec), (small_gates_h, small_gates), (large_gates_h, large_gates), (taps_h, taps),
        (decay_h, decay), (extra_h, extra_raw), (gatein_h, gatein), (gate_w_h, own_gate),
        (up_w_h, own_up), (down_w_h, own_down), (wout_h, wout), (index_h, index),
        (weight_h, weight), (stream_h, stream), (gain1_h, gain1), (bias1_h, bias1),
        (shared_gate_h, shared_gate), (shared_up_h, shared_up), (shared_down_h, shared_down),
        (gain2_h, gain2), (bias2_h, bias2),
    )
    loads = [pltpu.make_async_copy(src, dst, load_sem.at[k]) for k, (src, dst) in enumerate(names)]
    urgent = (0, 7, 8)
    for k in (*urgent, *(k for k in range(len(names)) if k not in urgent)):
        loads[k].start()
    wholes = (gate_up.at[0], gate_up.at[1], down_w)
    owns = (own_gate, own_up, own_down)
    slot_loads = [
        pltpu.make_async_copy(src, dst.at[tp], slot_sem.at[m])
        for m, (src, dst) in enumerate(zip((gate_w_h, up_w_h, down_w_h), wholes))
    ]

    @pl.when(owner)
    def _():
        for copy in slot_loads:
            copy.start()

    phase("wait_loads")
    length = rec.shape[0]
    loads[0].wait()
    phase("barrier")
    pl.semaphore_wait(barrier, 7 + 7 + 3 + 1 + 8 + 7)
    phase("send_gate")
    border_out = rec.at[length - HEAD_ROWS :]
    send(border_out, border, border_sem.at[0], border_sem.at[1], (sp + 1) % 64, tp)

    FROM_MATE, FROM_MIRROR, FROM_FAR = range(3)
    origin = {FROM_MATE: mate, FROM_MIRROR: mirror, FROM_FAR: far}

    def piece_of(ref, k, lead=()):
        if k < 4:
            return ref.at[(*lead, slice(1024 * (k % 2), 1024 * (k % 2) + 1024))]
        return ref.at[(*lead, slice(None), BACK[k - 4][0])]

    def buffer_of(k):
        return k // 2 if k < 4 else 2

    def held_piece(k, at):
        return piece_of(wholes[buffer_of(k)], k, (at,))

    def arrival(kind, k):
        return part_sem.at[kind, k if kind == FROM_MIRROR else max(k - 3, 0)]

    def across(src, k, at, kind, tp_to, when):
        out = part_out_sem.at[int(k >= 4)]
        send(src, held_piece(k, at), out, arrival(kind, k), sp, tp_to, when=when)

    def own_out(k):
        src = piece_of(owns[buffer_of(k)], k)
        across(src, k, tp, FROM_MATE, mate, owner)

    def own_mirror(k):
        src = piece_of(owns[buffer_of(k)], k)
        across(src, k, tp, FROM_MIRROR, mirror, guest)

    def held(k, kind):
        came(held_piece(k, origin[kind]), arrival(kind, k))

    def relay(k):
        @pl.when(owner)
        def _():
            held(k, FROM_MIRROR)

        across(held_piece(k, mirror), k, mirror, FROM_FAR, mate, owner)

    for k in (7, 8):
        loads[k].wait()
    for k in (0, 1, 2, 3):
        own_out(k)
        own_mirror(k)

    phase("prepare")
    for k in range(1, 6):
        loads[k].wait()
    for g in range(2):
        rec_f[HEAD_ROWS:, 256 * g : 256 * g + 256] = rec[:, g, :].astype(F32)
        extra[:, 256 * g : 256 * g + 256] = extra_raw[:, g, :]
    row_i = lax.broadcasted_iota(jnp.int32, (64, 128), 0)
    col_i = lax.broadcasted_iota(jnp.int32, (64, 128), 1)
    put_low = (row_i == col_i).astype(BF16)
    put_high = (row_i + 64 == col_i).astype(BF16)
    blocks = []
    for which in range(2):
        maps = []
        for pair in range(2):
            low = dot(small_gates[which, 2 * pair], put_low)
            high = dot(small_gates[which, 2 * pair + 1], put_high)
            maps.append(jnp.concatenate([low, high], axis=0).astype(BF16))
        for head in range(2):
            maps.append(large_gates[which, head])
        blocks.append(maps)
    rate = -8.0 * softplus_of_minus(decay[...])
    tap_f = taps[...].astype(F32)

    def tap(k, b):
        return tap_f[k, b // 2 : b // 2 + 1, 128 * (b % 2) : 128 * (b % 2) + 128]

    def scanned(first, count):
        for b in range(4):
            lanes = slice(128 * b, 128 * b + 128)
            conv = tap(0, b) * rec_f[first + HEAD_ROWS - 3 : first + HEAD_ROWS - 3 + count, lanes]
            for k in range(1, 4):
                at = first + HEAD_ROWS - 3 + k
                conv = conv + tap(k, b) * rec_f[at : at + count, lanes]
            conv = conv.astype(BF16)
            recur_gate = jax.nn.sigmoid(dot(conv, blocks[0][b]))
            input_gate = jax.nn.sigmoid(dot(conv, blocks[1][b]))
            log_decay = recur_gate * rate[b // 2 : b // 2 + 1, 128 * (b % 2) : 128 * (b % 2) + 128] + extra[first : first + count, lanes]
            p = jnp.exp(log_decay)
            s = jnp.sqrt(minus_expm1(2.0 * log_decay)) * input_gate * conv.astype(F32)
            p = p.reshape(count // 8, 8, 128)
            s = s.reshape(count // 8, 8, 128)
            row = lax.broadcasted_iota(jnp.int32, (count // 8, 8, 128), 1)
            for by in (1, 2, 4):
                p_prev = pltpu.roll(p, by, 1)
                s_prev = pltpu.roll(s, by, 1)
                s = jnp.where(row >= by, p * s_prev + s, s)
                p = jnp.where(row >= by, p * p_prev, p)
            p_in = jnp.ones((1, 128), F32)
            s_in = jnp.zeros((1, 128), F32)
            for t in range(count // 8):
                s_t = s[t] + p[t] * s_in
                p_t = p[t] * p_in
                cum_s[first + 8 * t : first + 8 * t + 8, lanes] = s_t
                cum_p[first + 8 * t : first + 8 * t + 8, lanes] = p_t
                s_in = s_t[7:8]
                p_in = p_t[7:8]

    phase("scan_tail")
    scanned(HEAD_ROWS, length - HEAD_ROWS)
    loads[9].wait()
    phase("border")
    came(border, border_sem.at[1])
    phase("scan_head")
    for g in range(2):
        border_f = border[:, g, :].astype(F32)
        rec_f[0:HEAD_ROWS, 256 * g : 256 * g + 256] = jnp.where(
            sp > 0, border_f, jnp.zeros_like(border_f)
        )
    scanned(0, HEAD_ROWS)

    head_p = cum_p[HEAD_ROWS - 1 : HEAD_ROWS, :]
    head_s = cum_s[HEAD_ROWS - 1 : HEAD_ROWS, :]
    tail_p = cum_p[length - 1 : length, :]
    tail_s = cum_s[length - 1 : length, :]
    total_p = head_p * tail_p
    total_s = tail_p * head_s + tail_s
    mine1 = carry1.at[pi]
    for b in range(4):
        mine1[0, b : b + 1, :] = total_p[:, 128 * b : 128 * b + 128]
        mine1[1, b : b + 1, :] = total_s[:, 128 * b : 128 * b + 128]
    for d in FAR_FIRST:
        send(mine1, mine1, carry_sem.at[0], carry_sem.at[1], plane_peer(d), tp)

    phase("slots")
    for k in (6, 11, 12):
        loads[k].wait()
    own_rows = pl.ds(pl.multiple_of(tp * 32, 32), 32)
    unused = jnp.zeros((4, 128), F32)
    turned[0] = jnp.concatenate([index[...].astype(F32), unused], axis=0).T
    turned[1] = jnp.concatenate([weight[...], unused], axis=0).T
    ids = turned[0, own_rows, :].astype(jnp.int32)
    factors = turned[1, own_rows, :]
    slot = lax.broadcasted_iota(jnp.int32, (32, 128), 1)
    named = jnp.zeros((32, 128), F32)
    scaled = jnp.zeros((32, 128), F32)
    for k in range(4):
        hit = ids[:, k : k + 1] == slot // 2
        named = named + jnp.where(hit, 1.0, 0.0)
        scaled = scaled + jnp.where(hit, factors[:, k : k + 1], 0.0)
    below = lax.broadcasted_iota(jnp.int32, (32, 32), 0) > lax.broadcasted_iota(
        jnp.int32, (32, 32), 1
    )
    earlier = dot(below.astype(BF16), named.astype(BF16))
    right_slot = jnp.abs(earlier - (slot % 2).astype(F32)) < 0.5
    to_row = lax.broadcasted_iota(jnp.int32, (128, 128), 0)
    from_row = lax.broadcasted_iota(jnp.int32, (128, 128), 1)
    outer, inner, pair = to_row // 16, (to_row // 2) % 8, to_row % 2
    pick = (from_row == inner * 16 + outer * 2 + pair).astype(BF16)
    slot_rows = jnp.where(right_slot, named, 0.0).T.astype(BF16)
    slot_buf[0] = slot_rows
    slot_buf[1] = dot(pick, slot_rows).astype(BF16)
    scaled = jnp.where(right_slot, scaled, 0.0)
    high = scaled.astype(BF16)
    low = (scaled - high.astype(F32)).astype(BF16)
    for part_no, values in enumerate((high, low)):
        weight_buf[part_no] = dot(values, pick).astype(BF16)
        weight_buf[2 + part_no] = values
    for g in range(2):
        gelu_buf[:, 256 * g : 256 * g + 256] = jax.nn.gelu(gatein[:, g, :].astype(F32))
    phase("carry1")

    came(carry1.at[0:7], carry_sem.at[1])
    one = jnp.ones((4, 128), F32)
    nought = jnp.zeros((4, 128), F32)
    all_p, all_s, in_p, in_s = one, nought, one, nought
    for j in range(PLANE):
        p_j, s_j = carry1[j, 0], carry1[j, 1]
        all_p, all_s = all_p * p_j, p_j * all_s + s_j
        in_p = jnp.where(j < pi, in_p * p_j, in_p)
        in_s = jnp.where(j < pi, p_j * in_s + s_j, in_s)
    mine2 = carry2.at[zi]
    mine2[0] = all_p
    mine2[1] = all_s
    for d in (4, 3, 5, 2, 6, 1, 7):
        send(
            mine2,
            mine2,
            plane_sem.at[0, d - 1],
            plane_sem.at[1, d - 1],
            z_peer(d),
            tp,
            when=zi + d < PLANES,
        )
    phase("carry2")
    for d in range(1, PLANES):
        got = carry2.at[(zi + PLANES - d) % PLANES]

        @pl.when(zi >= d)
        def _():
            came(got, plane_sem.at[1, d - 1])

    phase("fixup")
    planes_s = nought
    for k in range(PLANES):
        planes_s = jnp.where(k < zi, carry2[k, 0] * planes_s + carry2[k, 1], planes_s)
    carry_in = in_p * planes_s + in_s
    carry_row = jnp.concatenate([carry_in[b : b + 1] for b in range(4)], axis=1)
    carry_tail = head_s + head_p * carry_row
    states = cum_s[:HEAD_ROWS] + cum_p[:HEAD_ROWS] * carry_row
    branch[:HEAD_ROWS, :] = (gelu_buf[:HEAD_ROWS] * states).astype(BF16)
    states = cum_s[HEAD_ROWS:] + cum_p[HEAD_ROWS:] * carry_tail
    branch[HEAD_ROWS:, :] = (gelu_buf[HEAD_ROWS:] * states).astype(BF16)

    phase("out_proj")
    loads[10].wait()
    for c in range(4):
        cols = slice(512 * c, 512 * c + 512)
        value = dot(branch[...], wout[:, cols]).astype(BF16)
        part[:, :, cols] = value.reshape(TPS, 32, 512)
        for d in (2, 1, 3):
            to = (tp + d) % TPS
            lands = mixed_buf.at[tp, :, cols]
            send(part.at[to, :, cols], lands, mix_sem.at[0], mix_sem.at[1], sp, to)
    phase("gate_arrive")
    for k in (0, 1, 2, 3):
        relay(k)
    own_out(4)
    phase("mix_arrive")
    for k in (13, 14, 15):
        loads[k].wait()
    came(mixed_buf.at[0:3], mix_sem.at[1])
    phase("norm1")
    mixed = part[tp].astype(F32)
    for d in (1, 2, 3):
        mixed = mixed + mixed_buf[(tp + d) % TPS].astype(F32)
    normed[...] = layer_norm(
        RESIDUAL_SCALE * stream[...].astype(F32) + mixed, gain1[...], bias1[...]
    ).astype(BF16)

    width = 2048 // CHUNKS

    def cols_of(c):
        return slice(width * c, width * c + width)

    def z_out(src, dst, cols, out, recv):
        for d in FAR_FIRST:
            to = (zi + d) % PLANES
            lands = dst.at[zi, :, cols]
            send(src.at[to, :, cols], lands, out_sem.at[out], recv, z_peer(d), tp)
        dst[zi, :, cols] = src[zi, :, cols]

    def by_role(ref_of, sem):
        @pl.when(owner)
        def _():
            came(ref_of(slice(0, 7)), sem)

        @pl.when(guest)
        def _():
            came(ref_of(slice(0, 8)), sem)

    def plane_out(src, c, first):
        cols = cols_of(c)
        for dx in (2, 1, 3, 0):
            x_to = (xi + dx) % 4
            for other in (1, 0):
                expert = hosted + other * (1 - 2 * hosted)
                if first:
                    core_to, lands = hosted, arr1.at[pi, :, cols]
                    recv = first_sem.at[c]
                else:
                    core_to, lands = expert, arr2.at[other, pi, :, cols]
                    recv = last_sem.at[other, c]
                send(
                    src.at[x_to * 2 + expert, :, cols],
                    lands,
                    out_sem.at[1 if first else 2],
                    recv,
                    zi * PLANE + x_to * 2 + core_to,
                    mirror if other else tp,
                    when=guest if dx == 0 and other == 0 else None,
                )

        @pl.when(owner)
        def _():
            if first:
                arr1[pi, :, cols] = src[pi, :, cols]
            else:
                arr2[0, pi, :, cols] = src[pi, :, cols]

    def z_to_expert(src, c):
        cols = cols_of(c)
        group = jnp.where(owner, 0, 1)
        for d in (*FAR_FIRST, 0):
            to = (zi + d) % PLANES
            send(
                src.at[to, :, cols],
                arr2.at[group, zi, :, cols],
                out_sem.at[3],
                last_sem.at[group, c],
                to * PLANE + place,
                tp,
                when=guest if d == 0 else None,
            )

        @pl.when(owner)
        def _():
            arr2[0, zi, :, cols] = src[zi, :, cols]

    def expert_to_z(cols, recv):
        for d in (*FAR_FIRST, 0):
            to = (zi + d) % PLANES
            for group in (0, 1):
                if d == 0 and group == 0:
                    ret1[zi, :, cols] = moe_out[0, zi, :, cols]
                    continue
                remote(
                    moe_out.at[group, to, :, cols],
                    ret1.at[zi, :, cols],
                    out_sem.at[4 + group],
                    recv,
                    to * PLANE + place + group * (1 - 2 * hosted),
                    tp,
                ).start()

    def expert_to_plane(cols, recv):
        for d in (*FAR_FIRST, 0):
            j = (pi + d) % PLANE
            for group in (1, 0):
                if d == 0 and group == 0:
                    ret1[pi, :, cols] = moe_out[0, pi, :, cols]
                    continue
                remote(
                    moe_out.at[group, j, :, cols],
                    ret1.at[place, :, cols],
                    out_sem.at[6 + group],
                    recv,
                    zi * PLANE + j,
                    mirror if group else tp,
                ).start()

    home = jnp.where(owner, tp, mirror)

    def plane_back(src, dst, cols, recv):
        for dx in (2, 1, 3, 0):
            for target_core in (0, 1):
                j = ((xi + dx) % 4) * 2 + target_core
                send(
                    src.at[j, :, cols],
                    dst.at[place, :, cols],
                    out_sem.at[8],
                    recv,
                    zi * PLANE + j,
                    home,
                    when=jnp.logical_or(guest, core != target_core) if dx == 0 else None,
                )

        @pl.when(owner)
        def _():
            dst[pi, :, cols] = src[pi, :, cols]

    def permuted(rows):
        return dot(pick, rows).astype(BF16)

    def swapped(src, cols):
        size = cols.stop - cols.start
        return permuted(src[:, :, cols].reshape(128, size)).reshape(8, 16, size)

    Z_FIRST = tuple(range(CHUNKS // 2))
    P_FIRST = tuple(range(CHUNKS // 2, CHUNKS))
    for c in (*Z_FIRST, *P_FIRST):
        cols = cols_of(c)
        order = int(c in P_FIRST)
        value = dot(slot_buf[order], normed[:, cols]).astype(BF16)
        disp[:, :, cols] = value.reshape(8, 16, width)
        if c in Z_FIRST:
            z_out(disp, arr1, cols, 0, first_sem.at[c])
        else:
            plane_out(disp, c, True)
    for k in range(4, PIECES):
        own_mirror(k)
    phase("shared")
    for k in (16, 17, 18, 19, 20):
        loads[k].wait()
    rows = normed[...]
    hidden = jax.nn.silu(dot(rows, shared_gate[...])) * dot(rows, shared_up[...])
    acc[...] = RESIDUAL_SCALE * rows.astype(F32) + dot(hidden.astype(BF16), shared_down[...])

    for c in P_FIRST:
        phase(f"disp_p1_{c}")
        by_role(lambda blocks: arr1.at[blocks, :, cols_of(c)], first_sem.at[c])
        phase(f"disp_swap_{c}")
        disp2[:, :, cols_of(c)] = swapped(arr1, cols_of(c))
        z_to_expert(disp2, c)
    for c in Z_FIRST:
        phase(f"disp_z1_{c}")
        came(arr1.at[0:7, :, cols_of(c)], first_sem.at[c])
        phase(f"disp_swap_{c}")
        disp2[:, :, cols_of(c)] = swapped(arr1, cols_of(c))
        plane_out(disp2, c, False)
        phase(f"relay_{c}")
        for k in range(4, 6) if c == 0 else range(6, PIECES):
            relay(k)
            if k + 1 < PIECES:
                own_out(k + 1)
    phase()

    @pl.when(owner)
    def _():
        phase("weights")
        for copy in slot_loads:
            copy.wait()
        for kind in (FROM_MATE, FROM_FAR):
            came(gate_up.at[:, origin[kind]], part_sem.at[kind, 0])
        both = None
        for c in [c for both_kinds in zip(Z_FIRST, P_FIRST) for c in both_kinds]:
            cols = cols_of(c)
            phase(f"disp_2_{c}")
            came(arr2.at[0, 0:7, :, cols], last_sem.at[0, c])
            came(arr2.at[1, :, :, cols], last_sem.at[1, c])
            phase(f"gate_up_{c}")
            groups = [arr2[g, :, :, cols].reshape(128, width) for g in (0, 1)]
            if c in P_FIRST:
                groups = [permuted(rows) for rows in groups]
            picked = jnp.concatenate(groups, axis=0)
            terms = [
                dot(picked, jnp.concatenate([gate_up[0, k, cols], gate_up[1, k, cols]], axis=1))
                for k in range(TPS)
            ]
            both = terms if both is None else [x + y for x, y in zip(both, terms)]
        phase("hidden")
        hidden = jnp.concatenate(
            [(jax.nn.silu(x[:, :128]) * x[:, 128:]).astype(BF16) for x in both], axis=1
        )
        by_plane = hidden
        by_z = jnp.concatenate([permuted(hidden[:128]), permuted(hidden[128:])], axis=0)
        for n, (cols, way) in enumerate(BACK):
            phase(f"down_arrive_{n}")
            held(4 + n, FROM_MATE)
            held(4 + n, FROM_FAR)
            phase(f"down_{n}")
            rows = by_z if way == "z" else by_plane
            size = cols.stop - cols.start
            value = dot(rows, down_w[:, :, cols].reshape(512, size)).astype(BF16)
            moe_out[:, :, :, cols] = value.reshape(2, 8, 16, size)
            if way == "z":
                expert_to_z(cols, back_sem.at[0, n])
            else:
                expert_to_plane(cols, back_sem.at[0, n])
        phase()

    for n in (0, 1, 3, 2, 4, 5):
        cols, way = BACK[n]
        phase(f"ret_1_{n}")
        by_role(lambda blocks: ret1.at[blocks, :, cols], back_sem.at[0, n])
        phase(f"ret_swap_{n}")
        ret1p[:, :, cols] = swapped(ret1, cols)
        if way == "z":
            plane_back(ret1p, ret2, cols, back_sem.at[1, n])
        else:
            z_out(ret1p, ret2, cols, 9, back_sem.at[1, n])
    for n in (0, 1, 3, 4, 2, 5):
        cols, way = BACK[n]
        phase(f"ret_2_{n}")
        if way == "z":
            by_role(lambda blocks: ret2.at[blocks, :, cols], back_sem.at[1, n])
        else:
            came(ret2.at[0:7, :, cols], back_sem.at[1, n])
        phase(f"combine_{n}")
        back = ret2[:, :, cols].reshape(128, cols.stop - cols.start)
        order = 0 if way == "z" else 2
        acc[:, cols] = (
            acc[:, cols] + dot(weight_buf[order], back) + dot(weight_buf[order + 1], back)
        )
    phase("norm2")
    out_ref[...] = layer_norm(acc[...], gain2[...], bias2[...]).astype(BF16)
    phase("drain")
    left(border_out, border_sem.at[0])
    left(carry1.at[0:7], carry_sem.at[0])
    for d in range(1, PLANES):

        @pl.when(zi + d < PLANES)
        def _():
            left(mine2, plane_sem.at[0, d - 1])

    left(part.at[0:3], mix_sem.at[0])
    by_z_back = sum(cols.stop - cols.start for cols, way in BACK if way == "z")
    sent_cols = {0: 1024, 1: 1024, 2: 1024, 3: 1024, 4: by_z_back, 5: by_z_back, 8: by_z_back}

    def all_left(k, blocks):
        left(disp.at[0:blocks, :, 0 : sent_cols.get(k, 2048 - by_z_back)], out_sem.at[k])

    for k in (0, 9):
        all_left(k, 7)

    @pl.when(owner)
    def _():
        for k in (1, 2, 3, 4, 6, 8):
            all_left(k, 7)
        for k in (5, 7):
            all_left(k, 8)
        left(gate_up.at[:, 0:2], part_out_sem.at[0])
        left(down_w.at[0:2], part_out_sem.at[1])

    @pl.when(guest)
    def _():
        for k in (1, 2, 3, 8):
            all_left(k, 8)
        left(gate_up.at[0, 0:2], part_out_sem.at[0])
        left(down_w.at[0], part_out_sem.at[1])

    phase()


def shards(
    stream, recurrence_input, output_gate_input, convolution_taps, first_group_gates,
    second_group_gates, channel_decay, position_log_extra, recurrence_output_weight,
    first_norm_gain, first_norm_bias, routed_expert_index, routed_expert_weight,
    routed_gate_weight, routed_up_weight, routed_down_weight, shared_gate_weight,
    shared_up_weight, shared_down_weight, second_norm_gain, second_norm_bias,
):
    operands = (
        stream,
        recurrence_input,
        output_gate_input,
        convolution_taps,
        first_group_gates,
        second_group_gates,
        channel_decay,
        position_log_extra,
        recurrence_output_weight.reshape(512, 2048),
        first_norm_gain.reshape(1, 2048),
        first_norm_bias.reshape(1, 2048),
        routed_expert_index.T,
        routed_expert_weight.T,
        routed_gate_weight.reshape(2048, 128),
        routed_up_weight.reshape(2048, 128),
        routed_down_weight.reshape(128, 2048),
        shared_gate_weight,
        shared_up_weight,
        shared_down_weight,
        second_norm_gain.reshape(1, 2048),
        second_norm_bias.reshape(1, 2048),
    )
    held = [pltpu.VMEM(operand.shape, operand.dtype) for operand in operands]
    wide = pltpu.VMEM((8, 16, 2048), BF16)
    return pl.pallas_call(
        mega,
        out_shape=jax.ShapeDtypeStruct((32, 2048), BF16),
        in_specs=[pl.BlockSpec(memory_space=pl.ANY)] * len(operands),
        out_specs=pl.BlockSpec(memory_space=pltpu.VMEM),
        scratch_shapes=[
            *held,
            pltpu.VMEM((2, TPS, 2048, 128), BF16),
            pltpu.VMEM((TPS, 128, 2048), BF16),
            pltpu.VMEM((128, 512), F32),
            pltpu.VMEM((2, 128, 8), F32),
            pltpu.VMEM((128 + HEAD_ROWS, 512), F32),
            pltpu.VMEM((HEAD_ROWS, 2, 256), BF16),
            pltpu.VMEM((128, 512), F32),
            pltpu.VMEM((128, 512), F32),
            pltpu.VMEM((PLANE, 2, 4, 128), F32),
            pltpu.VMEM((PLANES, 2, 4, 128), F32),
            pltpu.VMEM((128, 512), F32),
            pltpu.VMEM((128, 512), BF16),
            pltpu.VMEM((TPS, 32, 2048), BF16),
            pltpu.VMEM((TPS, 32, 2048), BF16),
            pltpu.VMEM((32, 2048), BF16),
            pltpu.VMEM((2, 128, 32), BF16),
            pltpu.VMEM((4, 32, 128), BF16),
            wide, wide, wide,
            pltpu.VMEM((2, 8, 16, 2048), BF16),
            pltpu.VMEM((2, 8, 16, 2048), BF16),
            wide, wide, wide,
            pltpu.VMEM((32, 2048), F32),
            pltpu.SemaphoreType.DMA((len(operands),)),
            pltpu.SemaphoreType.DMA((3,)),
            pltpu.SemaphoreType.DMA((2,)),
            pltpu.SemaphoreType.DMA((3, PIECES)),
            pltpu.SemaphoreType.DMA((2,)),
            pltpu.SemaphoreType.DMA((2,)),
            pltpu.SemaphoreType.DMA((2, 7)),
            pltpu.SemaphoreType.DMA((2,)),
            pltpu.SemaphoreType.DMA((CHUNKS,)),
            pltpu.SemaphoreType.DMA((2, CHUNKS)),
            pltpu.SemaphoreType.DMA((2, len(BACK))),
            pltpu.SemaphoreType.DMA((10,)),
        ],
        compiler_params=pltpu.CompilerParams(
            collective_id=0, has_side_effects=True, vmem_limit_bytes=56 * 2**20
        ),
        name="mega",
    )(*operands)


def solution(mesh):
    in_specs = (
        P(("sp", "tp"), None),
        P("sp", None, "tp"),
        P("sp", None, "tp"),
        P(None, None, "tp"),
        P(None, "tp", None, None),
        P(None, "tp", None, None),
        P(None, "tp"),
        P("sp", None, "tp"),
        P(None, "tp", None),
        P(),
        P(),
        P("sp", None),
        P("sp", None),
        P("sp", None, "tp"),
        P("sp", None, "tp"),
        P("sp", "tp", None),
        P(),
        P(),
        P(),
        P(),
        P(),
    )
    out_specs = P(("sp", "tp"), None)
    return jax.shard_map(shards, mesh=mesh, in_specs=in_specs, out_specs=out_specs, check_vma=False)
```

```python
import jax
import jax.numpy as jnp
from jax import lax
from jax.experimental import pallas as pl
from jax.experimental.pallas import tpu as pltpu
from jax.sharding import PartitionSpec as P

RESIDUAL_SCALE = 8.0**0.25
NORM_EPSILON = 1e-05
MESH = pl.DeviceIdType.MESH
F32 = jnp.float32
BF16 = jnp.bfloat16

PLANE = 8
PLANES = 8
TPS = 4
HEAD_ROWS = 16
CHUNKS = 4
BACK = (
    (slice(0, 512), "z"),
    (slice(512, 1024), "z"),
    (slice(1024, 1280), "z"),
    (slice(1280, 1536), "plane"),
    (slice(1536, 1792), "plane"),
    (slice(1792, 2048), "plane"),
)
PIECES = 4 + len(BACK)
FAR_FIRST = (4, 3, 5, 2, 6, 1, 7)


class Phases:
    def __init__(self):
        self.scope = None

    def __call__(self, name=None):
        if self.scope is not None:
            self.scope.__exit__(None, None, None)
        self.scope = None
        if name is not None:
            self.scope = jax.named_scope(name)
            self.scope.__enter__()


def layer_norm(values, gain_vec, bias_vec):
    row_mean = jnp.mean(values, axis=-1, keepdims=True)
    centred = values - row_mean
    spread = jnp.mean(jnp.square(centred), axis=-1, keepdims=True)
    return centred * lax.rsqrt(spread + NORM_EPSILON) * gain_vec + bias_vec


def softplus_of_minus(d):
    u = jnp.exp(-jnp.abs(d))
    s = u / (2.0 + u)
    q = s * s
    series = jnp.full_like(s, 1.0 / 15.0)
    for odd in (13, 11, 9, 7, 5, 3, 1):
        series = series * q + 1.0 / odd
    return jnp.maximum(-d, 0.0) + 2.0 * s * series


def minus_expm1(z):
    series = jnp.full_like(z, 1.0 / 40320.0)
    for factor in (5040.0, 720.0, 120.0, 24.0, 6.0, 2.0, 1.0):
        series = series * z + 1.0 / factor
    return jnp.where(z > -0.25, -z * series, 1.0 - jnp.exp(z))


def dot(a, b):
    return jnp.dot(a, b, preferred_element_type=F32)


def mega(
    stream_h, rec_h, gatein_h, taps_h, small_gates_h, large_gates_h, decay_h, extra_h,
    wout_h, gain1_h, bias1_h, index_h, weight_h, gate_w_h, up_w_h, down_w_h,
    shared_gate_h, shared_up_h, shared_down_h, gain2_h, bias2_h,
    out_ref,
    stream, rec, gatein, taps, small_gates, large_gates, decay, extra_raw,
    wout, gain1, bias1, index, weight, own_gate, own_up, own_down,
    shared_gate, shared_up, shared_down, gain2, bias2,
    gate_up, down_w,
    extra, turned, rec_f, border, cum_p, cum_s, carry1, carry2, gelu_buf, branch,
    part, mixed_buf, normed, slot_buf, weight_buf,
    disp, arr1, disp2, arr2, moe_out, ret1, ret1p, ret2, acc,
    load_sem, slot_sem, border_sem, part_sem, part_out_sem, carry_sem, plane_sem, mix_sem,
    first_sem, last_sem, back_sem, out_sem,
):
    sp = lax.axis_index("sp")
    tp = lax.axis_index("tp")
    zi = sp // PLANE
    pi = sp % PLANE
    xi = pi // 2
    core = sp % 2
    hosted = tp // 2
    mirror = 3 - tp
    mate = tp + 1 - 2 * (tp % 2)
    far = 3 - mate
    place = xi * 2 + hosted
    owner = core == hosted
    guest = core != hosted
    phase = Phases()
    phase("loads")

    def remote(src, dst, send_sem, recv_sem, sp_to, tp_to):
        return pltpu.make_async_remote_copy(
            src_ref=src,
            dst_ref=dst,
            send_sem=send_sem,
            recv_sem=recv_sem,
            device_id={"sp": sp_to, "tp": tp_to},
            device_id_type=MESH,
        )

    def send(*args, when=None):
        copy = remote(*args)
        if when is None:
            copy.start()
        else:
            pl.when(when)(copy.start)

    def came(ref, sem):
        remote(ref, ref, sem, sem, sp, tp).wait_recv()

    def left(ref, sem):
        remote(ref, ref, sem, sem, sp, tp).wait_send()

    def plane_peer(d):
        return zi * PLANE + (pi + d) % PLANE

    def z_peer(d):
        return ((zi + d) % PLANES) * PLANE + pi

    barrier = pltpu.get_barrier_semaphore()

    def greet(sp_to, tp_to):
        pl.semaphore_signal(
            barrier, inc=1, device_id={"sp": sp_to, "tp": tp_to}, device_id_type=MESH
        )

    for d in FAR_FIRST:
        greet(z_peer(d), tp)
    for d in FAR_FIRST:
        greet(plane_peer(d), tp)
    for d in range(1, TPS):
        greet(sp, (tp + d) % TPS)
    greet((sp + 63) % 64, tp)
    for j in range(PLANE):
        greet(zi * PLANE + j, mirror)
    for d in FAR_FIRST:
        greet(z_peer(d) + 1 - 2 * core, tp)

    names = (
        (rec_h, rec), (small_gates_h, small_gates), (large_gates_h, large_gates), (taps_h, taps),
        (decay_h, decay), (extra_h, extra_raw), (gatein_h, gatein), (gate_w_h, own_gate),
        (up_w_h, own_up), (down_w_h, own_down), (wout_h, wout), (index_h, index),
        (weight_h, weight), (stream_h, stream), (gain1_h, gain1), (bias1_h, bias1),
        (shared_gate_h, shared_gate), (shared_up_h, shared_up), (shared_down_h, shared_down),
        (gain2_h, gain2), (bias2_h, bias2),
    )
    loads = [pltpu.make_async_copy(src, dst, load_sem.at[k]) for k, (src, dst) in enumerate(names)]
    urgent = (0, 7, 8)
    for k in (*urgent, *(k for k in range(len(names)) if k not in urgent)):
        loads[k].start()
    wholes = (gate_up.at[0], gate_up.at[1], down_w)
    owns = (own_gate, own_up, own_down)
    slot_loads = [
        pltpu.make_async_copy(src, dst.at[tp], slot_sem.at[m])
        for m, (src, dst) in enumerate(zip((gate_w_h, up_w_h, down_w_h), wholes))
    ]

    @pl.when(owner)
    def _():
        for copy in slot_loads:
            copy.start()

    phase("wait_loads")
    length = rec.shape[0]
    loads[0].wait()
    phase("barrier")
    pl.semaphore_wait(barrier, 7 + 7 + 3 + 1 + 8 + 7)
    phase("send_gate")
    border_out = rec.at[length - HEAD_ROWS :]
    send(border_out, border, border_sem.at[0], border_sem.at[1], (sp + 1) % 64, tp)

    FROM_MATE, FROM_MIRROR, FROM_FAR = range(3)
    origin = {FROM_MATE: mate, FROM_MIRROR: mirror, FROM_FAR: far}

    def piece_of(ref, k, lead=()):
        if k < 4:
            return ref.at[(*lead, slice(1024 * (k % 2), 1024 * (k % 2) + 1024))]
        return ref.at[(*lead, slice(None), BACK[k - 4][0])]

    def buffer_of(k):
        return k // 2 if k < 4 else 2

    def held_piece(k, at):
        return piece_of(wholes[buffer_of(k)], k, (at,))

    def arrival(kind, k):
        return part_sem.at[kind, k if kind == FROM_MIRROR else max(k - 3, 0)]

    def across(src, k, at, kind, tp_to, when):
        out = part_out_sem.at[int(k >= 4)]
        send(src, held_piece(k, at), out, arrival(kind, k), sp, tp_to, when=when)

    def own_out(k):
        src = piece_of(owns[buffer_of(k)], k)
        across(src, k, tp, FROM_MATE, mate, owner)

    def own_mirror(k):
        src = piece_of(owns[buffer_of(k)], k)
        across(src, k, tp, FROM_MIRROR, mirror, guest)

    def held(k, kind):
        came(held_piece(k, origin[kind]), arrival(kind, k))

    def relay(k):
        @pl.when(owner)
        def _():
            held(k, FROM_MIRROR)

        across(held_piece(k, mirror), k, mirror, FROM_FAR, mate, owner)

    for k in (7, 8):
        loads[k].wait()
    for k in (0, 1, 2, 3):
        own_out(k)
        own_mirror(k)

    phase("prepare")
    for k in range(1, 6):
        loads[k].wait()
    for g in range(2):
        rec_f[HEAD_ROWS:, 256 * g : 256 * g + 256] = rec[:, g, :].astype(F32)
        extra[:, 256 * g : 256 * g + 256] = extra_raw[:, g, :]
    row_i = lax.broadcasted_iota(jnp.int32, (64, 128), 0)
    col_i = lax.broadcasted_iota(jnp.int32, (64, 128), 1)
    put_low = (row_i == col_i).astype(BF16)
    put_high = (row_i + 64 == col_i).astype(BF16)
    blocks = []
    for which in range(2):
        maps = []
        for pair in range(2):
            low = dot(small_gates[which, 2 * pair], put_low)
            high = dot(small_gates[which, 2 * pair + 1], put_high)
            maps.append(jnp.concatenate([low, high], axis=0).astype(BF16))
        for head in range(2):
            maps.append(large_gates[which, head])
        blocks.append(maps)
    rate = -8.0 * softplus_of_minus(decay[...])
    tap_f = taps[...].astype(F32)

    def tap(k, b):
        return tap_f[k, b // 2 : b // 2 + 1, 128 * (b % 2) : 128 * (b % 2) + 128]

    def scanned(first, count):
        for b in range(4):
            lanes = slice(128 * b, 128 * b + 128)
            conv = tap(0, b) * rec_f[first + HEAD_ROWS - 3 : first + HEAD_ROWS - 3 + count, lanes]
            for k in range(1, 4):
                at = first + HEAD_ROWS - 3 + k
                conv = conv + tap(k, b) * rec_f[at : at + count, lanes]
            conv = conv.astype(BF16)
            recur_gate = jax.nn.sigmoid(dot(conv, blocks[0][b]))
            input_gate = jax.nn.sigmoid(dot(conv, blocks[1][b]))
            log_decay = recur_gate * rate[b // 2 : b // 2 + 1, 128 * (b % 2) : 128 * (b % 2) + 128] + extra[first : first + count, lanes]
            p = jnp.exp(log_decay)
            s = jnp.sqrt(minus_expm1(2.0 * log_decay)) * input_gate * conv.astype(F32)
            p = p.reshape(count // 8, 8, 128)
            s = s.reshape(count // 8, 8, 128)
            row = lax.broadcasted_iota(jnp.int32, (count // 8, 8, 128), 1)
            for by in (1, 2, 4):
                p_prev = pltpu.roll(p, by, 1)
                s_prev = pltpu.roll(s, by, 1)
                s = jnp.where(row >= by, p * s_prev + s, s)
                p = jnp.where(row >= by, p * p_prev, p)
            p_in = jnp.ones((1, 128), F32)
            s_in = jnp.zeros((1, 128), F32)
            for t in range(count // 8):
                s_t = s[t] + p[t] * s_in
                p_t = p[t] * p_in
                cum_s[first + 8 * t : first + 8 * t + 8, lanes] = s_t
                cum_p[first + 8 * t : first + 8 * t + 8, lanes] = p_t
                s_in = s_t[7:8]
                p_in = p_t[7:8]

    phase("scan_tail")
    scanned(HEAD_ROWS, length - HEAD_ROWS)
    loads[9].wait()
    phase("border")
    came(border, border_sem.at[1])
    phase("scan_head")
    for g in range(2):
        border_f = border[:, g, :].astype(F32)
        rec_f[0:HEAD_ROWS, 256 * g : 256 * g + 256] = jnp.where(
            sp > 0, border_f, jnp.zeros_like(border_f)
        )
    scanned(0, HEAD_ROWS)

    head_p = cum_p[HEAD_ROWS - 1 : HEAD_ROWS, :]
    head_s = cum_s[HEAD_ROWS - 1 : HEAD_ROWS, :]
    tail_p = cum_p[length - 1 : length, :]
    tail_s = cum_s[length - 1 : length, :]
    total_p = head_p * tail_p
    total_s = tail_p * head_s + tail_s
    mine1 = carry1.at[pi]
    for b in range(4):
        mine1[0, b : b + 1, :] = total_p[:, 128 * b : 128 * b + 128]
        mine1[1, b : b + 1, :] = total_s[:, 128 * b : 128 * b + 128]
    for d in FAR_FIRST:
        send(mine1, mine1, carry_sem.at[0], carry_sem.at[1], plane_peer(d), tp)

    phase("slots")
    for k in (6, 11, 12):
        loads[k].wait()
    own_rows = pl.ds(pl.multiple_of(tp * 32, 32), 32)
    unused = jnp.zeros((4, 128), F32)
    turned[0] = jnp.concatenate([index[...].astype(F32), unused], axis=0).T
    turned[1] = jnp.concatenate([weight[...], unused], axis=0).T
    ids = turned[0, own_rows, :].astype(jnp.int32)
    factors = turned[1, own_rows, :]
    slot = lax.broadcasted_iota(jnp.int32, (32, 128), 1)
    named = jnp.zeros((32, 128), F32)
    scaled = jnp.zeros((32, 128), F32)
    for k in range(4):
        hit = ids[:, k : k + 1] == slot // 2
        named = named + jnp.where(hit, 1.0, 0.0)
        scaled = scaled + jnp.where(hit, factors[:, k : k + 1], 0.0)
    below = lax.broadcasted_iota(jnp.int32, (32, 32), 0) > lax.broadcasted_iota(
        jnp.int32, (32, 32), 1
    )
    earlier = dot(below.astype(BF16), named.astype(BF16))
    right_slot = jnp.abs(earlier - (slot % 2).astype(F32)) < 0.5
    to_row = lax.broadcasted_iota(jnp.int32, (128, 128), 0)
    from_row = lax.broadcasted_iota(jnp.int32, (128, 128), 1)
    outer, inner, pair = to_row // 16, (to_row // 2) % 8, to_row % 2
    pick = (from_row == inner * 16 + outer * 2 + pair).astype(BF16)
    slot_rows = jnp.where(right_slot, named, 0.0).T.astype(BF16)
    slot_buf[0] = slot_rows
    slot_buf[1] = dot(pick, slot_rows).astype(BF16)
    scaled = jnp.where(right_slot, scaled, 0.0)
    high = scaled.astype(BF16)
    low = (scaled - high.astype(F32)).astype(BF16)
    for part_no, values in enumerate((high, low)):
        weight_buf[part_no] = dot(values, pick).astype(BF16)
        weight_buf[2 + part_no] = values
    for g in range(2):
        gelu_buf[:, 256 * g : 256 * g + 256] = jax.nn.gelu(gatein[:, g, :].astype(F32))
    phase("carry1")

    came(carry1.at[0:7], carry_sem.at[1])
    one = jnp.ones((4, 128), F32)
    nought = jnp.zeros((4, 128), F32)
    all_p, all_s, in_p, in_s = one, nought, one, nought
    for j in range(PLANE):
        p_j, s_j = carry1[j, 0], carry1[j, 1]
        all_p, all_s = all_p * p_j, p_j * all_s + s_j
        in_p = jnp.where(j < pi, in_p * p_j, in_p)
        in_s = jnp.where(j < pi, p_j * in_s + s_j, in_s)
    mine2 = carry2.at[zi]
    mine2[0] = all_p
    mine2[1] = all_s
    for d in (4, 3, 5, 2, 6, 1, 7):
        send(
            mine2,
            mine2,
            plane_sem.at[0, d - 1],
            plane_sem.at[1, d - 1],
            z_peer(d),
            tp,
            when=zi + d < PLANES,
        )
    phase("carry2")
    for d in range(1, PLANES):
        got = carry2.at[(zi + PLANES - d) % PLANES]

        @pl.when(zi >= d)
        def _():
            came(got, plane_sem.at[1, d - 1])

    phase("fixup")
    planes_s = nought
    for k in range(PLANES):
        planes_s = jnp.where(k < zi, carry2[k, 0] * planes_s + carry2[k, 1], planes_s)
    carry_in = in_p * planes_s + in_s
    carry_row = jnp.concatenate([carry_in[b : b + 1] for b in range(4)], axis=1)
    carry_tail = head_s + head_p * carry_row
    states = cum_s[:HEAD_ROWS] + cum_p[:HEAD_ROWS] * carry_row
    branch[:HEAD_ROWS, :] = (gelu_buf[:HEAD_ROWS] * states).astype(BF16)
    states = cum_s[HEAD_ROWS:] + cum_p[HEAD_ROWS:] * carry_tail
    branch[HEAD_ROWS:, :] = (gelu_buf[HEAD_ROWS:] * states).astype(BF16)

    phase("out_proj")
    loads[10].wait()
    for c in range(4):
        cols = slice(512 * c, 512 * c + 512)
        value = dot(branch[...], wout[:, cols]).astype(BF16)
        part[:, :, cols] = value.reshape(TPS, 32, 512)
        for d in (2, 1, 3):
            to = (tp + d) % TPS
            lands = mixed_buf.at[tp, :, cols]
            send(part.at[to, :, cols], lands, mix_sem.at[0], mix_sem.at[1], sp, to)
    phase("gate_arrive")
    for k in (0, 1, 2, 3):
        relay(k)
    own_out(4)
    phase("mix_arrive")
    for k in (13, 14, 15):
        loads[k].wait()
    came(mixed_buf.at[0:3], mix_sem.at[1])
    phase("norm1")
    mixed = part[tp].astype(F32)
    for d in (1, 2, 3):
        mixed = mixed + mixed_buf[(tp + d) % TPS].astype(F32)
    normed[...] = layer_norm(
        RESIDUAL_SCALE * stream[...].astype(F32) + mixed, gain1[...], bias1[...]
    ).astype(BF16)

    width = 2048 // CHUNKS

    def cols_of(c):
        return slice(width * c, width * c + width)

    def z_out(src, dst, cols, out, recv):
        for d in FAR_FIRST:
            to = (zi + d) % PLANES
            lands = dst.at[zi, :, cols]
            send(src.at[to, :, cols], lands, out_sem.at[out], recv, z_peer(d), tp)
        dst[zi, :, cols] = src[zi, :, cols]

    def by_role(ref_of, sem):
        @pl.when(owner)
        def _():
            came(ref_of(slice(0, 7)), sem)

        @pl.when(guest)
        def _():
            came(ref_of(slice(0, 8)), sem)

    def plane_out(src, c, first):
        cols = cols_of(c)
        for dx in (2, 1, 3, 0):
            x_to = (xi + dx) % 4
            for other in (1, 0):
                expert = hosted + other * (1 - 2 * hosted)
                if first:
                    core_to, lands = hosted, arr1.at[pi, :, cols]
                    recv = first_sem.at[c]
                else:
                    core_to, lands = expert, arr2.at[other, pi, :, cols]
                    recv = last_sem.at[other, c]
                send(
                    src.at[x_to * 2 + expert, :, cols],
                    lands,
                    out_sem.at[1 if first else 2],
                    recv,
                    zi * PLANE + x_to * 2 + core_to,
                    mirror if other else tp,
                    when=guest if dx == 0 and other == 0 else None,
                )

        @pl.when(owner)
        def _():
            if first:
                arr1[pi, :, cols] = src[pi, :, cols]
            else:
                arr2[0, pi, :, cols] = src[pi, :, cols]

    def z_to_expert(src, c):
        cols = cols_of(c)
        group = jnp.where(owner, 0, 1)
        for d in (*FAR_FIRST, 0):
            to = (zi + d) % PLANES
            send(
                src.at[to, :, cols],
                arr2.at[group, zi, :, cols],
                out_sem.at[3],
                last_sem.at[group, c],
                to * PLANE + place,
                tp,
                when=guest if d == 0 else None,
            )

        @pl.when(owner)
        def _():
            arr2[0, zi, :, cols] = src[zi, :, cols]

    def expert_to_z(cols, recv):
        for d in (*FAR_FIRST, 0):
            to = (zi + d) % PLANES
            for group in (0, 1):
                if d == 0 and group == 0:
                    ret1[zi, :, cols] = moe_out[0, zi, :, cols]
                    continue
                remote(
                    moe_out.at[group, to, :, cols],
                    ret1.at[zi, :, cols],
                    out_sem.at[4 + group],
                    recv,
                    to * PLANE + place + group * (1 - 2 * hosted),
                    tp,
                ).start()

    def expert_to_plane(cols, recv):
        for d in (*FAR_FIRST, 0):
            j = (pi + d) % PLANE
            for group in (1, 0):
                if d == 0 and group == 0:
                    ret1[pi, :, cols] = moe_out[0, pi, :, cols]
                    continue
                remote(
                    moe_out.at[group, j, :, cols],
                    ret1.at[place, :, cols],
                    out_sem.at[6 + group],
                    recv,
                    zi * PLANE + j,
                    mirror if group else tp,
                ).start()

    home = jnp.where(owner, tp, mirror)

    def plane_back(src, dst, cols, recv):
        for dx in (2, 1, 3, 0):
            for target_core in (0, 1):
                j = ((xi + dx) % 4) * 2 + target_core
                send(
                    src.at[j, :, cols],
                    dst.at[place, :, cols],
                    out_sem.at[8],
                    recv,
                    zi * PLANE + j,
                    home,
                    when=jnp.logical_or(guest, core != target_core) if dx == 0 else None,
                )

        @pl.when(owner)
        def _():
            dst[pi, :, cols] = src[pi, :, cols]

    def permuted(rows):
        return dot(pick, rows).astype(BF16)

    def swapped(src, cols):
        size = cols.stop - cols.start
        return permuted(src[:, :, cols].reshape(128, size)).reshape(8, 16, size)

    Z_FIRST = tuple(range(CHUNKS // 2))
    P_FIRST = tuple(range(CHUNKS // 2, CHUNKS))
    for c in [c for pair_of in zip(Z_FIRST, P_FIRST) for c in pair_of]:
        cols = cols_of(c)
        order = int(c in P_FIRST)
        value = dot(slot_buf[order], normed[:, cols]).astype(BF16)
        disp[:, :, cols] = value.reshape(8, 16, width)
        if c in Z_FIRST:
            z_out(disp, arr1, cols, 0, first_sem.at[c])
        else:
            plane_out(disp, c, True)
    for k in range(4, PIECES):
        own_mirror(k)
    phase("shared")
    for k in (16, 17, 18, 19, 20):
        loads[k].wait()
    rows = normed[...]
    hidden = jax.nn.silu(dot(rows, shared_gate[...])) * dot(rows, shared_up[...])
    acc[...] = RESIDUAL_SCALE * rows.astype(F32) + dot(hidden.astype(BF16), shared_down[...])

    for c in P_FIRST:
        phase(f"disp_p1_{c}")
        by_role(lambda blocks: arr1.at[blocks, :, cols_of(c)], first_sem.at[c])
        phase(f"disp_swap_{c}")
        disp2[:, :, cols_of(c)] = swapped(arr1, cols_of(c))
        z_to_expert(disp2, c)
    for c in Z_FIRST:
        phase(f"disp_z1_{c}")
        came(arr1.at[0:7, :, cols_of(c)], first_sem.at[c])
        phase(f"disp_swap_{c}")
        disp2[:, :, cols_of(c)] = swapped(arr1, cols_of(c))
        plane_out(disp2, c, False)
        phase(f"relay_{c}")
        for k in range(4, 6) if c == 0 else range(6, PIECES):
            relay(k)
            if k + 1 < PIECES:
                own_out(k + 1)
    phase()

    @pl.when(owner)
    def _():
        phase("weights")
        for copy in slot_loads:
            copy.wait()
        for kind in (FROM_MATE, FROM_FAR):
            came(gate_up.at[:, origin[kind]], part_sem.at[kind, 0])
        both = None
        for c in [c for both_kinds in zip(Z_FIRST, P_FIRST) for c in both_kinds]:
            cols = cols_of(c)
            phase(f"disp_2_{c}")
            came(arr2.at[0, 0:7, :, cols], last_sem.at[0, c])
            came(arr2.at[1, :, :, cols], last_sem.at[1, c])
            phase(f"gate_up_{c}")
            groups = [arr2[g, :, :, cols].reshape(128, width) for g in (0, 1)]
            if c in P_FIRST:
                groups = [permuted(rows) for rows in groups]
            picked = jnp.concatenate(groups, axis=0)
            terms = [
                dot(picked, jnp.concatenate([gate_up[0, k, cols], gate_up[1, k, cols]], axis=1))
                for k in range(TPS)
            ]
            both = terms if both is None else [x + y for x, y in zip(both, terms)]
        phase("hidden")
        hidden = jnp.concatenate(
            [(jax.nn.silu(x[:, :128]) * x[:, 128:]).astype(BF16) for x in both], axis=1
        )
        by_plane = hidden
        by_z = jnp.concatenate([permuted(hidden[:128]), permuted(hidden[128:])], axis=0)
        for n, (cols, way) in enumerate(BACK):
            phase(f"down_arrive_{n}")
            held(4 + n, FROM_MATE)
            held(4 + n, FROM_FAR)
            phase(f"down_{n}")
            rows = by_z if way == "z" else by_plane
            size = cols.stop - cols.start
            value = dot(rows, down_w[:, :, cols].reshape(512, size)).astype(BF16)
            moe_out[:, :, :, cols] = value.reshape(2, 8, 16, size)
            if way == "z":
                expert_to_z(cols, back_sem.at[0, n])
            else:
                expert_to_plane(cols, back_sem.at[0, n])
        phase()

    for n in (0, 1, 3, 4, 2, 5):
        cols, way = BACK[n]
        phase(f"ret_1_{n}")
        by_role(lambda blocks: ret1.at[blocks, :, cols], back_sem.at[0, n])
        phase(f"ret_swap_{n}")
        ret1p[:, :, cols] = swapped(ret1, cols)
        if way == "z":
            plane_back(ret1p, ret2, cols, back_sem.at[1, n])
        else:
            z_out(ret1p, ret2, cols, 9, back_sem.at[1, n])
    for n in (0, 1, 3, 4, 2, 5):
        cols, way = BACK[n]
        phase(f"ret_2_{n}")
        if way == "z":
            by_role(lambda blocks: ret2.at[blocks, :, cols], back_sem.at[1, n])
        else:
            came(ret2.at[0:7, :, cols], back_sem.at[1, n])
        phase(f"combine_{n}")
        back = ret2[:, :, cols].reshape(128, cols.stop - cols.start)
        order = 0 if way == "z" else 2
        acc[:, cols] = (
            acc[:, cols] + dot(weight_buf[order], back) + dot(weight_buf[order + 1], back)
        )
    phase("norm2")
    out_ref[...] = layer_norm(acc[...], gain2[...], bias2[...]).astype(BF16)
    phase("drain")
    left(border_out, border_sem.at[0])
    left(carry1.at[0:7], carry_sem.at[0])
    for d in range(1, PLANES):

        @pl.when(zi + d < PLANES)
        def _():
            left(mine2, plane_sem.at[0, d - 1])

    left(part.at[0:3], mix_sem.at[0])
    by_z_back = sum(cols.stop - cols.start for cols, way in BACK if way == "z")
    sent_cols = {0: 1024, 1: 1024, 2: 1024, 3: 1024, 4: by_z_back, 5: by_z_back, 8: by_z_back}

    def all_left(k, blocks):
        left(disp.at[0:blocks, :, 0 : sent_cols.get(k, 2048 - by_z_back)], out_sem.at[k])

    for k in (0, 9):
        all_left(k, 7)

    @pl.when(owner)
    def _():
        for k in (1, 2, 3, 4, 6, 8):
            all_left(k, 7)
        for k in (5, 7):
            all_left(k, 8)
        left(gate_up.at[:, 0:2], part_out_sem.at[0])
        left(down_w.at[0:2], part_out_sem.at[1])

    @pl.when(guest)
    def _():
        for k in (1, 2, 3, 8):
            all_left(k, 8)
        left(gate_up.at[0, 0:2], part_out_sem.at[0])
        left(down_w.at[0], part_out_sem.at[1])

    phase()


def shards(
    stream, recurrence_input, output_gate_input, convolution_taps, first_group_gates,
    second_group_gates, channel_decay, position_log_extra, recurrence_output_weight,
    first_norm_gain, first_norm_bias, routed_expert_index, routed_expert_weight,
    routed_gate_weight, routed_up_weight, routed_down_weight, shared_gate_weight,
    shared_up_weight, shared_down_weight, second_norm_gain, second_norm_bias,
):
    operands = (
        stream,
        recurrence_input,
        output_gate_input,
        convolution_taps,
        first_group_gates,
        second_group_gates,
        channel_decay,
        position_log_extra,
        recurrence_output_weight.reshape(512, 2048),
        first_norm_gain.reshape(1, 2048),
        first_norm_bias.reshape(1, 2048),
        routed_expert_index.T,
        routed_expert_weight.T,
        routed_gate_weight.reshape(2048, 128),
        routed_up_weight.reshape(2048, 128),
        routed_down_weight.reshape(128, 2048),
        shared_gate_weight,
        shared_up_weight,
        shared_down_weight,
        second_norm_gain.reshape(1, 2048),
        second_norm_bias.reshape(1, 2048),
    )
    held = [pltpu.VMEM(operand.shape, operand.dtype) for operand in operands]
    wide = pltpu.VMEM((8, 16, 2048), BF16)
    return pl.pallas_call(
        mega,
        out_shape=jax.ShapeDtypeStruct((32, 2048), BF16),
        in_specs=[pl.BlockSpec(memory_space=pl.ANY)] * len(operands),
        out_specs=pl.BlockSpec(memory_space=pltpu.VMEM),
        scratch_shapes=[
            *held,
            pltpu.VMEM((2, TPS, 2048, 128), BF16),
            pltpu.VMEM((TPS, 128, 2048), BF16),
            pltpu.VMEM((128, 512), F32),
            pltpu.VMEM((2, 128, 8), F32),
            pltpu.VMEM((128 + HEAD_ROWS, 512), F32),
            pltpu.VMEM((HEAD_ROWS, 2, 256), BF16),
            pltpu.VMEM((128, 512), F32),
            pltpu.VMEM((128, 512), F32),
            pltpu.VMEM((PLANE, 2, 4, 128), F32),
            pltpu.VMEM((PLANES, 2, 4, 128), F32),
            pltpu.VMEM((128, 512), F32),
            pltpu.VMEM((128, 512), BF16),
            pltpu.VMEM((TPS, 32, 2048), BF16),
            pltpu.VMEM((TPS, 32, 2048), BF16),
            pltpu.VMEM((32, 2048), BF16),
            pltpu.VMEM((2, 128, 32), BF16),
            pltpu.VMEM((4, 32, 128), BF16),
            wide, wide, wide,
            pltpu.VMEM((2, 8, 16, 2048), BF16),
            pltpu.VMEM((2, 8, 16, 2048), BF16),
            wide, wide, wide,
            pltpu.VMEM((32, 2048), F32),
            pltpu.SemaphoreType.DMA((len(operands),)),
            pltpu.SemaphoreType.DMA((3,)),
            pltpu.SemaphoreType.DMA((2,)),
            pltpu.SemaphoreType.DMA((3, PIECES)),
            pltpu.SemaphoreType.DMA((2,)),
            pltpu.SemaphoreType.DMA((2,)),
            pltpu.SemaphoreType.DMA((2, 7)),
            pltpu.SemaphoreType.DMA((2,)),
            pltpu.SemaphoreType.DMA((CHUNKS,)),
            pltpu.SemaphoreType.DMA((2, CHUNKS)),
            pltpu.SemaphoreType.DMA((2, len(BACK))),
            pltpu.SemaphoreType.DMA((10,)),
        ],
        compiler_params=pltpu.CompilerParams(
            collective_id=0, has_side_effects=True, vmem_limit_bytes=56 * 2**20
        ),
        name="mega",
    )(*operands)


def solution(mesh):
    in_specs = (
        P(("sp", "tp"), None),
        P("sp", None, "tp"),
        P("sp", None, "tp"),
        P(None, None, "tp"),
        P(None, "tp", None, None),
        P(None, "tp", None, None),
        P(None, "tp"),
        P("sp", None, "tp"),
        P(None, "tp", None),
        P(),
        P(),
        P("sp", None),
        P("sp", None),
        P("sp", None, "tp"),
        P("sp", None, "tp"),
        P("sp", "tp", None),
        P(),
        P(),
        P(),
        P(),
        P(),
    )
    out_specs = P(("sp", "tp"), None)
    return jax.shard_map(shards, mesh=mesh, in_specs=in_specs, out_specs=out_specs, check_vma=False)
```
